512 devices in a mesh: sp: 32 (over z, core), tp: 16 (over y, x).
Axes of the slice: x: 4, y: 4, z: 16, core: 2. Of those that a mesh axis runs over, the one named last changes fastest.
Arguments:
- query_major: bfloat16 [4096, 3072], P('sp', 'tp'), may hold values from -256 to 256
- query_minor: bfloat16 [4096, 2048], P('sp', 'tp'), may hold values from -256 to 256
- latent_rows: bfloat16 [4096, 512], P('sp'), may hold values from -6 to 6
- rope_keys: bfloat16 [4096, 64], P('sp'), may hold values from -4 to 4
- key_up_major: bfloat16 [512, 2048], P(None, 'tp'), may hold values from -0.25 to 0.25
- value_up_major: bfloat16 [512, 2048], P(None, 'tp'), may hold values from -0.25 to 0.25
- key_up_minor: bfloat16 [512, 1024], P(None, 'tp'), may hold values from -0.25 to 0.25
- value_up_minor: bfloat16 [512, 1024], P(None, 'tp'), may hold values from -0.25 to 0.25
- out_major: bfloat16 [2048, 2048], P('tp'), may hold values from -0.625 to 0.625
- out_minor: bfloat16 [1024, 2048], P('tp'), may hold values from -0.625 to 0.625
- residual: bfloat16 [4096, 2048], P('sp', 'tp'), may hold values from -4 to 4
- norm_gain: float32 [2048], replicated, may hold values from 0.1 to 1.9
- expert_ids: int32 [4096, 2], P('sp'), may hold values from 0 to 31, all different within a row; in each aligned block of 128 rows (0 to 127, 128 to 255, ...) at most 16 rows name the same one
- expert_weights: float32 [4096, 2], P('sp'), may hold values from 0.2 to 1
- gate_proj: bfloat16 [32, 2048, 4096], P('sp', None, 'tp'), may hold values from -0.125 to 0.125
- up_proj: bfloat16 [32, 2048, 4096], P('sp', None, 'tp'), may hold values from -0.125 to 0.125
- down_proj: bfloat16 [32, 4096, 2048], P('sp', 'tp'), may hold values from -0.125 to 0.125
Outputs:
- mixed: bfloat16 [4096, 2048], P('sp', 'tp')
The draws below stay inside these ranges and needn't reach their ends.
Inputs may be any that keep to these rules, and one draw needn't show every extreme that they name: `expert_ids`: each row names 2 different experts. In each aligned block of 128 rows (the rows of one index of sp) no expert is named by more than 16 rows, and in some blocks one expert is named by exactly 16 rows.
All inputs are finite; a program needn't handle non-finite values.
Results may differ from the reference program's by a relative error of at most 0.02.
Values may be sent and summed in bfloat16 or wider, within the bound.
No kernel may reach another device: no remote copies, remote signals or barrier semaphores. Data moves between devices by JAX's collectives and lax.ppermute only.
A program may use at most 64 MiB of HBM per device.

```python
import math
import jax
import jax.numpy as jnp
import numpy as np
from jax import lax

D = 2048
HEADS_MAJOR = 16
HEADS_MINOR = 16
NOPE_MAJOR = 128
VAL_MAJOR = 128
NOPE_MINOR = 64
VAL_MINOR = 64
ROPE = 64
LATENT = 512
FF = 4096
TOP = 2
TOK_DEV = 128
TOKENS = 4096
EXPERTS = 32
CAP = 16
N_SP = 32
N_TP = 16


def rope_base(key):
    inner_key = jax.random.fold_in(key, 101)
    values = jnp.clip(jax.random.normal(inner_key, (TOKENS, ROPE), jnp.float32), -4.0, 4.0)
    return values


def draw_rope_keys(key, part):
    values = rope_base(key)
    return values.astype(jnp.bfloat16)


def drawn_query(key, salt, head_count, nope_width):
    inner_key = jax.random.fold_in(key, salt)
    full_shape = (TOKENS, head_count, nope_width + ROPE)
    drawn = jnp.clip(jax.random.normal(inner_key, full_shape, jnp.float32), -4.0, 4.0)
    return drawn.reshape(TOKENS, head_count * (nope_width + ROPE)).astype(jnp.bfloat16)


def draw_query_major(key, part):
    return drawn_query(key, 201, HEADS_MAJOR, NOPE_MAJOR)


def draw_query_minor(key, part):
    return drawn_query(key, 202, HEADS_MINOR, NOPE_MINOR)


def draw_residual(key, part):
    column = jnp.arange(D, dtype=jnp.float32)
    ramp = 0.15 * 6.0 ** (column / D)
    inner_key = jax.random.fold_in(key, 301)
    drawn = jnp.clip(jax.random.normal(inner_key, (TOKENS, D), jnp.float32), -4.0, 4.0)
    return (drawn * ramp[None, :]).astype(jnp.bfloat16)


def with_spikes(entries, rng, source, target, parts, factor):
    owner, partner = [(jnp.arange(entries.shape[position]) // (entries.shape[position] // parts)).reshape([-1 if axis == position else 1 for axis in range(entries.ndim)]) for position in (source, target)]
    chosen = jax.random.permutation(rng, parts)[partner]
    strong = (owner == chosen) | (owner == (partner + parts // 2) % parts)
    return jnp.where(strong, factor * entries, entries)


def block_levels(own_key, dims, cuts, least, top_value):
    def one(axis_at, blocks):
        draws = jax.random.uniform(jax.random.fold_in(jax.random.fold_in(own_key, 6), axis_at), (blocks,), jnp.float32, least / len(cuts), top_value / len(cuts))
        return jnp.repeat(jnp.exp(draws), dims[axis_at] // blocks).reshape((-1,) + (1,) * (len(dims) - axis_at - 1))

    gain = one(*cuts[0])
    for cut in cuts[1:]:
        gain = gain * one(*cut)
    return gain


def shared_out(stream_key, own, number, rows, amount, top, limit, skew):
    order = jax.random.permutation(stream_key, amount)
    crowded, usual = shares(amount, rows * top, limit, skew, True), shares(amount, rows * top, limit, skew, False)
    places = jnp.arange(amount)

    def named(lengths, turn):
        used = int((lengths > 0).sum())
        fixed = max(1, used // 4)
        shifted = fixed + (places - fixed + turn * (used - fixed)) % max(1, amount - fixed)
        return jnp.zeros((amount,), jnp.int32).at[order[jnp.where(places < fixed, places, shifted)]].set(jnp.asarray(lengths, jnp.int32))

    lengths = jnp.where(number % 4 == 0, named(crowded, number // 4), named(usual, number - number // 4 - 1))
    mixed = jax.random.permutation(jax.random.fold_in(own, 3), amount)
    giver, sink = mixed[0:amount // 2 * 2:2], mixed[1:amount // 2 * 2:2]
    slack = jnp.minimum(lengths[giver] - 1, limit - lengths[sink]) // 2
    slack = jnp.where((giver == order[0]) | (sink == order[0]) | (lengths[sink] == 0), 0, jnp.maximum(slack, 0))
    shifted = jax.random.randint(jax.random.fold_in(own, 4), (amount // 2,), 0, 1 << 20) % (slack + 1)
    lengths = lengths.at[giver].add(-shifted).at[sink].add(shifted)
    items = jnp.searchsorted(jnp.cumsum(lengths), jnp.arange(rows * top), side="right").astype(jnp.int32)
    listing = items.reshape(top, rows).T
    listing = listing[jax.random.permutation(jax.random.fold_in(own, 1), rows)]
    turn = jax.random.randint(jax.random.fold_in(own, 2), (rows, 1), 0, top)
    return jnp.take_along_axis(listing, (jnp.arange(top)[None, :] + turn) % top, axis=1)


def shares(amount, total, limit, lean, full):
    portions = [(1 << 20) // math.isqrt(grade ** lean) + 1 for grade in range(1, amount + 1)]
    largest = limit if full else min(limit, max(-(-total // amount), total * portions[0] // sum(portions)))
    least = 1 if total - largest >= amount - 1 else 0
    counts, rest = [largest] + [least] * (amount - 1), total - largest - least * (amount - 1)
    while rest > 0:
        candidates = [i for i in range(1, amount) if counts[i] < largest] or [i for i in range(1, amount) if counts[i] < limit]
        mass, remaining = sum([portions[i] for i in candidates]), rest
        for i in candidates:
            more = min(limit - counts[i], max(1, remaining * portions[i] // mass), rest)
            counts[i] = counts[i] + more
            rest = rest - more
    return np.array(counts)


def bell_draw(rng, shape, deviation, reach, split=(), kind=jnp.bfloat16):
    values = jax.random.normal(rng, shape, jnp.float32) * deviation
    if len(split) > 0:
        values = block_levels(rng, shape, split, -0.22, 0.18) * values
    return jnp.clip(values, min=-reach, max=reach).astype(kind)


def heavy_noise(stream_key, extent, scale, bound, pieces, heavy, kind=jnp.bfloat16):
    values = scale * jax.random.normal(stream_key, extent, jnp.float32)
    if pieces:
        values = values * block_levels(stream_key, extent, pieces, -0.22, 0.18)
    return jnp.clip(with_spikes(values, jax.random.fold_in(stream_key, 3), *heavy), -bound, bound).astype(kind)


def setup_inputs(seed: int = 0) -> dict:
    keys = jax.random.split(jax.random.key(seed), 18)
    query_major = draw_query_major(jax.random.fold_in(keys[17], 71), 0)
    query_minor = draw_query_minor(jax.random.fold_in(keys[17], 71), 0)
    latent_rows = bell_draw(keys[2], (TOKENS, LATENT), 1.0, 6.0, ((0, 32),))
    rope_keys = draw_rope_keys(jax.random.fold_in(keys[17], 71), 0)
    key_up_major = bell_draw(keys[4], (LATENT, HEADS_MAJOR * NOPE_MAJOR), LATENT ** -0.5, 0.25, ((1, 16),))
    value_up_major = bell_draw(keys[5], (LATENT, HEADS_MAJOR * VAL_MAJOR), LATENT ** -0.5, 0.25, ((1, 16),))
    key_up_minor = bell_draw(keys[6], (LATENT, HEADS_MINOR * NOPE_MINOR), LATENT ** -0.5, 0.25, ((1, 16),))
    value_up_minor = bell_draw(keys[7], (LATENT, HEADS_MINOR * VAL_MINOR), LATENT ** -0.5, 0.25, ((1, 16),))
    out_major = heavy_noise(keys[8], (HEADS_MAJOR * VAL_MAJOR, D), ((HEADS_MAJOR * VAL_MAJOR + HEADS_MINOR * VAL_MINOR) // 16) ** -0.5, 0.625, ((0, 16),), (0, 1, 16, 2.0))
    out_minor = heavy_noise(keys[9], (HEADS_MINOR * VAL_MINOR, D), ((HEADS_MAJOR * VAL_MAJOR + HEADS_MINOR * VAL_MINOR) // 16) ** -0.5, 0.625, ((0, 16),), (0, 1, 16, 2.0))
    residual = draw_residual(jax.random.fold_in(keys[17], 71), 0)
    norm_gain = jnp.clip(1.0 + 0.18 * jax.random.normal(keys[11], (D,), jnp.float32), 0.1, 1.9)
    expert_ids_keys = jax.random.split(jax.random.fold_in(keys[12], 1), TOKENS // TOK_DEV)
    expert_ids_turns = jax.random.permutation(jax.random.fold_in(keys[12], 3), TOKENS // TOK_DEV)
    expert_ids = jax.vmap(lambda own, number: shared_out(jax.random.fold_in(keys[12], 2), own, number, TOK_DEV, EXPERTS, TOP, CAP, 1))(expert_ids_keys, expert_ids_turns).reshape((TOKENS, TOP))
    expert_weights = jnp.clip(0.2 + 0.8 * jax.random.uniform(keys[13], (TOKENS, TOP), jnp.float32) ** block_levels(keys[13], (TOKENS, TOP), ((0, 32),), -0.2, 0.2), 0.2, 1.0)
    gate_proj = bell_draw(keys[14], (EXPERTS, D, FF), D ** -0.5, 0.125, ((0, 32), (2, 16)))
    up_proj = bell_draw(keys[15], (EXPERTS, D, FF), D ** -0.5, 0.125, ((0, 32), (2, 16)))
    down_proj = heavy_noise(keys[16], (EXPERTS, FF, D), FF ** -0.5, 0.125, ((0, 32), (1, 16)), (1, 2, 16, 2.0))
    return {"query_major": query_major, "query_minor": query_minor, "latent_rows": latent_rows, "rope_keys": rope_keys, "key_up_major": key_up_major, "value_up_major": value_up_major, "key_up_minor": key_up_minor, "value_up_minor": value_up_minor, "out_major": out_major, "out_minor": out_minor, "residual": residual, "norm_gain": norm_gain, "expert_ids": expert_ids, "expert_weights": expert_weights, "gate_proj": gate_proj, "up_proj": up_proj, "down_proj": down_proj}


theta_base = 10000.0
norm_eps = 1e-06

def rotary(values, positions):
    half_width = values.shape[-1] // 2
    inverse_freq = 1.0 / theta_base ** (jnp.arange(half_width, dtype=jnp.float32) * (2.0 / values.shape[-1]))
    angles = positions.astype(jnp.float32)[:, None] * inverse_freq[None, :]
    view_shape = (angles.shape[0],) + (1,) * (values.ndim - 2) + (half_width,)
    cosine = jnp.cos(angles).reshape(view_shape)
    sine_table = jnp.sin(angles).reshape(view_shape)
    lower_half = values[..., :half_width].astype(jnp.float32)
    upper_half = values[..., half_width:].astype(jnp.float32)
    return jnp.concatenate([lower_half * cosine - upper_half * sine_table, upper_half * cosine + lower_half * sine_table], axis=-1)

def group_attention(query, latent_rows, rope_rot, key_up, value_up, head_count, nope_width, positions):
    tok_count = query.shape[0]
    rope_width = rope_rot.shape[1]
    shaped = query.reshape(tok_count, head_count, nope_width + rope_width)
    q_nope = shaped[:, :, :nope_width]
    q_rope = rotary(shaped[:, :, nope_width:], positions).astype(jnp.bfloat16)
    key_rows = jnp.dot(latent_rows, key_up, preferred_element_type=jnp.float32).astype(jnp.bfloat16).reshape(tok_count, head_count, nope_width)
    value_rows = jnp.dot(latent_rows, value_up, preferred_element_type=jnp.float32).astype(jnp.bfloat16).reshape(tok_count, head_count, -1)
    scale = (nope_width + rope_width) ** (-0.5)
    visible = positions[None, :] <= positions[:, None]

    def one_head(operands):
        head_nope, head_rope, head_keys, head_values = operands
        scores = jnp.dot(head_nope, head_keys.T, preferred_element_type=jnp.float32)
        scores = scores + jnp.dot(head_rope, rope_rot.T, preferred_element_type=jnp.float32)
        scores = jnp.where(visible, scores * scale, -jnp.inf)
        largest = lax.optimization_barrier(jnp.max(scores, axis=1, keepdims=True))
        weights = jnp.exp(scores - largest)
        totals = lax.optimization_barrier(jnp.sum(weights, axis=1, keepdims=True))
        summed = jnp.dot(weights.astype(jnp.bfloat16), head_values, preferred_element_type=jnp.float32)
        return (summed / totals).astype(jnp.bfloat16)
    stacked = lax.map(one_head, (q_nope.transpose(1, 0, 2), q_rope.transpose(1, 0, 2), key_rows.transpose(1, 0, 2), value_rows.transpose(1, 0, 2)))
    return stacked.transpose(1, 0, 2).reshape(tok_count, -1)

def head_projection(attn_major, attn_minor, out_major, out_minor):
    tok_count = attn_major.shape[0]
    width = out_major.shape[1]
    major_sets = attn_major.reshape(tok_count, N_TP, -1).transpose(1, 0, 2)
    minor_sets = attn_minor.reshape(tok_count, N_TP, -1).transpose(1, 0, 2)
    major_weights = out_major.reshape(N_TP, -1, width)
    minor_weights = out_minor.reshape(N_TP, -1, width)

    def add_set(summed, operands):
        set_major, set_minor, weight_major, weight_minor = operands
        partial_value = jnp.dot(set_major, weight_major, preferred_element_type=jnp.float32)
        partial_value = partial_value + jnp.dot(set_minor, weight_minor, preferred_element_type=jnp.float32)
        partial_value = lax.optimization_barrier(partial_value.astype(jnp.bfloat16)).astype(jnp.float32)
        return (summed + partial_value, None)
    summed, unused = lax.scan(add_set, jnp.zeros((tok_count, width), jnp.float32), (major_sets, minor_sets, major_weights, minor_weights))
    return summed

def slot_ids(route_block, experts, capacity):
    pairs = route_block.reshape(-1)
    matches = (pairs[:, None] == jnp.arange(experts, dtype=jnp.int32)[None, :]).astype(jnp.int32)
    ranks = jnp.cumsum(matches, axis=0) - 1
    return pairs * capacity + lax.optimization_barrier(jnp.sum(ranks * matches, axis=1))

def reference(query_major, query_minor, latent_rows, rope_keys, key_up_major, value_up_major, key_up_minor, value_up_minor, out_major, out_minor, residual, norm_gain, expert_ids, expert_weights, gate_proj, up_proj, down_proj):
    positions = jnp.arange(TOKENS, dtype=jnp.int32)
    rope_rot = rotary(rope_keys, positions).astype(jnp.bfloat16)
    attn_major = group_attention(query_major, latent_rows, rope_rot, key_up_major, value_up_major, HEADS_MAJOR, NOPE_MAJOR, positions)
    attn_minor = group_attention(query_minor, latent_rows, rope_rot, key_up_minor, value_up_minor, HEADS_MINOR, NOPE_MINOR, positions)
    head_total = head_projection(attn_major, attn_minor, out_major, out_minor)
    stream_mid = (residual.astype(jnp.float32) + head_total).astype(jnp.bfloat16)
    stream_f = stream_mid.astype(jnp.float32)
    normed = (stream_f * lax.rsqrt(lax.optimization_barrier(jnp.mean(stream_f * stream_f, axis=1, keepdims=True)) + norm_eps) * norm_gain[None, :]).astype(jnp.bfloat16)
    blocks = expert_ids.reshape(N_SP, TOK_DEV, TOP)
    local_slots = jax.vmap(lambda block_ids: slot_ids(block_ids, EXPERTS, CAP))(blocks)
    block_index = jnp.arange(N_SP, dtype=jnp.int32)[:, None]
    global_slots = (local_slots // CAP * (N_SP * CAP) + block_index * CAP + local_slots % CAP).reshape(-1)
    buffer = jnp.zeros((EXPERTS * N_SP * CAP, D), jnp.bfloat16).at[global_slots].set(jnp.repeat(normed, TOP, axis=0))

    def one_expert(operands):
        slot_rows, gate_weight, up_weight, down_weight = operands
        gate_pre = jnp.dot(slot_rows, gate_weight, preferred_element_type=jnp.float32)
        up_pre = jnp.dot(slot_rows, up_weight, preferred_element_type=jnp.float32)
        hidden = (jax.nn.silu(gate_pre) * up_pre).astype(jnp.bfloat16)
        hidden_sets = hidden.reshape(hidden.shape[0], N_TP, -1).transpose(1, 0, 2)
        down_sets = down_weight.reshape(N_TP, -1, D)

        def add_set(summed, operands_set):
            hidden_set, down_set = operands_set
            partial_value = jnp.dot(hidden_set, down_set, preferred_element_type=jnp.float32)
            partial_value = lax.optimization_barrier(partial_value.astype(jnp.bfloat16)).astype(jnp.float32)
            return (summed + partial_value, None)
        summed, unused = lax.scan(add_set, jnp.zeros((hidden.shape[0], D), jnp.float32), (hidden_sets, down_sets))
        return summed.astype(jnp.bfloat16)
    expert_out = lax.map(one_expert, (buffer.reshape(EXPERTS, N_SP * CAP, D), gate_proj, up_proj, down_proj))
    picked = expert_out.reshape(EXPERTS * N_SP * CAP, D)[global_slots].astype(jnp.float32)
    weighted = picked * expert_weights.reshape(-1)[:, None]
    moe_out = lax.optimization_barrier(jnp.sum(weighted.reshape(TOKENS, TOP, D), axis=1))
    return (stream_f + moe_out).astype(jnp.bfloat16)
```

```python
import jax
import jax.numpy as jnp
import numpy as np
from jax import lax
from jax.experimental import pallas as pl
from jax.experimental.pallas import tpu as pltpu
from jax.sharding import PartitionSpec as P

F32 = jnp.float32
BF16 = jnp.bfloat16
D = 2048
ROPE = 64
NOPE_MAJOR = 128
NOPE_MINOR = 64
LATENT = 512
TOK = 128
N_TP = 16
N_Z = 16
EXPERTS = 32
CAP = 16
SLOTS = EXPERTS * CAP
ROWS = TOK // N_TP
KEYS = N_Z * TOK
MASKED = -1e30
NORM_EPS = 1e-6
INV_FREQ = (1.0 / 10000.0 ** (np.arange(32, dtype=np.float64) / 32.0)).astype(np.float32)

SAME_CORE = [[z * 2 + c for z in range(N_Z)] for c in range(2)]
OTHER_CORE = [(i, i ^ 1) for i in range(2 * N_Z)]


def vmem(n):
    return [pl.BlockSpec(memory_space=pltpu.VMEM)] * n


def dot(a, b, dims=((1,), (0,))):
    return lax.dot_general(a, b, (dims, ((), ())), preferred_element_type=F32)


def turned(values, cosine, sine):
    low = values[:, :32].astype(F32)
    high = values[:, 32:].astype(F32)
    return jnp.concatenate(
        [low * cosine - high * sine, high * cosine + low * sine], axis=1
    ).astype(BF16)


def prepare_body(lat, rope, qmaj, qmin, cos_k, sin_k, cos_q, sin_q, rows_out, q_out):
    key = turned(rope[...], cos_k[...], sin_k[...])
    row = jnp.concatenate([lat[...], key, jnp.zeros((ROWS, 64), BF16)], axis=1)
    for z in range(N_Z):
        rows_out[z] = row
    c, s = cos_q[...], sin_q[...]
    maj, low = qmaj[...], qmin[...]
    q_out[...] = jnp.concatenate(
        [
            maj[:, :NOPE_MAJOR],
            turned(maj[:, NOPE_MAJOR:], c, s),
            low[:, :NOPE_MINOR],
            turned(low[:, NOPE_MINOR:], c, s),
        ],
        axis=1,
    )


def spread_body(got, out):
    flat = got[...].reshape(N_Z * ROWS, 640)
    rope = flat[:, 512:576]
    half = jnp.concatenate([rope[:64], rope[64:]], axis=1)
    for t in range(N_TP):
        for k in range(4):
            out[t, 128 * k : 128 * (k + 1), :] = flat[:, 128 * k : 128 * (k + 1)]
        out[t, 512:576, :] = half


CHUNK = 512
N_CHUNK = KEYS // CHUNK


def attend_body(where, keys, q_own, q_other, ku_maj, vu_maj, ku_min, vu_min, own, other, s_maj, s_min, v_all):
    me = where[0]
    core = me % 2
    weights = jnp.concatenate([ku_maj[...], vu_maj[...], ku_min[...], vu_min[...]], axis=1)
    q = jnp.concatenate([q_own[...], q_other[...]], axis=0)
    q_maj, q_min = q[:, :192], q[:, 192:320]
    row = lax.broadcasted_iota(jnp.int32, (2 * TOK, 1), 0)
    q_pos = jnp.where(row < TOK, me * TOK + row, (me + 1 - 2 * core) * TOK + row - TOK)
    scale_maj = (NOPE_MAJOR + ROPE) ** -0.5
    scale_min = (NOPE_MINOR + ROPE) ** -0.5
    top_maj = jnp.full((2 * TOK, 128), MASKED, F32)
    top_min = jnp.full((2 * TOK, 128), MASKED, F32)
    per = CHUNK // 128
    for n in range(N_CHUNK):
        lat_rows, rope_rows = [], []
        for t in range(n * per, (n + 1) * per):
            lat_rows.append(
                jnp.concatenate([keys[t, 128 * k : 128 * (k + 1), :] for k in range(4)], axis=1)
            )
            half = keys[t, 512:576, :]
            rope_rows.append(jnp.concatenate([half[:, :64], half[:, 64:]], axis=0))
        lat = jnp.concatenate(lat_rows, axis=0)
        rope = jnp.concatenate(rope_rows, axis=0)
        up = dot(lat, weights).astype(BF16)
        k_maj = jnp.concatenate([up[:, :128], rope], axis=1)
        k_min = jnp.concatenate([up[:, 256:320], rope], axis=1)
        v_all[CHUNK * n : CHUNK * (n + 1), :] = jnp.concatenate([up[:, 128:256], up[:, 320:384]], axis=1)
        col = lax.broadcasted_iota(jnp.int32, (1, CHUNK), 1) + CHUNK * n
        k_pos = (2 * ((col >> 3) & 15) + core) * TOK + 8 * (col >> 7) + (col & 7)
        seen = k_pos <= q_pos
        a = jnp.where(seen, dot(q_maj, k_maj, ((1,), (1,))) * scale_maj, MASKED)
        b = jnp.where(seen, dot(q_min, k_min, ((1,), (1,))) * scale_min, MASKED)
        s_maj[:, CHUNK * n : CHUNK * (n + 1)] = a
        s_min[:, CHUNK * n : CHUNK * (n + 1)] = b
        for k in range(CHUNK // 128):
            top_maj = jnp.maximum(top_maj, a[:, 128 * k : 128 * (k + 1)])
            top_min = jnp.maximum(top_min, b[:, 128 * k : 128 * (k + 1)])
    m_maj = jnp.max(top_maj, axis=1, keepdims=True)
    m_min = jnp.max(top_min, axis=1, keepdims=True)
    sum_maj = jnp.zeros((2 * TOK, 128), F32)
    sum_min = jnp.zeros((2 * TOK, 128), F32)
    o_maj = jnp.zeros((2 * TOK, 128), F32)
    o_min = jnp.zeros((2 * TOK, 64), F32)
    for n in range(N_CHUNK):
        p = jnp.exp(s_maj[:, CHUNK * n : CHUNK * (n + 1)] - m_maj)
        r = jnp.exp(s_min[:, CHUNK * n : CHUNK * (n + 1)] - m_min)
        for k in range(CHUNK // 128):
            sum_maj = sum_maj + p[:, 128 * k : 128 * (k + 1)]
            sum_min = sum_min + r[:, 128 * k : 128 * (k + 1)]
        v = v_all[CHUNK * n : CHUNK * (n + 1), :]
        o_maj = o_maj + dot(p.astype(BF16), v[:, :128])
        o_min = o_min + dot(r.astype(BF16), v[:, 128:192])
    l_maj = jnp.sum(sum_maj, axis=1, keepdims=True)
    l_min = jnp.sum(sum_min, axis=1, keepdims=True)
    lane = lax.broadcasted_iota(jnp.int32, (2 * TOK, 64), 1)
    stats = jnp.where(
        lane == 0, m_maj, jnp.where(lane == 1, l_maj, jnp.where(lane == 2, m_min, l_min))
    )
    result = jnp.concatenate([o_maj, o_min, stats], axis=1)
    own[...] = result[:TOK]
    other[...] = result[TOK:]


def project_body(a, b, out_maj, out_min, parts):
    a, b = a[...], b[...]

    def joined(m_at, lo, hi):
        m_a, m_b = a[:, m_at : m_at + 1], b[:, m_at : m_at + 1]
        l_a, l_b = a[:, m_at + 1 : m_at + 2], b[:, m_at + 1 : m_at + 2]
        top = jnp.maximum(m_a, m_b)
        f_a, f_b = jnp.exp(m_a - top), jnp.exp(m_b - top)
        total = l_a * f_a + l_b * f_b
        return ((a[:, lo:hi] * f_a + b[:, lo:hi] * f_b) / total).astype(BF16)

    attn_maj = joined(192, 0, 128)
    attn_min = joined(194, 128, 192)
    value = dot(attn_maj, out_maj[...]) + dot(attn_min, out_min[...])
    for t in range(N_TP):
        parts[t] = value[:, 128 * t : 128 * (t + 1)].astype(BF16)


def slot_columns(ids):
    lane = lax.broadcasted_iota(jnp.int32, (TOK, EXPERTS), 1)
    first = (ids[:, 0:1] == lane).astype(F32)
    second = (ids[:, 1:2] == lane).astype(F32)
    below = (
        lax.broadcasted_iota(jnp.int32, (TOK, TOK), 1) < lax.broadcasted_iota(jnp.int32, (TOK, TOK), 0)
    ).astype(BF16)
    earlier = dot(below, (first + second).astype(BF16))
    rank_0 = jnp.sum(first * earlier, axis=1, keepdims=True).astype(jnp.int32)
    rank_1 = jnp.sum(second * earlier, axis=1, keepdims=True).astype(jnp.int32)
    return ids[:, 0:1] * CAP + rank_0, ids[:, 1:2] * CAP + rank_1


def place_body(parts, residual, ids, stream, placed):
    total = residual[...].astype(F32)
    summed = parts[0].astype(F32)
    for t in range(1, N_TP):
        summed = summed + parts[t].astype(F32)
    rows = (total + summed).astype(BF16)
    stream[...] = rows
    slot_0, slot_1 = slot_columns(ids[...])
    lane = lax.broadcasted_iota(jnp.int32, (TOK, SLOTS), 1)
    select = ((lane == slot_0) | (lane == slot_1)).astype(BF16)
    placed[...] = dot(select, rows, ((0,), (0,))).astype(BF16)


def expert_body(got, gain, gate_hbm, up_hbm, down_hbm, parts, x, gate_w, up_w, down_w, sems):
    copies = [
        pltpu.make_async_copy(src, dst, sems.at[i])
        for i, (src, dst) in enumerate(((gate_hbm, gate_w), (up_hbm, up_w), (down_hbm, down_w)))
    ]
    for c in copies:
        c.start()
    squares = jnp.zeros((SLOTS, 128), F32)
    for t in range(N_TP):
        v = got[t].astype(F32)
        squares = squares + v * v
    factor = lax.rsqrt(jnp.sum(squares, axis=1, keepdims=True) / D + NORM_EPS)
    for t in range(N_TP):
        x[:, 128 * t : 128 * (t + 1)] = (
            got[t].astype(F32) * factor * gain[:, 128 * t : 128 * (t + 1)]
        ).astype(BF16)
    copies[0].wait()
    gate = dot(x[...], gate_w[...])
    copies[1].wait()
    up = dot(x[...], up_w[...])
    hidden = (gate / (1.0 + jnp.exp(-gate)) * up).astype(BF16)
    copies[2].wait()
    for t in range(N_TP):
        parts[t] = dot(hidden, down_w[:, 128 * t : 128 * (t + 1)]).astype(BF16)


def mix_body(returned, stream, ids, weights, out):
    slot_0, slot_1 = slot_columns(ids[...])
    lane = lax.broadcasted_iota(jnp.int32, (TOK, SLOTS), 1)
    rows = returned[...]
    w = weights[...]
    first = dot((lane == slot_0).astype(BF16), rows) * w[:, 0:1]
    second = dot((lane == slot_1).astype(BF16), rows) * w[:, 1:2]
    out[...] = (stream[...].astype(F32) + (first + second)).astype(BF16)


def shape(dims, kind=BF16):
    return jax.ShapeDtypeStruct(dims, kind)


def to_each(array, axis, groups=None):
    return lax.all_to_all(array, axis, 0, 0, tiled=True, axis_index_groups=groups)


def per_device(
    query_major,
    query_minor,
    latent_rows,
    rope_keys,
    key_up_major,
    value_up_major,
    key_up_minor,
    value_up_minor,
    out_major,
    out_minor,
    residual,
    norm_gain,
    expert_ids,
    expert_weights,
    gate_proj,
    up_proj,
    down_proj,
):
    block = lax.axis_index("sp").astype(jnp.int32)
    part = lax.axis_index("tp").astype(jnp.int32)
    angles = (block * TOK + jnp.arange(TOK, dtype=jnp.int32)).astype(F32)[:, None] * INV_FREQ[None, :]
    cosine, sine = jnp.cos(angles), jnp.sin(angles)
    mine = part * ROWS

    def my_rows(a):
        return lax.dynamic_slice_in_dim(a, mine, ROWS, 0)

    rows, q_own = pl.pallas_call(
        prepare_body,
        out_shape=(shape((N_Z, ROWS, 640)), shape((TOK, 320))),
        in_specs=vmem(8),
        out_specs=tuple(vmem(2)),
        name="prepare",
    )(
        my_rows(latent_rows),
        my_rows(rope_keys),
        query_major,
        query_minor,
        my_rows(cosine),
        my_rows(sine),
        cosine,
        sine,
    )
    q_other = lax.ppermute(q_own, "sp", OTHER_CORE)
    got_rows = to_each(rows, "sp", SAME_CORE)
    spread = pl.pallas_call(
        spread_body,
        out_shape=shape((N_TP, 576, 128)),
        in_specs=vmem(1),
        out_specs=vmem(1)[0],
        name="spread",
    )(got_rows)
    keys = to_each(spread, "tp")
    own, other = pl.pallas_call(
        attend_body,
        out_shape=(shape((TOK, 256), F32), shape((TOK, 256), F32)),
        in_specs=[pl.BlockSpec(memory_space=pltpu.SMEM)] + vmem(7),
        out_specs=tuple(vmem(2)),
        scratch_shapes=[
            pltpu.VMEM((2 * TOK, KEYS), F32),
            pltpu.VMEM((2 * TOK, KEYS), F32),
            pltpu.VMEM((KEYS, 192), BF16),
        ],
        name="attend",
    )(
        block.reshape(1),
        keys,
        q_own,
        q_other,
        key_up_major,
        value_up_major,
        key_up_minor,
        value_up_minor,
    )
    from_other = lax.ppermute(other, "sp", OTHER_CORE)
    head_parts = pl.pallas_call(
        project_body,
        out_shape=shape((N_TP, TOK, 128)),
        in_specs=vmem(4),
        out_specs=vmem(1)[0],
        name="project",
    )(own, from_other, out_major, out_minor)
    head_parts = to_each(head_parts, "tp")
    stream, placed = pl.pallas_call(
        place_body,
        out_shape=(shape((TOK, 128)), shape((SLOTS, 128))),
        in_specs=vmem(3),
        out_specs=tuple(vmem(2)),
        name="place",
    )(head_parts, residual, expert_ids)
    arrived = to_each(placed.reshape(EXPERTS, CAP, 128), "sp").reshape(SLOTS, 128)
    everyone = to_each(jnp.broadcast_to(arrived, (N_TP, SLOTS, 128)), "tp")
    any_spec = pl.BlockSpec(memory_space=pl.ANY)
    down_parts = pl.pallas_call(
        expert_body,
        out_shape=shape((N_TP, SLOTS, 128)),
        in_specs=vmem(2) + [any_spec] * 3,
        out_specs=vmem(1)[0],
        scratch_shapes=[
            pltpu.VMEM((SLOTS, D), BF16),
            pltpu.VMEM((D, 256), BF16),
            pltpu.VMEM((D, 256), BF16),
            pltpu.VMEM((256, D), BF16),
            pltpu.SemaphoreType.DMA((3,)),
        ],
        name="expert",
    )(everyone, norm_gain.reshape(1, D), gate_proj[0], up_proj[0], down_proj[0])
    down_parts = to_each(down_parts, "tp")
    expert_out = jnp.sum(down_parts.astype(F32), axis=0).astype(BF16)
    returned = to_each(expert_out.reshape(EXPERTS, CAP, 128), "sp").reshape(SLOTS, 128)
    return pl.pallas_call(
        mix_body,
        out_shape=shape((TOK, 128)),
        in_specs=vmem(4),
        out_specs=vmem(1)[0],
        name="mix",
    )(returned, stream, expert_ids, expert_weights)


def solution(mesh):
    in_specs = (
        P("sp", "tp"),
        P("sp", "tp"),
        P("sp", None),
        P("sp", None),
        P(None, "tp"),
        P(None, "tp"),
        P(None, "tp"),
        P(None, "tp"),
        P("tp", None),
        P("tp", None),
        P("sp", "tp"),
        P(),
        P("sp", None),
        P("sp", None),
        P("sp", None, "tp"),
        P("sp", None, "tp"),
        P("sp", "tp", None),
    )
    return jax.shard_map(
        per_device, mesh=mesh, in_specs=in_specs, out_specs=P("sp", "tp"), check_vma=False
    )
```

```python
import jax
import jax.numpy as jnp
import numpy as np
from jax import lax
from jax.experimental import pallas as pl
from jax.experimental.pallas import tpu as pltpu
from jax.sharding import PartitionSpec as P


F32 = jnp.float32
BF16 = jnp.bfloat16
D = 2048
ROPE = 64
NOPE_MAJOR = 128
NOPE_MINOR = 64
LATENT = 512
TOK = 128
N_TP = 16
N_Z = 16
EXPERTS = 32
CAP = 16
SLOTS = EXPERTS * CAP
ROWS = TOK // N_TP
KEYS = N_Z * TOK
MASKED = -1e30
NORM_EPS = 1e-6
HALF = SLOTS // 2


def turns(positions):
    angles = positions[:, None] * (1.0 / 10000.0 ** (np.arange(32) / 32.0))[None, :]
    return np.concatenate([np.cos(angles), np.sin(angles), np.zeros((len(positions), 64))], axis=1)


TABLE = np.concatenate([turns(np.arange(2 * N_Z) * float(TOK)), turns(np.arange(TOK) * 1.0)]).astype(
    np.float32
)

SAME_CORE = [[z * 2 + c for z in range(N_Z)] for c in range(2)]
OTHER_CORE = [(i, i ^ 1) for i in range(2 * N_Z)]
PARTNER = [(s * N_TP + t, s * N_TP + (t ^ (4 if s % 2 else 1))) for s in range(2 * N_Z) for t in range(N_TP)]


ANY = pl.BlockSpec(memory_space=pl.ANY)


def vmem(n):
    return [pl.BlockSpec(memory_space=pltpu.VMEM)] * n


def fetch(pairs, sems):
    copies = [pltpu.make_async_copy(src, dst, sems.at[i]) for i, (src, dst) in enumerate(pairs)]
    for c in copies:
        c.start()
    return copies


def dot(a, b, dims=((1,), (0,))):
    return lax.dot_general(a, b, (dims, ((), ())), preferred_element_type=F32)


def turn_at(table, block, rows):
    first = table[pl.ds(block, 1), :]
    c_0, s_0 = first[:, :32], first[:, 32:64]
    c_1, s_1 = rows[:, :32], rows[:, 32:64]
    return c_0 * c_1 - s_0 * s_1, s_0 * c_1 + c_0 * s_1


def turned(values, cosine, sine):
    low = values[:, :32].astype(F32)
    high = values[:, 32:].astype(F32)
    return jnp.concatenate(
        [low * cosine - high * sine, high * cosine + low * sine], axis=1
    ).astype(BF16)


def rows_body(lat_in, rope_in, table_in, out, lat, rope, table, by_row, sems):
    block, part = lax.axis_index("sp"), lax.axis_index("tp")
    mine = pl.ds(pl.multiple_of(part * ROWS, ROWS), ROWS)
    for c in fetch(((lat_in.at[mine], lat), (rope_in, rope), (table_in, table)), sems):
        c.wait()
    at = pl.ds(pl.multiple_of(2 * N_Z + part * ROWS, ROWS), ROWS)
    cosine, sine = turn_at(table, block, table[at, :])
    by_row[...] = rope[...].astype(F32).T
    key = turned(by_row[pl.ds(pl.multiple_of(part * ROWS, ROWS), ROWS), :], cosine, sine)
    row = jnp.concatenate([lat[...], key, jnp.zeros((ROWS, 64), BF16)], axis=1)
    for z in range(N_Z):
        out[z] = row


def queries_body(maj, low, table, after, ku_maj, vu_maj, ku_min, vu_min, out, weights):
    weights[...] = jnp.concatenate([ku_maj[...], vu_maj[...], ku_min[...], vu_min[...]], axis=1)
    c, s = turn_at(table, lax.axis_index("sp"), table[2 * N_Z :, :])
    out[...] = jnp.concatenate(
        [
            maj[:, :NOPE_MAJOR],
            turned(maj[:, NOPE_MAJOR:], c, s),
            low[:, :NOPE_MINOR],
            turned(low[:, NOPE_MINOR:], c, s),
        ],
        axis=1,
    )


CHUNK = 512
N_CHUNK = KEYS // CHUNK


def attend_body(keys, q_own, q_other, up_weights, own, other, s_maj, s_min, v_all):
    per = CHUNK // 128
    me = lax.axis_index("sp")
    core = me % 2
    weights = up_weights[...]
    q = jnp.concatenate([q_own[...], q_other[...]], axis=0)
    q_maj, q_min = q[:, :192], q[:, 192:320]
    row = lax.broadcasted_iota(jnp.int32, (2 * TOK, 1), 0)
    q_pos = jnp.where(row < TOK, me * TOK + row, (me + 1 - 2 * core) * TOK + row - TOK)
    scale_maj = (NOPE_MAJOR + ROPE) ** -0.5
    scale_min = (NOPE_MINOR + ROPE) ** -0.5
    top_maj = jnp.full((2 * TOK, 128), MASKED, F32)
    top_min = jnp.full((2 * TOK, 128), MASKED, F32)
    for n in range(N_CHUNK):
        lat_rows, rope_rows = [], []
        for t in range(n * per, (n + 1) * per):
            lat_rows.append(
                jnp.concatenate([keys[t, 128 * k : 128 * (k + 1), :] for k in range(4)], axis=1)
            )
            half = keys[t, 512:576, :]
            rope_rows.append(jnp.concatenate([half[:, :64], half[:, 64:]], axis=0))
        lat = jnp.concatenate(lat_rows, axis=0)
        rope = jnp.concatenate(rope_rows, axis=0)
        up = dot(lat, weights).astype(BF16)
        k_maj = jnp.concatenate([up[:, :128], rope], axis=1)
        k_min = jnp.concatenate([up[:, 256:320], rope], axis=1)
        v_all[CHUNK * n : CHUNK * (n + 1), :] = jnp.concatenate([up[:, 128:256], up[:, 320:384]], axis=1)
        col = lax.broadcasted_iota(jnp.int32, (1, CHUNK), 1) + CHUNK * n
        k_pos = (2 * ((col >> 3) & 15) + core) * TOK + 8 * (col >> 7) + (col & 7)
        seen = k_pos <= q_pos
        a = jnp.where(seen, dot(q_maj, k_maj, ((1,), (1,))) * scale_maj, MASKED)
        b = jnp.where(seen, dot(q_min, k_min, ((1,), (1,))) * scale_min, MASKED)
        s_maj[:, CHUNK * n : CHUNK * (n + 1)] = a
        s_min[:, CHUNK * n : CHUNK * (n + 1)] = b
        for k in range(CHUNK // 128):
            top_maj = jnp.maximum(top_maj, a[:, 128 * k : 128 * (k + 1)])
            top_min = jnp.maximum(top_min, b[:, 128 * k : 128 * (k + 1)])
    m_maj = jnp.max(top_maj, axis=1, keepdims=True)
    m_min = jnp.max(top_min, axis=1, keepdims=True)
    sum_maj = jnp.zeros((2 * TOK, 128), F32)
    sum_min = jnp.zeros((2 * TOK, 128), F32)
    o_maj = jnp.zeros((2 * TOK, 128), F32)
    o_min = jnp.zeros((2 * TOK, 64), F32)
    for n in range(N_CHUNK):
        p = jnp.exp(s_maj[:, CHUNK * n : CHUNK * (n + 1)] - m_maj)
        r = jnp.exp(s_min[:, CHUNK * n : CHUNK * (n + 1)] - m_min)
        for k in range(CHUNK // 128):
            sum_maj = sum_maj + p[:, 128 * k : 128 * (k + 1)]
            sum_min = sum_min + r[:, 128 * k : 128 * (k + 1)]
        v = v_all[CHUNK * n : CHUNK * (n + 1), :]
        o_maj = o_maj + dot(p.astype(BF16), v[:, :128])
        o_min = o_min + dot(r.astype(BF16), v[:, 128:192])
    l_maj = jnp.sum(sum_maj, axis=1, keepdims=True)
    l_min = jnp.sum(sum_min, axis=1, keepdims=True)
    lane = lax.broadcasted_iota(jnp.int32, (2 * TOK, 64), 1)
    stats = jnp.where(
        lane == 0, m_maj, jnp.where(lane == 1, l_maj, jnp.where(lane == 2, m_min, l_min))
    )
    result = jnp.concatenate([o_maj, o_min, stats], axis=1)
    own[...] = result[:TOK]
    other[...] = result[TOK:]


def project_body(a, b, out_maj, out_min, parts):
    a, b = a[...], b[...]

    def joined(m_at, lo, hi):
        m_a, m_b = a[:, m_at : m_at + 1], b[:, m_at : m_at + 1]
        l_a, l_b = a[:, m_at + 1 : m_at + 2], b[:, m_at + 1 : m_at + 2]
        top = jnp.maximum(m_a, m_b)
        f_a, f_b = jnp.exp(m_a - top), jnp.exp(m_b - top)
        total = l_a * f_a + l_b * f_b
        return ((a[:, lo:hi] * f_a + b[:, lo:hi] * f_b) / total).astype(BF16)

    attn_maj = joined(192, 0, 128)
    attn_min = joined(194, 128, 192)
    value = dot(attn_maj, out_maj[...]) + dot(attn_min, out_min[...])
    for t in range(N_TP):
        parts[t] = value[:, 128 * t : 128 * (t + 1)].astype(BF16)


def slot_columns(ids):
    lane = lax.broadcasted_iota(jnp.int32, (TOK, EXPERTS), 1)
    first = (ids[:, 0:1] == lane).astype(F32)
    second = (ids[:, 1:2] == lane).astype(F32)
    below = (
        lax.broadcasted_iota(jnp.int32, (TOK, TOK), 1) < lax.broadcasted_iota(jnp.int32, (TOK, TOK), 0)
    ).astype(BF16)
    earlier = dot(below, (first + second).astype(BF16))
    rank_0 = jnp.sum(first * earlier, axis=1, keepdims=True).astype(jnp.int32)
    rank_1 = jnp.sum(second * earlier, axis=1, keepdims=True).astype(jnp.int32)
    return ids[:, 0:1] * CAP + rank_0, ids[:, 1:2] * CAP + rank_1


def place_body(parts, residual, ids, stream, placed):
    slot_0, slot_1 = slot_columns(ids[...])
    lane = lax.broadcasted_iota(jnp.int32, (TOK, SLOTS), 1)
    select = ((lane == slot_0) | (lane == slot_1)).astype(BF16)
    summed = parts[0].astype(F32)
    for t in range(1, N_TP):
        summed = summed + parts[t].astype(F32)
    rows = (residual[...].astype(F32) + summed).astype(BF16)
    stream[...] = rows
    placed[...] = dot(select, rows, ((0,), (0,))).astype(BF16)


def expert_body(
    got, gain, gate_a, up_a, down_a, gate_b, up_b, down_b,
    parts,
    gate_w, up_w, down_w, x, sems,
):
    copies = fetch(
        (
            (gate_a.at[0], gate_w.at[0]),
            (gate_b.at[0], gate_w.at[1]),
            (up_a.at[0], up_w.at[0]),
            (up_b.at[0], up_w.at[1]),
            (down_a.at[0], down_w.at[0]),
            (down_b.at[0], down_w.at[1]),
        ),
        sems,
    )
    squares = jnp.zeros((HALF, 128), F32)
    for t in range(N_TP):
        v = got[t].astype(F32)
        squares = squares + v * v
    factor = lax.rsqrt(jnp.sum(squares, axis=1, keepdims=True) / D + NORM_EPS)
    for t in range(N_TP):
        x[:, 128 * t : 128 * (t + 1)] = (
            got[t].astype(F32) * factor * gain[:, 128 * t : 128 * (t + 1)]
        ).astype(BF16)
    hidden = []
    for i in range(2):
        copies[i].wait()
        copies[2 + i].wait()
        gate = dot(x[...], gate_w[i])
        up = dot(x[...], up_w[i])
        hidden.append((gate / (1.0 + jnp.exp(-gate)) * up).astype(BF16))
    copies[4].wait()
    copies[5].wait()
    for t in range(0, N_TP, 2):
        cols = slice(128 * t, 128 * (t + 2))
        value = dot(hidden[0], down_w[0, :, cols]) + dot(hidden[1], down_w[1, :, cols])
        parts[t] = value[:, :128].astype(BF16)
        parts[t + 1] = value[:, 128:].astype(BF16)


def gather_sum_body(parts, out):
    core = lax.axis_index("sp") % 2
    for half in range(2):
        total = jnp.zeros((HALF, 128), F32)
        for k in range(N_TP // 2):
            by_x = 2 * k + half
            by_y = (k // 4) * 8 + half * 4 + k % 4
            total = total + parts[jnp.where(core == 0, by_x, by_y)].astype(F32)
        out[half * HALF : (half + 1) * HALF, :] = total.astype(BF16)


def mix_body(returned, stream, ids, weights, out):
    slot_0, slot_1 = slot_columns(ids[...])
    lane = lax.broadcasted_iota(jnp.int32, (TOK, SLOTS), 1)
    rows = returned[...]
    w = weights[...]
    first = dot((lane == slot_0).astype(BF16), rows) * w[:, 0:1]
    second = dot((lane == slot_1).astype(BF16), rows) * w[:, 1:2]
    out[...] = (stream[...].astype(F32) + (first + second)).astype(BF16)


def shape(dims, kind=BF16):
    return pltpu.VMEM(dims, kind)


def room(dims, kind=BF16):
    return pltpu.VMEM(dims, kind)


def kernel(body, outs, rooms, sems, operands, near=()):
    single = not isinstance(outs, tuple)
    places = [pltpu.VMEM if i in near else pltpu.HBM for i in range(len(operands))]
    operands = [pltpu.with_memory_space_constraint(x, m) for x, m in zip(operands, places)]
    return pl.pallas_call(
        body,
        out_shape=outs,
        in_specs=[pl.BlockSpec(memory_space=m) for m in places],
        out_specs=vmem(1)[0] if single else tuple(vmem(len(outs))),
        scratch_shapes=rooms + ([pltpu.SemaphoreType.DMA((sems,))] if sems else []),
        compiler_params=pltpu.CompilerParams(vmem_limit_bytes=24 * 2**20),
    )(*operands)


def to_each(array, axis, groups=None):
    return lax.all_to_all(array, axis, 0, 0, tiled=True, axis_index_groups=groups)


def per_device(
    query_major,
    query_minor,
    latent_rows,
    rope_keys,
    key_up_major,
    value_up_major,
    key_up_minor,
    value_up_minor,
    out_major,
    out_minor,
    residual,
    norm_gain,
    expert_ids,
    expert_weights,
    gate_proj,
    up_proj,
    down_proj,
):
    table = jnp.asarray(TABLE)
    rows = kernel(
        rows_body,
        shape((N_Z, ROWS, 640)),
        [room((ROWS, LATENT)), room((ROPE, TOK)), room((160, 128), F32), room((TOK, ROPE), F32)],
        3,
        (latent_rows, rope_keys.T, table),
    )
    flat = to_each(rows, "sp", SAME_CORE).reshape(N_Z * ROWS, 640)
    rope = flat[:, 512:576]
    packed = jnp.concatenate(
        [flat[:, 128 * k : 128 * (k + 1)] for k in range(4)]
        + [jnp.concatenate([rope[:64], rope[64:]], axis=1)],
        axis=0,
    )
    spread = jnp.broadcast_to(packed, (N_TP, 576, 128))
    keys = to_each(spread, "tp")
    q_own, up_weights = kernel(
        queries_body,
        (shape((TOK, 320)), shape((LATENT, 384))),
        [],
        0,
        (
            query_major,
            query_minor,
            table,
            packed,
            key_up_major,
            value_up_major,
            key_up_minor,
            value_up_minor,
        ),
        range(8),
    )
    q_other = lax.ppermute(q_own, "sp", OTHER_CORE)
    gate_b = lax.ppermute(gate_proj, ("sp", "tp"), PARTNER)
    up_b = lax.ppermute(up_proj, ("sp", "tp"), PARTNER)
    down_b = lax.ppermute(down_proj, ("sp", "tp"), PARTNER)
    own, other = kernel(
        attend_body,
        (shape((TOK, 256), F32), shape((TOK, 256), F32)),
        [
            room((2 * TOK, KEYS), F32),
            room((2 * TOK, KEYS), F32),
            room((KEYS, 192)),
        ],
        0,
        (keys, q_own, q_other, up_weights),
        range(4),
    )
    from_other = lax.ppermute(other, "sp", OTHER_CORE)
    head_parts = kernel(
        project_body,
        shape((N_TP, TOK, 128)),
        [],
        0,
        (own, from_other, out_major, out_minor),
        range(4),
    )
    head_parts = to_each(head_parts, "tp")
    stream, placed = kernel(
        place_body,
        (shape((TOK, 128)), shape((SLOTS, 128))),
        [],
        0,
        (head_parts, residual, expert_ids),
        range(3),
    )
    arrived = to_each(placed.reshape(EXPERTS, CAP, 128), "sp").reshape(2, 1, HALF, 128)
    peers = jnp.arange(N_TP, dtype=jnp.int32)
    half_of = jnp.where(lax.axis_index("sp") % 2 == 0, peers % 2, (peers // 4) % 2)
    half_rows = jnp.where(half_of[:, None, None] == 0, arrived[0], arrived[1])
    everyone = to_each(half_rows, "tp")
    down_parts = kernel(
        expert_body,
        shape((N_TP, HALF, 128)),
        [
            room((2, D, 256)),
            room((2, D, 256)),
            room((2, 256, D)),
            room((HALF, D)),
        ],
        6,
        (everyone, norm_gain.reshape(1, D), gate_proj, up_proj, down_proj, gate_b, up_b, down_b),
        (0, 1),
    )
    down_parts = to_each(down_parts, "tp")
    expert_out = kernel(gather_sum_body, shape((SLOTS, 128)), [], 0, (down_parts,), (0,))
    returned = to_each(expert_out.reshape(EXPERTS, CAP, 128), "sp").reshape(SLOTS, 128)
    return kernel(
        mix_body, shape((TOK, 128)), [], 0, (returned, stream, expert_ids, expert_weights), range(4)
    )


def solution(mesh):
    in_specs = (
        P("sp", "tp"),
        P("sp", "tp"),
        P("sp", None),
        P("sp", None),
        P(None, "tp"),
        P(None, "tp"),
        P(None, "tp"),
        P(None, "tp"),
        P("tp", None),
        P("tp", None),
        P("sp", "tp"),
        P(),
        P("sp", None),
        P("sp", None),
        P("sp", None, "tp"),
        P("sp", None, "tp"),
        P("sp", "tp", None),
    )

    return jax.shard_map(
        per_device, mesh=mesh, in_specs=in_specs, out_specs=P("sp", "tp"), check_vma=False
    )
```

```python
import jax
import jax.numpy as jnp
import numpy as np
from jax import lax
from jax.experimental import pallas as pl
from jax.experimental.pallas import tpu as pltpu
from jax.sharding import PartitionSpec as P


F32 = jnp.float32
BF16 = jnp.bfloat16
D = 2048
ROPE = 64
NOPE_MAJOR = 128
NOPE_MINOR = 64
LATENT = 512
TOK = 128
N_TP = 16
N_Z = 16
EXPERTS = 32
CAP = 16
SLOTS = EXPERTS * CAP
ROWS = TOK // N_TP
KEYS = N_Z * TOK
MASKED = -1e30
NORM_EPS = 1e-6
HALF = SLOTS // 2


def turns(positions):
    angles = positions[:, None] * (1.0 / 10000.0 ** (np.arange(32) / 32.0))[None, :]
    return np.concatenate([np.cos(angles), np.sin(angles), np.zeros((len(positions), 64))], axis=1)


TABLE = np.concatenate([turns(np.arange(2 * N_Z) * float(TOK)), turns(np.arange(TOK) * 1.0)]).astype(
    np.float32
)

SAME_CORE = [[z * 2 + c for z in range(N_Z)] for c in range(2)]
OTHER_CORE = [(i, i ^ 1) for i in range(2 * N_Z)]


def ring(step):
    moves = []
    for s in range(2 * N_Z):
        for t in range(N_TP):
            y, x = divmod(t, 4)
            to = (y + step) % 4 * 4 + x if s % 2 else y * 4 + (x + step) % 4
            moves.append((s * N_TP + t, s * N_TP + to))
    return moves


HALF = SLOTS // 2


def turns(positions):
    angles = positions[:, None] * (1.0 / 10000.0 ** (np.arange(32) / 32.0))[None, :]
    return np.concatenate([np.cos(angles), np.sin(angles), np.zeros((len(positions), 64))], axis=1)


TABLE = np.concatenate([turns(np.arange(2 * N_Z) * float(TOK)), turns(np.arange(TOK) * 1.0)]).astype(
    np.float32
)

SAME_CORE = [[z * 2 + c for z in range(N_Z)] for c in range(2)]
OTHER_CORE = [(i, i ^ 1) for i in range(2 * N_Z)]


ANY = pl.BlockSpec(memory_space=pl.ANY)


def vmem(n):
    return [pl.BlockSpec(memory_space=pltpu.VMEM)] * n


def fetch(pairs, sems):
    copies = [pltpu.make_async_copy(src, dst, sems.at[i]) for i, (src, dst) in enumerate(pairs)]
    for c in copies:
        c.start()
    return copies


def dot(a, b, dims=((1,), (0,))):
    return lax.dot_general(a, b, (dims, ((), ())), preferred_element_type=F32)


def turn_at(table, block, rows):
    first = table[pl.ds(block, 1), :]
    c_0, s_0 = first[:, :32], first[:, 32:64]
    c_1, s_1 = rows[:, :32], rows[:, 32:64]
    return c_0 * c_1 - s_0 * s_1, s_0 * c_1 + c_0 * s_1


def turned(values, cosine, sine):
    low = values[:, :32].astype(F32)
    high = values[:, 32:].astype(F32)
    return jnp.concatenate(
        [low * cosine - high * sine, high * cosine + low * sine], axis=1
    ).astype(BF16)


def rows_body(lat_in, rope_in, table_in, out, lat, rope, table, by_row, sems):
    block, part = lax.axis_index("sp"), lax.axis_index("tp")
    mine = pl.ds(pl.multiple_of(part * ROWS, ROWS), ROWS)
    for c in fetch(((lat_in.at[mine], lat), (rope_in, rope), (table_in, table)), sems):
        c.wait()
    at = pl.ds(pl.multiple_of(2 * N_Z + part * ROWS, ROWS), ROWS)
    cosine, sine = turn_at(table, block, table[at, :])
    by_row[...] = rope[...].astype(F32).T
    key = turned(by_row[pl.ds(pl.multiple_of(part * ROWS, ROWS), ROWS), :], cosine, sine)
    row = jnp.concatenate([lat[...], key, jnp.zeros((ROWS, 64), BF16)], axis=1)
    for z in range(N_Z):
        out[z] = row


def queries_body(maj, low, table, after, ku_maj, vu_maj, ku_min, vu_min, out, weights):
    weights[...] = jnp.concatenate([ku_maj[...], vu_maj[...], ku_min[...], vu_min[...]], axis=1)
    c, s = turn_at(table, lax.axis_index("sp"), table[2 * N_Z :, :])
    out[...] = jnp.concatenate(
        [
            maj[:, :NOPE_MAJOR],
            turned(maj[:, NOPE_MAJOR:], c, s),
            low[:, :NOPE_MINOR],
            turned(low[:, NOPE_MINOR:], c, s),
        ],
        axis=1,
    )


CHUNK = 512
N_CHUNK = KEYS // CHUNK


def attend_body(
    keys, q_own_in, q_other_in, up_in, own, other, s_maj, s_min, v_all, q_all, up_weights, sems
):
    copies = fetch(
        ((up_in, up_weights), (q_own_in, q_all.at[pl.ds(0, TOK)]), (q_other_in, q_all.at[pl.ds(TOK, TOK)])),
        sems,
    )
    per = CHUNK // 128
    copies[0].wait()
    weights = up_weights[...]
    me = lax.axis_index("sp")
    core = me % 2
    row = lax.broadcasted_iota(jnp.int32, (2 * TOK, 1), 0)
    q_pos = jnp.where(row < TOK, me * TOK + row, (me + 1 - 2 * core) * TOK + row - TOK)
    scale_maj = (NOPE_MAJOR + ROPE) ** -0.5
    scale_min = (NOPE_MINOR + ROPE) ** -0.5
    top_maj = jnp.full((2 * TOK, 128), MASKED, F32)
    top_min = jnp.full((2 * TOK, 128), MASKED, F32)
    for n in range(N_CHUNK):
        lat_rows, rope_rows = [], []
        for t in range(n * per, (n + 1) * per):
            lat_rows.append(
                jnp.concatenate([keys[t, 128 * k : 128 * (k + 1), :] for k in range(4)], axis=1)
            )
            half = keys[t, 512:576, :]
            rope_rows.append(jnp.concatenate([half[:, :64], half[:, 64:]], axis=0))
        lat = jnp.concatenate(lat_rows, axis=0)
        rope = jnp.concatenate(rope_rows, axis=0)
        up = dot(lat, weights).astype(BF16)
        if n == 0:
            copies[1].wait()
            copies[2].wait()
            q_maj, q_min = q_all[:, :192], q_all[:, 192:320]
        k_maj = jnp.concatenate([up[:, :128], rope], axis=1)
        k_min = jnp.concatenate([up[:, 256:320], rope], axis=1)
        v_all[CHUNK * n : CHUNK * (n + 1), :] = jnp.concatenate([up[:, 128:256], up[:, 320:384]], axis=1)
        col = lax.broadcasted_iota(jnp.int32, (1, CHUNK), 1) + CHUNK * n
        k_pos = (2 * ((col >> 3) & 15) + core) * TOK + 8 * (col >> 7) + (col & 7)
        seen = k_pos <= q_pos
        a = jnp.where(seen, dot(q_maj, k_maj, ((1,), (1,))) * scale_maj, MASKED)
        b = jnp.where(seen, dot(q_min, k_min, ((1,), (1,))) * scale_min, MASKED)
        s_maj[:, CHUNK * n : CHUNK * (n + 1)] = a
        s_min[:, CHUNK * n : CHUNK * (n + 1)] = b
        for k in range(CHUNK // 128):
            top_maj = jnp.maximum(top_maj, a[:, 128 * k : 128 * (k + 1)])
            top_min = jnp.maximum(top_min, b[:, 128 * k : 128 * (k + 1)])
    m_maj = jnp.max(top_maj, axis=1, keepdims=True)
    m_min = jnp.max(top_min, axis=1, keepdims=True)
    sum_maj = jnp.zeros((2 * TOK, 128), F32)
    sum_min = jnp.zeros((2 * TOK, 128), F32)
    o_maj = jnp.zeros((2 * TOK, 128), F32)
    o_min = jnp.zeros((2 * TOK, 64), F32)
    for n in range(N_CHUNK):
        p = jnp.exp(s_maj[:, CHUNK * n : CHUNK * (n + 1)] - m_maj)
        r = jnp.exp(s_min[:, CHUNK * n : CHUNK * (n + 1)] - m_min)
        for k in range(CHUNK // 128):
            sum_maj = sum_maj + p[:, 128 * k : 128 * (k + 1)]
            sum_min = sum_min + r[:, 128 * k : 128 * (k + 1)]
        v = v_all[CHUNK * n : CHUNK * (n + 1), :]
        o_maj = o_maj + dot(p.astype(BF16), v[:, :128])
        o_min = o_min + dot(r.astype(BF16), v[:, 128:192])
    l_maj = jnp.sum(sum_maj, axis=1, keepdims=True)
    l_min = jnp.sum(sum_min, axis=1, keepdims=True)
    lane = lax.broadcasted_iota(jnp.int32, (2 * TOK, 64), 1)
    stats = jnp.where(
        lane == 0, m_maj, jnp.where(lane == 1, l_maj, jnp.where(lane == 2, m_min, l_min))
    )
    result = jnp.concatenate([o_maj, o_min, stats], axis=1)
    own[...] = result[:TOK]
    other[...] = result[TOK:]


def project_body(a, b, out_maj, out_min, parts):
    a, b = a[...], b[...]

    def joined(m_at, lo, hi):
        m_a, m_b = a[:, m_at : m_at + 1], b[:, m_at : m_at + 1]
        l_a, l_b = a[:, m_at + 1 : m_at + 2], b[:, m_at + 1 : m_at + 2]
        top = jnp.maximum(m_a, m_b)
        f_a, f_b = jnp.exp(m_a - top), jnp.exp(m_b - top)
        total = l_a * f_a + l_b * f_b
        return ((a[:, lo:hi] * f_a + b[:, lo:hi] * f_b) / total).astype(BF16)

    attn_maj = joined(192, 0, 128)
    attn_min = joined(194, 128, 192)
    value = dot(attn_maj, out_maj[...]) + dot(attn_min, out_min[...])
    for t in range(N_TP):
        parts[t] = value[:, 128 * t : 128 * (t + 1)].astype(BF16)


def slot_columns(ids):
    lane = lax.broadcasted_iota(jnp.int32, (TOK, EXPERTS), 1)
    first = (ids[:, 0:1] == lane).astype(F32)
    second = (ids[:, 1:2] == lane).astype(F32)
    below = (
        lax.broadcasted_iota(jnp.int32, (TOK, TOK), 1) < lax.broadcasted_iota(jnp.int32, (TOK, TOK), 0)
    ).astype(BF16)
    earlier = dot(below, (first + second).astype(BF16))
    rank_0 = jnp.sum(first * earlier, axis=1, keepdims=True).astype(jnp.int32)
    rank_1 = jnp.sum(second * earlier, axis=1, keepdims=True).astype(jnp.int32)
    return ids[:, 0:1] * CAP + rank_0, ids[:, 1:2] * CAP + rank_1


def place_body(parts, residual, ids, stream, placed):
    slot_0, slot_1 = slot_columns(ids[...])
    lane = lax.broadcasted_iota(jnp.int32, (TOK, SLOTS), 1)
    select = ((lane == slot_0) | (lane == slot_1)).astype(BF16)
    summed = parts[0].astype(F32)
    for t in range(1, N_TP):
        summed = summed + parts[t].astype(F32)
    rows = (residual[...].astype(F32) + summed).astype(BF16)
    stream[...] = rows
    placed[...] = dot(select, rows, ((0,), (0,))).astype(BF16)


def pack_body(gate, up, down, low, high, sems):
    pairs = []
    for i, out in enumerate((low, high)):
        mine = pl.ds(128 * i, 128)
        pairs.append((gate.at[0, :, mine], out.at[pl.ds(0, D)]))
        pairs.append((up.at[0, :, mine], out.at[pl.ds(D, D)]))
        for t in range(N_TP):
            pairs.append((down.at[0, mine, pl.ds(128 * t, 128)], out.at[pl.ds(2 * D + 128 * t, 128)]))
    for c in fetch(pairs, sems):
        c.wait()


def expert_body(
    got, gain, gate_a, up_a, down_a, low, high,
    parts,
    gate_w, up_w, down_w, x, sems,
):
    pairs = [(gate_a.at[0], gate_w.at[0]), (up_a.at[0], up_w.at[0])]
    for i, packed in enumerate((low, high)):
        mine = pl.ds(128 * i, 128)
        pairs.append((packed.at[pl.ds(0, D)], gate_w.at[1, :, mine]))
        pairs.append((packed.at[pl.ds(D, D)], up_w.at[1, :, mine]))
    pairs.append((down_a.at[0], down_w.at[0]))
    for i, packed in enumerate((low, high)):
        for t in range(N_TP):
            pairs.append(
                (
                    packed.at[pl.ds(2 * D + 128 * t, 128)],
                    down_w.at[1, pl.ds(128 * i, 128), pl.ds(128 * t, 128)],
                )
            )
    copies = fetch(pairs, sems)
    squares = jnp.zeros((HALF, 128), F32)
    for t in range(N_TP):
        v = got[t].astype(F32)
        squares = squares + v * v
    factor = lax.rsqrt(jnp.sum(squares, axis=1, keepdims=True) / D + NORM_EPS)
    for t in range(N_TP):
        x[:, 128 * t : 128 * (t + 1)] = (
            got[t].astype(F32) * factor * gain[:, 128 * t : 128 * (t + 1)]
        ).astype(BF16)
    hidden = []
    for i in range(2):
        for c in copies[2 * i : 2 + 4 * i]:
            c.wait()
        gate = dot(x[...], gate_w[i])
        up = dot(x[...], up_w[i])
        hidden.append((gate / (1.0 + jnp.exp(-gate)) * up).astype(BF16))
    for c in copies[6:]:
        c.wait()
    for t in range(0, N_TP, 2):
        cols = slice(128 * t, 128 * (t + 2))
        value = dot(hidden[0], down_w[0, :, cols]) + dot(hidden[1], down_w[1, :, cols])
        parts[t] = value[:, :128].astype(BF16)
        parts[t + 1] = value[:, 128:].astype(BF16)


def gather_sum_body(parts, out):
    core = lax.axis_index("sp") % 2
    for half in range(2):
        total = jnp.zeros((HALF, 128), F32)
        for k in range(N_TP // 2):
            by_x = 2 * k + half
            by_y = (k // 4) * 8 + half * 4 + k % 4
            total = total + parts[jnp.where(core == 0, by_x, by_y)].astype(F32)
        out[half * HALF : (half + 1) * HALF, :] = total.astype(BF16)


def mix_body(returned, stream, ids, weights, out):
    slot_0, slot_1 = slot_columns(ids[...])
    lane = lax.broadcasted_iota(jnp.int32, (TOK, SLOTS), 1)
    rows = returned[...]
    w = weights[...]
    first = dot((lane == slot_0).astype(BF16), rows) * w[:, 0:1]
    second = dot((lane == slot_1).astype(BF16), rows) * w[:, 1:2]
    out[...] = (stream[...].astype(F32) + (first + second)).astype(BF16)


def shape(dims, kind=BF16):
    return pltpu.VMEM(dims, kind)


def room(dims, kind=BF16):
    return pltpu.VMEM(dims, kind)


def kernel(body, outs, rooms, sems, operands, near=()):
    single = not isinstance(outs, tuple)
    places = [pltpu.VMEM if i in near else pltpu.HBM for i in range(len(operands))]
    operands = [pltpu.with_memory_space_constraint(x, m) for x, m in zip(operands, places)]
    return pl.pallas_call(
        body,
        out_shape=outs,
        in_specs=[pl.BlockSpec(memory_space=m) for m in places],
        out_specs=vmem(1)[0] if single else tuple(vmem(len(outs))),
        scratch_shapes=rooms + ([pltpu.SemaphoreType.DMA((sems,))] if sems else []),
        compiler_params=pltpu.CompilerParams(vmem_limit_bytes=24 * 2**20),
    )(*operands)


def to_each(array, axis, groups=None):
    return lax.all_to_all(array, axis, 0, 0, tiled=True, axis_index_groups=groups)


def per_device(
    query_major,
    query_minor,
    latent_rows,
    rope_keys,
    key_up_major,
    value_up_major,
    key_up_minor,
    value_up_minor,
    out_major,
    out_minor,
    residual,
    norm_gain,
    expert_ids,
    expert_weights,
    gate_proj,
    up_proj,
    down_proj,
):
    table = jnp.asarray(TABLE)
    rows = kernel(
        rows_body,
        shape((N_Z, ROWS, 640)),
        [room((ROWS, LATENT)), room((ROPE, TOK)), room((160, 128), F32), room((TOK, ROPE), F32)],
        3,
        (latent_rows, rope_keys.T, table),
    )
    got_rows = to_each(rows, "sp", SAME_CORE)
    low, high = kernel(
        pack_body,
        (shape((3 * D, 128)), shape((3 * D, 128))),
        [],
        4 + 2 * N_TP,
        (gate_proj, up_proj, down_proj),
    )
    flat = got_rows.reshape(N_Z * ROWS, 640)
    rope = flat[:, 512:576]
    packed = jnp.concatenate(
        [flat[:, 128 * k : 128 * (k + 1)] for k in range(4)]
        + [jnp.concatenate([rope[:64], rope[64:]], axis=1)],
        axis=0,
    )
    spread = jnp.broadcast_to(packed, (N_TP, 576, 128))
    keys = to_each(spread, "tp")
    q_own, up_weights = kernel(
        queries_body,
        (shape((TOK, 320)), shape((LATENT, 384))),
        [],
        0,
        (
            query_major,
            query_minor,
            table,
            packed,
            key_up_major,
            value_up_major,
            key_up_minor,
            value_up_minor,
        ),
        range(8),
    )
    q_other = lax.ppermute(q_own, "sp", OTHER_CORE)
    from_low = lax.ppermute(low, ("sp", "tp"), ring(1))
    from_high = lax.ppermute(high, ("sp", "tp"), ring(-1))
    own, other = kernel(
        attend_body,
        (shape((TOK, 256), F32), shape((TOK, 256), F32)),
        [
            room((2 * TOK, KEYS), F32),
            room((2 * TOK, KEYS), F32),
            room((KEYS, 192)),
            room((2 * TOK, 320)),
            room((LATENT, 384)),
        ],
        3,
        (keys, q_own, q_other, up_weights),
        (0,),
    )
    from_other = lax.ppermute(other, "sp", OTHER_CORE)
    head_parts = kernel(
        project_body,
        shape((N_TP, TOK, 128)),
        [],
        0,
        (own, from_other, out_major, out_minor),
        range(4),
    )
    head_parts = to_each(head_parts, "tp")
    stream, placed = kernel(
        place_body,
        (shape((TOK, 128)), shape((SLOTS, 128))),
        [],
        0,
        (head_parts, residual, expert_ids),
        range(3),
    )
    arrived = to_each(placed.reshape(EXPERTS, CAP, 128), "sp").reshape(2, 1, HALF, 128)
    peers = jnp.arange(N_TP, dtype=jnp.int32)
    half_of = jnp.where(lax.axis_index("sp") % 2 == 0, peers % 2, (peers // 4) % 2)
    half_rows = jnp.where(half_of[:, None, None] == 0, arrived[0], arrived[1])
    everyone = to_each(half_rows, "tp")
    down_parts = kernel(
        expert_body,
        shape((N_TP, HALF, 128)),
        [
            room((2, D, 256)),
            room((2, D, 256)),
            room((2, 256, D)),
            room((HALF, D)),
        ],
        7 + 2 * N_TP,
        (everyone, norm_gain.reshape(1, D), gate_proj, up_proj, down_proj, from_low, from_high),
        (0, 1),
    )
    down_parts = to_each(down_parts, "tp")
    expert_out = kernel(gather_sum_body, shape((SLOTS, 128)), [], 0, (down_parts,), (0,))
    returned = to_each(expert_out.reshape(EXPERTS, CAP, 128), "sp").reshape(SLOTS, 128)
    return kernel(
        mix_body, shape((TOK, 128)), [], 0, (returned, stream, expert_ids, expert_weights), range(4)
    )


def solution(mesh):
    in_specs = (
        P("sp", "tp"),
        P("sp", "tp"),
        P("sp", None),
        P("sp", None),
        P(None, "tp"),
        P(None, "tp"),
        P(None, "tp"),
        P(None, "tp"),
        P("tp", None),
        P("tp", None),
        P("sp", "tp"),
        P(),
        P("sp", None),
        P("sp", None),
        P("sp", None, "tp"),
        P("sp", None, "tp"),
        P("sp", "tp", None),
    )

    return jax.shard_map(
        per_device, mesh=mesh, in_specs=in_specs, out_specs=P("sp", "tp"), check_vma=False
    )
```

```python
import jax
import jax.numpy as jnp
import numpy as np
from jax import lax
from jax.experimental import pallas as pl
from jax.experimental.pallas import tpu as pltpu
from jax.sharding import PartitionSpec as P


F32 = jnp.float32
BF16 = jnp.bfloat16
D = 2048
ROPE = 64
NOPE_MAJOR = 128
NOPE_MINOR = 64
LATENT = 512
TOK = 128
N_TP = 16
N_Z = 16
EXPERTS = 32
CAP = 16
SLOTS = EXPERTS * CAP
ROWS = TOK // N_TP
KEYS = N_Z * TOK
MASKED = -1e30
NORM_EPS = 1e-6
HALF = SLOTS // 2
NEAR = (-2, -1, 0, 1)
FAR = N_Z - len(NEAR)
FAR_ROWS = FAR * ROWS
PACKED = 4 * FAR_ROWS + FAR_ROWS // 2


def along_z(step):
    return [(z * 2 + c, (z + step) % N_Z * 2 + c) for z in range(N_Z) for c in range(2)]


def turns(positions):
    angles = positions[:, None] * (1.0 / 10000.0 ** (np.arange(32) / 32.0))[None, :]
    return np.concatenate([np.cos(angles), np.sin(angles), np.zeros((len(positions), 64))], axis=1)


TABLE = np.concatenate([turns(np.arange(2 * N_Z) * float(TOK)), turns(np.arange(TOK) * 1.0)]).astype(
    np.float32
)

SAME_CORE = [[z * 2 + c for z in range(N_Z)] for c in range(2)]
OTHER_CORE = [(i, i ^ 1) for i in range(2 * N_Z)]


def ring(step):
    moves = []
    for s in range(2 * N_Z):
        for t in range(N_TP):
            y, x = divmod(t, 4)
            to = (y + step) % 4 * 4 + x if s % 2 else y * 4 + (x + step) % 4
            moves.append((s * N_TP + t, s * N_TP + to))
    return moves


HALF = SLOTS // 2
NEAR = (-2, -1, 0, 1)
FAR = N_Z - len(NEAR)
FAR_ROWS = FAR * ROWS
PACKED = 4 * FAR_ROWS + FAR_ROWS // 2


def along_z(step):
    return [(z * 2 + c, (z + step) % N_Z * 2 + c) for z in range(N_Z) for c in range(2)]


def turns(positions):
    angles = positions[:, None] * (1.0 / 10000.0 ** (np.arange(32) / 32.0))[None, :]
    return np.concatenate([np.cos(angles), np.sin(angles), np.zeros((len(positions), 64))], axis=1)


TABLE = np.concatenate([turns(np.arange(2 * N_Z) * float(TOK)), turns(np.arange(TOK) * 1.0)]).astype(
    np.float32
)

SAME_CORE = [[z * 2 + c for z in range(N_Z)] for c in range(2)]
OTHER_CORE = [(i, i ^ 1) for i in range(2 * N_Z)]


ANY = pl.BlockSpec(memory_space=pl.ANY)


def vmem(n):
    return [pl.BlockSpec(memory_space=pltpu.VMEM)] * n


def fetch(pairs, sems):
    copies = [pltpu.make_async_copy(src, dst, sems.at[i]) for i, (src, dst) in enumerate(pairs)]
    for c in copies:
        c.start()
    return copies


def dot(a, b, dims=((1,), (0,))):
    return lax.dot_general(a, b, (dims, ((), ())), preferred_element_type=F32)


def turn_at(table, block, rows):
    first = table[pl.ds(block, 1), :]
    c_0, s_0 = first[:, :32], first[:, 32:64]
    c_1, s_1 = rows[:, :32], rows[:, 32:64]
    return c_0 * c_1 - s_0 * s_1, s_0 * c_1 + c_0 * s_1


def turned(values, cosine, sine):
    low = values[:, :32].astype(F32)
    high = values[:, 32:].astype(F32)
    return jnp.concatenate(
        [low * cosine - high * sine, high * cosine + low * sine], axis=1
    ).astype(BF16)


def rows_body(lat_in, rope_in, table_in, out, lat, rope, table, by_row, sems):
    block, part = lax.axis_index("sp"), lax.axis_index("tp")
    mine = pl.ds(pl.multiple_of(part * ROWS, ROWS), ROWS)
    for c in fetch(((lat_in.at[mine], lat), (rope_in, rope), (table_in, table)), sems):
        c.wait()
    at = pl.ds(pl.multiple_of(2 * N_Z + part * ROWS, ROWS), ROWS)
    cosine, sine = turn_at(table, block, table[at, :])
    by_row[...] = rope[...].astype(F32).T
    key = turned(by_row[pl.ds(pl.multiple_of(part * ROWS, ROWS), ROWS), :], cosine, sine)
    row = jnp.concatenate([lat[...], key, jnp.zeros((ROWS, 64), BF16)], axis=1)
    for z in range(N_Z):
        out[z] = row


def queries_body(maj, low, table, after, ku_maj, vu_maj, ku_min, vu_min, lat, rope, out, weights, block):
    weights[...] = jnp.concatenate([ku_maj[...], vu_maj[...], ku_min[...], vu_min[...]], axis=1)
    c, s = turn_at(table, lax.axis_index("sp"), table[2 * N_Z :, :])
    key = turned(rope[...].astype(F32).T, c, s)
    block[...] = jnp.concatenate([lat[...], key, jnp.zeros((TOK, 64), BF16)], axis=1)
    out[...] = jnp.concatenate(
        [
            maj[:, :NOPE_MAJOR],
            turned(maj[:, NOPE_MAJOR:], c, s),
            low[:, :NOPE_MINOR],
            turned(low[:, NOPE_MINOR:], c, s),
        ],
        axis=1,
    )


def choose_body(got, out, flat):
    z = lax.axis_index("sp") // 2
    for o in range(FAR):
        flat[ROWS * o : ROWS * (o + 1), :] = got[(z + NEAR[-1] + 1 + o) % N_Z]
    for k in range(4):
        out[FAR_ROWS * k : FAR_ROWS * (k + 1), :] = flat[:, 128 * k : 128 * (k + 1)]
    rope = flat[:, 512:576]
    out[4 * FAR_ROWS :, :] = jnp.concatenate([rope[: FAR_ROWS // 2], rope[FAR_ROWS // 2 :]], axis=1)


PER = 4
CHUNK = PER * FAR_ROWS
N_CHUNK = N_TP // PER


def attend_body(keys, q_own_in, q_other_in, up_in, *refs):
    near_in = refs[: len(NEAR)]
    own, other, s_maj, s_min, v_all, q_all, up_weights, near, sems = refs[len(NEAR) :]
    copies = fetch(
        (
            (up_in, up_weights),
            (q_own_in, q_all.at[pl.ds(0, TOK)]),
            (q_other_in, q_all.at[pl.ds(TOK, TOK)]),
        )
        + tuple((b, near.at[pl.ds(TOK * i, TOK)]) for i, b in enumerate(near_in)),
        sems,
    )
    me = lax.axis_index("sp")
    core, z = me % 2, me // 2
    row = lax.broadcasted_iota(jnp.int32, (2 * TOK, 1), 0)
    q_pos = jnp.where(row < TOK, me * TOK + row, (me + 1 - 2 * core) * TOK + row - TOK)
    scale_maj = (NOPE_MAJOR + ROPE) ** -0.5
    scale_min = (NOPE_MINOR + ROPE) ** -0.5
    tops = [jnp.full((2 * TOK, 128), MASKED, F32)] * 2
    for c in copies:
        c.wait()
    weights = up_weights[...]
    q_maj, q_min = q_all[:, :192], q_all[:, 192:320]

    def scored(at, width, lat, rope, k_pos, tops):
        up = dot(lat, weights).astype(BF16)
        k_maj = jnp.concatenate([up[:, :128], rope], axis=1)
        k_min = jnp.concatenate([up[:, 256:320], rope], axis=1)
        v_all[at : at + width, :] = jnp.concatenate([up[:, 128:256], up[:, 320:384]], axis=1)
        seen = k_pos <= q_pos
        found = []
        for q, k, scale, store, top in (
            (q_maj, k_maj, scale_maj, s_maj, tops[0]),
            (q_min, k_min, scale_min, s_min, tops[1]),
        ):
            s = jnp.where(seen, dot(q, k, ((1,), (1,))) * scale, MASKED)
            store[:, at : at + width] = s
            for i in range(width // 128):
                top = jnp.maximum(top, s[:, 128 * i : 128 * (i + 1)])
            found.append(top)
        return found

    col = lax.broadcasted_iota(jnp.int32, (1, len(NEAR) * TOK), 1)
    k_pos = (2 * ((z + NEAR[0] + N_Z + col // TOK) % N_Z) + core) * TOK + col % TOK
    tops = scored(0, len(NEAR) * TOK, near[:, :512], near[:, 512:576], k_pos, tops)
    first = len(NEAR) * TOK
    col = lax.broadcasted_iota(jnp.int32, (1, CHUNK), 1)
    for n in range(N_CHUNK):
        lat_rows, rope_rows = [], []
        for t in range(n * PER, (n + 1) * PER):
            lat_rows.append(
                jnp.concatenate(
                    [keys[t, FAR_ROWS * k : FAR_ROWS * (k + 1), :] for k in range(4)], axis=1
                )
            )
            half = keys[t, 4 * FAR_ROWS :, :]
            rope_rows.append(jnp.concatenate([half[:, :64], half[:, 64:]], axis=0))
        lat = jnp.concatenate(lat_rows, axis=0)
        rope = jnp.concatenate(rope_rows, axis=0)
        inner = col % FAR_ROWS
        k_z = (z + NEAR[-1] + 1 + inner // ROWS) % N_Z
        k_pos = (2 * k_z + core) * TOK + ROWS * (n * PER + col // FAR_ROWS) + inner % ROWS
        tops = scored(first + CHUNK * n, CHUNK, lat, rope, k_pos, tops)
    top_maj, top_min = tops
    m_maj = jnp.max(top_maj, axis=1, keepdims=True)
    m_min = jnp.max(top_min, axis=1, keepdims=True)
    sum_maj = jnp.zeros((2 * TOK, 128), F32)
    sum_min = jnp.zeros((2 * TOK, 128), F32)
    o_maj = jnp.zeros((2 * TOK, 128), F32)
    o_min = jnp.zeros((2 * TOK, 64), F32)
    step = 512
    for at in range(0, KEYS, step):
        p = jnp.exp(s_maj[:, at : at + step] - m_maj)
        r = jnp.exp(s_min[:, at : at + step] - m_min)
        for k in range(step // 128):
            sum_maj = sum_maj + p[:, 128 * k : 128 * (k + 1)]
            sum_min = sum_min + r[:, 128 * k : 128 * (k + 1)]
        v = v_all[at : at + step, :]
        o_maj = o_maj + dot(p.astype(BF16), v[:, :128])
        o_min = o_min + dot(r.astype(BF16), v[:, 128:192])
    l_maj = jnp.sum(sum_maj, axis=1, keepdims=True)
    l_min = jnp.sum(sum_min, axis=1, keepdims=True)
    lane = lax.broadcasted_iota(jnp.int32, (2 * TOK, 64), 1)
    stats = jnp.where(
        lane == 0, m_maj, jnp.where(lane == 1, l_maj, jnp.where(lane == 2, m_min, l_min))
    )
    result = jnp.concatenate([o_maj, o_min, stats], axis=1)
    own[...] = result[:TOK]
    other[...] = result[TOK:]


def project_body(a, b, out_maj, out_min, parts):
    a, b = a[...], b[...]

    def joined(m_at, lo, hi):
        m_a, m_b = a[:, m_at : m_at + 1], b[:, m_at : m_at + 1]
        l_a, l_b = a[:, m_at + 1 : m_at + 2], b[:, m_at + 1 : m_at + 2]
        top = jnp.maximum(m_a, m_b)
        f_a, f_b = jnp.exp(m_a - top), jnp.exp(m_b - top)
        total = l_a * f_a + l_b * f_b
        return ((a[:, lo:hi] * f_a + b[:, lo:hi] * f_b) / total).astype(BF16)

    attn_maj = joined(192, 0, 128)
    attn_min = joined(194, 128, 192)
    value = dot(attn_maj, out_maj[...]) + dot(attn_min, out_min[...])
    for t in range(N_TP):
        parts[t] = value[:, 128 * t : 128 * (t + 1)].astype(BF16)


def slot_columns(ids):
    lane = lax.broadcasted_iota(jnp.int32, (TOK, EXPERTS), 1)
    first = (ids[:, 0:1] == lane).astype(F32)
    second = (ids[:, 1:2] == lane).astype(F32)
    below = (
        lax.broadcasted_iota(jnp.int32, (TOK, TOK), 1) < lax.broadcasted_iota(jnp.int32, (TOK, TOK), 0)
    ).astype(BF16)
    earlier = dot(below, (first + second).astype(BF16))
    rank_0 = jnp.sum(first * earlier, axis=1, keepdims=True).astype(jnp.int32)
    rank_1 = jnp.sum(second * earlier, axis=1, keepdims=True).astype(jnp.int32)
    return ids[:, 0:1] * CAP + rank_0, ids[:, 1:2] * CAP + rank_1


def place_body(parts, residual, ids, stream, placed):
    slot_0, slot_1 = slot_columns(ids[...])
    lane = lax.broadcasted_iota(jnp.int32, (TOK, SLOTS), 1)
    select = ((lane == slot_0) | (lane == slot_1)).astype(BF16)
    summed = parts[0].astype(F32)
    for t in range(1, N_TP):
        summed = summed + parts[t].astype(F32)
    rows = (residual[...].astype(F32) + summed).astype(BF16)
    stream[...] = rows
    placed[...] = dot(select, rows, ((0,), (0,))).astype(BF16)


def pack_body(gate, up, down, low, high, sems):
    pairs = []
    for i, out in enumerate((low, high)):
        mine = pl.ds(128 * i, 128)
        pairs.append((gate.at[0, :, mine], out.at[pl.ds(0, D)]))
        pairs.append((up.at[0, :, mine], out.at[pl.ds(D, D)]))
        for t in range(N_TP):
            pairs.append((down.at[0, mine, pl.ds(128 * t, 128)], out.at[pl.ds(2 * D + 128 * t, 128)]))
    for c in fetch(pairs, sems):
        c.wait()


def expert_body(
    got, gain, gate_a, up_a, down_a, low, high,
    parts,
    gate_w, up_w, down_w, x, sems,
):
    pairs = [(gate_a.at[0], gate_w.at[0]), (up_a.at[0], up_w.at[0])]
    for i, packed in enumerate((low, high)):
        mine = pl.ds(128 * i, 128)
        pairs.append((packed.at[pl.ds(0, D)], gate_w.at[1, :, mine]))
        pairs.append((packed.at[pl.ds(D, D)], up_w.at[1, :, mine]))
    pairs.append((down_a.at[0], down_w.at[0]))
    for i, packed in enumerate((low, high)):
        for t in range(N_TP):
            pairs.append(
                (
                    packed.at[pl.ds(2 * D + 128 * t, 128)],
                    down_w.at[1, pl.ds(128 * i, 128), pl.ds(128 * t, 128)],
                )
            )
    copies = fetch(pairs, sems)
    squares = jnp.zeros((HALF, 128), F32)
    for t in range(N_TP):
        v = got[t].astype(F32)
        squares = squares + v * v
    factor = lax.rsqrt(jnp.sum(squares, axis=1, keepdims=True) / D + NORM_EPS)
    for t in range(N_TP):
        x[:, 128 * t : 128 * (t + 1)] = (
            got[t].astype(F32) * factor * gain[:, 128 * t : 128 * (t + 1)]
        ).astype(BF16)
    hidden = []
    for i in range(2):
        for c in copies[2 * i : 2 + 4 * i]:
            c.wait()
        gate = dot(x[...], gate_w[i])
        up = dot(x[...], up_w[i])
        hidden.append((gate / (1.0 + jnp.exp(-gate)) * up).astype(BF16))
    for c in copies[6:]:
        c.wait()
    for t in range(0, N_TP, 2):
        cols = slice(128 * t, 128 * (t + 2))
        value = dot(hidden[0], down_w[0, :, cols]) + dot(hidden[1], down_w[1, :, cols])
        parts[t] = value[:, :128].astype(BF16)
        parts[t + 1] = value[:, 128:].astype(BF16)


def gather_sum_body(parts, out):
    core = lax.axis_index("sp") % 2
    for half in range(2):
        total = jnp.zeros((HALF, 128), F32)
        for k in range(N_TP // 2):
            by_x = 2 * k + half
            by_y = (k // 4) * 8 + half * 4 + k % 4
            total = total + parts[jnp.where(core == 0, by_x, by_y)].astype(F32)
        out[half * HALF : (half + 1) * HALF, :] = total.astype(BF16)


def mix_body(returned, stream, ids, weights, out):
    slot_0, slot_1 = slot_columns(ids[...])
    lane = lax.broadcasted_iota(jnp.int32, (TOK, SLOTS), 1)
    rows = returned[...]
    w = weights[...]
    first = dot((lane == slot_0).astype(BF16), rows) * w[:, 0:1]
    second = dot((lane == slot_1).astype(BF16), rows) * w[:, 1:2]
    out[...] = (stream[...].astype(F32) + (first + second)).astype(BF16)


def shape(dims, kind=BF16):
    return pltpu.VMEM(dims, kind)


def room(dims, kind=BF16):
    return pltpu.VMEM(dims, kind)


def kernel(body, outs, rooms, sems, operands, near=()):
    single = not isinstance(outs, tuple)
    places = [pltpu.VMEM if i in near else pltpu.HBM for i in range(len(operands))]
    operands = [pltpu.with_memory_space_constraint(x, m) for x, m in zip(operands, places)]
    return pl.pallas_call(
        body,
        out_shape=outs,
        in_specs=[pl.BlockSpec(memory_space=m) for m in places],
        out_specs=vmem(1)[0] if single else tuple(vmem(len(outs))),
        scratch_shapes=rooms + ([pltpu.SemaphoreType.DMA((sems,))] if sems else []),
        compiler_params=pltpu.CompilerParams(vmem_limit_bytes=24 * 2**20),
    )(*operands)


def to_each(array, axis, groups=None):
    return lax.all_to_all(array, axis, 0, 0, tiled=True, axis_index_groups=groups)


def per_device(
    query_major,
    query_minor,
    latent_rows,
    rope_keys,
    key_up_major,
    value_up_major,
    key_up_minor,
    value_up_minor,
    out_major,
    out_minor,
    residual,
    norm_gain,
    expert_ids,
    expert_weights,
    gate_proj,
    up_proj,
    down_proj,
):
    table = jnp.asarray(TABLE)
    rows = kernel(
        rows_body,
        shape((N_Z, ROWS, 640)),
        [room((ROWS, LATENT)), room((ROPE, TOK)), room((160, 128), F32), room((TOK, ROPE), F32)],
        3,
        (latent_rows, rope_keys.T, table),
    )
    got_rows = to_each(rows, "sp", SAME_CORE)
    low, high = kernel(
        pack_body,
        (shape((3 * D, 128)), shape((3 * D, 128))),
        [],
        4 + 2 * N_TP,
        (gate_proj, up_proj, down_proj),
    )
    packed = kernel(
        choose_body, shape((PACKED, 128)), [room((FAR_ROWS, 640))], 0, (got_rows,), (0,)
    )
    spread = jnp.broadcast_to(packed, (N_TP, PACKED, 128))
    keys = to_each(spread, "tp")
    q_own, up_weights, own_block = kernel(
        queries_body,
        (shape((TOK, 320)), shape((LATENT, 384)), shape((TOK, 640))),
        [],
        0,
        (
            query_major,
            query_minor,
            table,
            packed,
            key_up_major,
            value_up_major,
            key_up_minor,
            value_up_minor,
            latent_rows,
            rope_keys.T,
        ),
        range(10),
    )
    q_other = lax.ppermute(q_own, "sp", OTHER_CORE)
    blocks = [lax.ppermute(own_block, "sp", along_z(-step)) if step else own_block for step in NEAR]
    from_low = lax.ppermute(low, ("sp", "tp"), ring(1))
    from_high = lax.ppermute(high, ("sp", "tp"), ring(-1))
    own, other = kernel(
        attend_body,
        (shape((TOK, 256), F32), shape((TOK, 256), F32)),
        [
            room((2 * TOK, KEYS), F32),
            room((2 * TOK, KEYS), F32),
            room((KEYS, 192)),
            room((2 * TOK, 320)),
            room((LATENT, 384)),
            room((len(NEAR) * TOK, 640)),
        ],
        3 + len(NEAR),
        (keys, q_own, q_other, up_weights, *blocks),
        (0,),
    )
    from_other = lax.ppermute(other, "sp", OTHER_CORE)
    head_parts = kernel(
        project_body,
        shape((N_TP, TOK, 128)),
        [],
        0,
        (own, from_other, out_major, out_minor),
        range(4),
    )
    head_parts = to_each(head_parts, "tp")
    stream, placed = kernel(
        place_body,
        (shape((TOK, 128)), shape((SLOTS, 128))),
        [],
        0,
        (head_parts, residual, expert_ids),
        range(3),
    )
    arrived = to_each(placed.reshape(EXPERTS, CAP, 128), "sp").reshape(2, 1, HALF, 128)
    peers = jnp.arange(N_TP, dtype=jnp.int32)
    half_of = jnp.where(lax.axis_index("sp") % 2 == 0, peers % 2, (peers // 4) % 2)
    half_rows = jnp.where(half_of[:, None, None] == 0, arrived[0], arrived[1])
    everyone = to_each(half_rows, "tp")
    down_parts = kernel(
        expert_body,
        shape((N_TP, HALF, 128)),
        [
            room((2, D, 256)),
            room((2, D, 256)),
            room((2, 256, D)),
            room((HALF, D)),
        ],
        7 + 2 * N_TP,
        (everyone, norm_gain.reshape(1, D), gate_proj, up_proj, down_proj, from_low, from_high),
        (0, 1),
    )
    down_parts = to_each(down_parts, "tp")
    expert_out = kernel(gather_sum_body, shape((SLOTS, 128)), [], 0, (down_parts,), (0,))
    returned = to_each(expert_out.reshape(EXPERTS, CAP, 128), "sp").reshape(SLOTS, 128)
    return kernel(
        mix_body,
        jax.ShapeDtypeStruct((TOK, 128), BF16),
        [],
        0,
        (returned, stream, expert_ids, expert_weights),
        range(4),
    )


def solution(mesh):
    in_specs = (
        P("sp", "tp"),
        P("sp", "tp"),
        P("sp", None),
        P("sp", None),
        P(None, "tp"),
        P(None, "tp"),
        P(None, "tp"),
        P(None, "tp"),
        P("tp", None),
        P("tp", None),
        P("sp", "tp"),
        P(),
        P("sp", None),
        P("sp", None),
        P("sp", None, "tp"),
        P("sp", None, "tp"),
        P("sp", "tp", None),
    )

    return jax.shard_map(
        per_device, mesh=mesh, in_specs=in_specs, out_specs=P("sp", "tp"), check_vma=False
    )
```

```python
import jax
import jax.numpy as jnp
import numpy as np
from jax import lax
from jax.experimental import pallas as pl
from jax.experimental.pallas import tpu as pltpu
from jax.sharding import PartitionSpec as P


F32 = jnp.float32
BF16 = jnp.bfloat16
D = 2048
ROPE = 64
NOPE_MAJOR = 128
NOPE_MINOR = 64
LATENT = 512
TOK = 128
N_TP = 16
N_Z = 16
EXPERTS = 32
CAP = 16
SLOTS = EXPERTS * CAP
ROWS = TOK // N_TP
KEYS = N_Z * TOK
MASKED = -1e30
NORM_EPS = 1e-6
HALF = SLOTS // 2
NEAR = (-2, -1, 0, 1)
FAR = N_Z - len(NEAR)
FAR_ROWS = FAR * ROWS
PACKED = 4 * FAR_ROWS + FAR_ROWS // 2


def along_z(step):
    return [(z * 2 + c, (z + step) % N_Z * 2 + c) for z in range(N_Z) for c in range(2)]


def turns(positions):
    angles = positions[:, None] * (1.0 / 10000.0 ** (np.arange(32) / 32.0))[None, :]
    return np.concatenate([np.cos(angles), np.sin(angles), np.zeros((len(positions), 64))], axis=1)


TABLE = np.concatenate([turns(np.arange(2 * N_Z) * float(TOK)), turns(np.arange(TOK) * 1.0)]).astype(
    np.float32
)

SAME_CORE = [[z * 2 + c for z in range(N_Z)] for c in range(2)]
OTHER_CORE = [(i, i ^ 1) for i in range(2 * N_Z)]


def ring(step):
    moves = []
    for s in range(2 * N_Z):
        for t in range(N_TP):
            y, x = divmod(t, 4)
            to = (y + step) % 4 * 4 + x if s % 2 else y * 4 + (x + step) % 4
            moves.append((s * N_TP + t, s * N_TP + to))
    return moves


HALF = SLOTS // 2
NEAR = (-2, -1, 0, 1)
FAR = N_Z - len(NEAR)
FAR_ROWS = FAR * ROWS
PACKED = 4 * FAR_ROWS + FAR_ROWS // 2


def along_z(step):
    return [(z * 2 + c, (z + step) % N_Z * 2 + c) for z in range(N_Z) for c in range(2)]


def turns(positions):
    angles = positions[:, None] * (1.0 / 10000.0 ** (np.arange(32) / 32.0))[None, :]
    return np.concatenate([np.cos(angles), np.sin(angles), np.zeros((len(positions), 64))], axis=1)


TABLE = np.concatenate([turns(np.arange(2 * N_Z) * float(TOK)), turns(np.arange(TOK) * 1.0)]).astype(
    np.float32
)

SAME_CORE = [[z * 2 + c for z in range(N_Z)] for c in range(2)]
OTHER_CORE = [(i, i ^ 1) for i in range(2 * N_Z)]


ANY = pl.BlockSpec(memory_space=pl.ANY)


def vmem(n):
    return [pl.BlockSpec(memory_space=pltpu.VMEM)] * n


def fetch(pairs, sems):
    copies = [pltpu.make_async_copy(src, dst, sems.at[i]) for i, (src, dst) in enumerate(pairs)]
    for c in copies:
        c.start()
    return copies


def dot(a, b, dims=((1,), (0,))):
    return lax.dot_general(a, b, (dims, ((), ())), preferred_element_type=F32)


def turn_at(table, block, rows):
    first = table[pl.ds(block, 1), :]
    c_0, s_0 = first[:, :32], first[:, 32:64]
    c_1, s_1 = rows[:, :32], rows[:, 32:64]
    return c_0 * c_1 - s_0 * s_1, s_0 * c_1 + c_0 * s_1


def turned(values, cosine, sine):
    low = values[:, :32].astype(F32)
    high = values[:, 32:].astype(F32)
    return jnp.concatenate(
        [low * cosine - high * sine, high * cosine + low * sine], axis=1
    ).astype(BF16)


def rows_body(lat_in, rope_in, table_in, out, lat, rope, table, by_row, sems):
    block, part = lax.axis_index("sp"), lax.axis_index("tp")
    mine = pl.ds(pl.multiple_of(part * ROWS, ROWS), ROWS)
    for c in fetch(((lat_in.at[mine], lat), (rope_in, rope), (table_in, table)), sems):
        c.wait()
    at = pl.ds(pl.multiple_of(2 * N_Z + part * ROWS, ROWS), ROWS)
    cosine, sine = turn_at(table, block, table[at, :])
    by_row[...] = rope[...].astype(F32).T
    key = turned(by_row[pl.ds(pl.multiple_of(part * ROWS, ROWS), ROWS), :], cosine, sine)
    row = jnp.concatenate([lat[...], key, jnp.zeros((ROWS, 64), BF16)], axis=1)
    for z in range(N_Z):
        out[z] = row


def queries_body(maj, low, table, after, ku_maj, vu_maj, ku_min, vu_min, lat, rope, out, weights, block):
    weights[...] = jnp.concatenate([ku_maj[...], vu_maj[...], ku_min[...], vu_min[...]], axis=1)
    c, s = turn_at(table, lax.axis_index("sp"), table[2 * N_Z :, :])
    key = turned(rope[...].astype(F32).T, c, s)
    block[...] = jnp.concatenate([lat[...], key, jnp.zeros((TOK, 64), BF16)], axis=1)
    out[...] = jnp.concatenate(
        [
            maj[:, :NOPE_MAJOR],
            turned(maj[:, NOPE_MAJOR:], c, s),
            low[:, :NOPE_MINOR],
            turned(low[:, NOPE_MINOR:], c, s),
        ],
        axis=1,
    )


def choose_body(got, out, flat):
    z = lax.axis_index("sp") // 2
    for o in range(FAR):
        flat[ROWS * o : ROWS * (o + 1), :] = got[(z + NEAR[-1] + 1 + o) % N_Z]
    for k in range(4):
        out[FAR_ROWS * k : FAR_ROWS * (k + 1), :] = flat[:, 128 * k : 128 * (k + 1)]
    rope = flat[:, 512:576]
    out[4 * FAR_ROWS :, :] = jnp.concatenate([rope[: FAR_ROWS // 2], rope[FAR_ROWS // 2 :]], axis=1)


PER = 4
CHUNK = PER * FAR_ROWS
N_CHUNK = N_TP // PER


def attend_body(keys, q_own_in, q_other_in, up_in, *refs):
    near_in = refs[: len(NEAR)]
    own, other, s_maj, s_min, v_all, q_all, up_weights, near, sems = refs[len(NEAR) :]
    copies = fetch(
        (
            (up_in, up_weights),
            (q_own_in, q_all.at[pl.ds(0, TOK)]),
            (q_other_in, q_all.at[pl.ds(TOK, TOK)]),
        )
        + tuple((b, near.at[pl.ds(TOK * i, TOK)]) for i, b in enumerate(near_in)),
        sems,
    )
    me = lax.axis_index("sp")
    core, z = me % 2, me // 2
    row = lax.broadcasted_iota(jnp.int32, (2 * TOK, 1), 0)
    q_pos = jnp.where(row < TOK, me * TOK + row, (me + 1 - 2 * core) * TOK + row - TOK)
    scale_maj = (NOPE_MAJOR + ROPE) ** -0.5
    scale_min = (NOPE_MINOR + ROPE) ** -0.5
    tops = [jnp.full((2 * TOK, 128), MASKED, F32)] * 2
    for c in copies[:3]:
        c.wait()
    weights = up_weights[...]
    q_maj, q_min = q_all[:, :192], q_all[:, 192:320]

    def scored(at, width, lat, rope, k_pos, tops):
        up = dot(lat, weights).astype(BF16)
        k_maj = jnp.concatenate([up[:, :128], rope], axis=1)
        k_min = jnp.concatenate([up[:, 256:320], rope], axis=1)
        v_all[at : at + width, :] = jnp.concatenate([up[:, 128:256], up[:, 320:384]], axis=1)
        seen = k_pos <= q_pos
        found = []
        for q, k, scale, store, top in (
            (q_maj, k_maj, scale_maj, s_maj, tops[0]),
            (q_min, k_min, scale_min, s_min, tops[1]),
        ):
            s = jnp.where(seen, dot(q, k, ((1,), (1,))) * scale, MASKED)
            store[:, at : at + width] = s
            for i in range(width // 128):
                top = jnp.maximum(top, s[:, 128 * i : 128 * (i + 1)])
            found.append(top)
        return found

    col = lax.broadcasted_iota(jnp.int32, (1, CHUNK), 1)
    for n in range(N_CHUNK):
        lat_rows, rope_rows = [], []
        for t in range(n * PER, (n + 1) * PER):
            lat_rows.append(
                jnp.concatenate(
                    [keys[t, FAR_ROWS * k : FAR_ROWS * (k + 1), :] for k in range(4)], axis=1
                )
            )
            half = keys[t, 4 * FAR_ROWS :, :]
            rope_rows.append(jnp.concatenate([half[:, :64], half[:, 64:]], axis=0))
        lat = jnp.concatenate(lat_rows, axis=0)
        rope = jnp.concatenate(rope_rows, axis=0)
        inner = col % FAR_ROWS
        k_z = (z + NEAR[-1] + 1 + inner // ROWS) % N_Z
        k_pos = (2 * k_z + core) * TOK + ROWS * (n * PER + col // FAR_ROWS) + inner % ROWS
        tops = scored(CHUNK * n, CHUNK, lat, rope, k_pos, tops)
    for c in copies[3:]:
        c.wait()
    col = lax.broadcasted_iota(jnp.int32, (1, len(NEAR) * TOK), 1)
    k_pos = (2 * ((z + NEAR[0] + N_Z + col // TOK) % N_Z) + core) * TOK + col % TOK
    tops = scored(N_CHUNK * CHUNK, len(NEAR) * TOK, near[:, :512], near[:, 512:576], k_pos, tops)
    top_maj, top_min = tops
    m_maj = jnp.max(top_maj, axis=1, keepdims=True)
    m_min = jnp.max(top_min, axis=1, keepdims=True)
    sum_maj = jnp.zeros((2 * TOK, 128), F32)
    sum_min = jnp.zeros((2 * TOK, 128), F32)
    o_maj = jnp.zeros((2 * TOK, 128), F32)
    o_min = jnp.zeros((2 * TOK, 64), F32)
    step = 512
    for at in range(0, KEYS, step):
        p = jnp.exp(s_maj[:, at : at + step] - m_maj)
        r = jnp.exp(s_min[:, at : at + step] - m_min)
        for k in range(step // 128):
            sum_maj = sum_maj + p[:, 128 * k : 128 * (k + 1)]
            sum_min = sum_min + r[:, 128 * k : 128 * (k + 1)]
        v = v_all[at : at + step, :]
        o_maj = o_maj + dot(p.astype(BF16), v[:, :128])
        o_min = o_min + dot(r.astype(BF16), v[:, 128:192])
    l_maj = jnp.sum(sum_maj, axis=1, keepdims=True)
    l_min = jnp.sum(sum_min, axis=1, keepdims=True)
    lane = lax.broadcasted_iota(jnp.int32, (2 * TOK, 64), 1)
    stats = jnp.where(
        lane == 0, m_maj, jnp.where(lane == 1, l_maj, jnp.where(lane == 2, m_min, l_min))
    )
    result = jnp.concatenate([o_maj, o_min, stats], axis=1)
    own[...] = result[:TOK]
    other[...] = result[TOK:]


def project_body(a, b, out_maj, out_min, parts):
    a, b = a[...], b[...]

    def joined(m_at, lo, hi):
        m_a, m_b = a[:, m_at : m_at + 1], b[:, m_at : m_at + 1]
        l_a, l_b = a[:, m_at + 1 : m_at + 2], b[:, m_at + 1 : m_at + 2]
        top = jnp.maximum(m_a, m_b)
        f_a, f_b = jnp.exp(m_a - top), jnp.exp(m_b - top)
        total = l_a * f_a + l_b * f_b
        return ((a[:, lo:hi] * f_a + b[:, lo:hi] * f_b) / total).astype(BF16)

    attn_maj = joined(192, 0, 128)
    attn_min = joined(194, 128, 192)
    value = dot(attn_maj, out_maj[...]) + dot(attn_min, out_min[...])
    for t in range(N_TP):
        parts[t] = value[:, 128 * t : 128 * (t + 1)].astype(BF16)


def slot_columns(ids):
    lane = lax.broadcasted_iota(jnp.int32, (TOK, EXPERTS), 1)
    first = (ids[:, 0:1] == lane).astype(F32)
    second = (ids[:, 1:2] == lane).astype(F32)
    below = (
        lax.broadcasted_iota(jnp.int32, (TOK, TOK), 1) < lax.broadcasted_iota(jnp.int32, (TOK, TOK), 0)
    ).astype(BF16)
    earlier = dot(below, (first + second).astype(BF16))
    rank_0 = jnp.sum(first * earlier, axis=1, keepdims=True).astype(jnp.int32)
    rank_1 = jnp.sum(second * earlier, axis=1, keepdims=True).astype(jnp.int32)
    return ids[:, 0:1] * CAP + rank_0, ids[:, 1:2] * CAP + rank_1


def place_body(parts, residual, ids, stream, placed):
    slot_0, slot_1 = slot_columns(ids[...])
    lane = lax.broadcasted_iota(jnp.int32, (TOK, SLOTS), 1)
    select = ((lane == slot_0) | (lane == slot_1)).astype(BF16)
    summed = parts[0].astype(F32)
    for t in range(1, N_TP):
        summed = summed + parts[t].astype(F32)
    rows = (residual[...].astype(F32) + summed).astype(BF16)
    stream[...] = rows
    placed[...] = dot(select, rows, ((0,), (0,))).astype(BF16)


def pack_body(gate, up, down, low, high, sems):
    pairs = []
    for i, out in enumerate((low, high)):
        mine = pl.ds(128 * i, 128)
        pairs.append((gate.at[0, :, mine], out.at[pl.ds(0, D)]))
        pairs.append((up.at[0, :, mine], out.at[pl.ds(D, D)]))
        for t in range(N_TP):
            pairs.append((down.at[0, mine, pl.ds(128 * t, 128)], out.at[pl.ds(2 * D + 128 * t, 128)]))
    for c in fetch(pairs, sems):
        c.wait()


def expert_body(
    got, gain, gate_a, up_a, down_a, low, high,
    parts,
    gate_w, up_w, down_w, x, sems,
):
    pairs = [(gate_a.at[0], gate_w.at[0]), (up_a.at[0], up_w.at[0])]
    for i, packed in enumerate((low, high)):
        mine = pl.ds(128 * i, 128)
        pairs.append((packed.at[pl.ds(0, D)], gate_w.at[1, :, mine]))
        pairs.append((packed.at[pl.ds(D, D)], up_w.at[1, :, mine]))
    pairs.append((down_a.at[0], down_w.at[0]))
    for i, packed in enumerate((low, high)):
        for t in range(N_TP):
            pairs.append(
                (
                    packed.at[pl.ds(2 * D + 128 * t, 128)],
                    down_w.at[1, pl.ds(128 * i, 128), pl.ds(128 * t, 128)],
                )
            )
    copies = fetch(pairs, sems)
    squares = jnp.zeros((HALF, 128), F32)
    for t in range(N_TP):
        v = got[t].astype(F32)
        squares = squares + v * v
    factor = lax.rsqrt(jnp.sum(squares, axis=1, keepdims=True) / D + NORM_EPS)
    for t in range(N_TP):
        x[:, 128 * t : 128 * (t + 1)] = (
            got[t].astype(F32) * factor * gain[:, 128 * t : 128 * (t + 1)]
        ).astype(BF16)
    hidden = []
    for i in range(2):
        for c in copies[2 * i : 2 + 4 * i]:
            c.wait()
        gate = dot(x[...], gate_w[i])
        up = dot(x[...], up_w[i])
        hidden.append((gate / (1.0 + jnp.exp(-gate)) * up).astype(BF16))
    for c in copies[6:]:
        c.wait()
    for t in range(0, N_TP, 2):
        cols = slice(128 * t, 128 * (t + 2))
        value = dot(hidden[0], down_w[0, :, cols]) + dot(hidden[1], down_w[1, :, cols])
        parts[t] = value[:, :128].astype(BF16)
        parts[t + 1] = value[:, 128:].astype(BF16)


def gather_sum_body(parts, out):
    core = lax.axis_index("sp") % 2
    for half in range(2):
        total = jnp.zeros((HALF, 128), F32)
        for k in range(N_TP // 2):
            by_x = 2 * k + half
            by_y = (k // 4) * 8 + half * 4 + k % 4
            total = total + parts[jnp.where(core == 0, by_x, by_y)].astype(F32)
        out[half * HALF : (half + 1) * HALF, :] = total.astype(BF16)


def mix_body(returned, stream, ids, weights, out):
    slot_0, slot_1 = slot_columns(ids[...])
    lane = lax.broadcasted_iota(jnp.int32, (TOK, SLOTS), 1)
    rows = returned[...]
    w = weights[...]
    first = dot((lane == slot_0).astype(BF16), rows) * w[:, 0:1]
    second = dot((lane == slot_1).astype(BF16), rows) * w[:, 1:2]
    out[...] = (stream[...].astype(F32) + (first + second)).astype(BF16)


def shape(dims, kind=BF16):
    return pltpu.VMEM(dims, kind)


def room(dims, kind=BF16):
    return pltpu.VMEM(dims, kind)


def kernel(body, outs, rooms, sems, operands, near=()):
    single = not isinstance(outs, tuple)
    places = [pltpu.VMEM if i in near else pltpu.HBM for i in range(len(operands))]
    operands = [pltpu.with_memory_space_constraint(x, m) for x, m in zip(operands, places)]
    return pl.pallas_call(
        body,
        out_shape=outs,
        in_specs=[pl.BlockSpec(memory_space=m) for m in places],
        out_specs=vmem(1)[0] if single else tuple(vmem(len(outs))),
        scratch_shapes=rooms + ([pltpu.SemaphoreType.DMA((sems,))] if sems else []),
        compiler_params=pltpu.CompilerParams(vmem_limit_bytes=24 * 2**20),
    )(*operands)


def to_each(array, axis, groups=None):
    return lax.all_to_all(array, axis, 0, 0, tiled=True, axis_index_groups=groups)


def per_device(
    query_major,
    query_minor,
    latent_rows,
    rope_keys,
    key_up_major,
    value_up_major,
    key_up_minor,
    value_up_minor,
    out_major,
    out_minor,
    residual,
    norm_gain,
    expert_ids,
    expert_weights,
    gate_proj,
    up_proj,
    down_proj,
):
    table = jnp.asarray(TABLE)
    rows = kernel(
        rows_body,
        shape((N_Z, ROWS, 640)),
        [room((ROWS, LATENT)), room((ROPE, TOK)), room((160, 128), F32), room((TOK, ROPE), F32)],
        3,
        (latent_rows, rope_keys.T, table),
    )
    got_rows = to_each(rows, "sp", SAME_CORE)
    low, high = kernel(
        pack_body,
        (shape((3 * D, 128)), shape((3 * D, 128))),
        [],
        4 + 2 * N_TP,
        (gate_proj, up_proj, down_proj),
    )
    packed = kernel(
        choose_body, shape((PACKED, 128)), [room((FAR_ROWS, 640))], 0, (got_rows,), (0,)
    )
    spread = jnp.broadcast_to(packed, (N_TP, PACKED, 128))
    keys = to_each(spread, "tp")
    q_own, up_weights, own_block = kernel(
        queries_body,
        (shape((TOK, 320)), shape((LATENT, 384)), shape((TOK, 640))),
        [],
        0,
        (
            query_major,
            query_minor,
            table,
            packed,
            key_up_major,
            value_up_major,
            key_up_minor,
            value_up_minor,
            latent_rows,
            rope_keys.T,
        ),
        range(10),
    )
    q_other = lax.ppermute(q_own, "sp", OTHER_CORE)
    blocks = [lax.ppermute(own_block, "sp", along_z(-step)) if step else own_block for step in NEAR]
    from_low = lax.ppermute(low, ("sp", "tp"), ring(1))
    from_high = lax.ppermute(high, ("sp", "tp"), ring(-1))
    own, other = kernel(
        attend_body,
        (shape((TOK, 256), F32), shape((TOK, 256), F32)),
        [
            room((2 * TOK, KEYS), F32),
            room((2 * TOK, KEYS), F32),
            room((KEYS, 192)),
            room((2 * TOK, 320)),
            room((LATENT, 384)),
            room((len(NEAR) * TOK, 640)),
        ],
        3 + len(NEAR),
        (keys, q_own, q_other, up_weights, *blocks),
        (0,),
    )
    from_other = lax.ppermute(other, "sp", OTHER_CORE)
    head_parts = kernel(
        project_body,
        shape((N_TP, TOK, 128)),
        [],
        0,
        (own, from_other, out_major, out_minor),
        range(4),
    )
    head_parts = to_each(head_parts, "tp")
    stream, placed = kernel(
        place_body,
        (shape((TOK, 128)), shape((SLOTS, 128))),
        [],
        0,
        (head_parts, residual, expert_ids),
        range(3),
    )
    arrived = to_each(placed.reshape(EXPERTS, CAP, 128), "sp").reshape(2, 1, HALF, 128)
    peers = jnp.arange(N_TP, dtype=jnp.int32)
    half_of = jnp.where(lax.axis_index("sp") % 2 == 0, peers % 2, (peers // 4) % 2)
    half_rows = jnp.where(half_of[:, None, None] == 0, arrived[0], arrived[1])
    everyone = to_each(half_rows, "tp")
    down_parts = kernel(
        expert_body,
        shape((N_TP, HALF, 128)),
        [
            room((2, D, 256)),
            room((2, D, 256)),
            room((2, 256, D)),
            room((HALF, D)),
        ],
        7 + 2 * N_TP,
        (everyone, norm_gain.reshape(1, D), gate_proj, up_proj, down_proj, from_low, from_high),
        (0, 1),
    )
    down_parts = to_each(down_parts, "tp")
    expert_out = kernel(gather_sum_body, shape((SLOTS, 128)), [], 0, (down_parts,), (0,))
    returned = to_each(expert_out.reshape(EXPERTS, CAP, 128), "sp").reshape(SLOTS, 128)
    return kernel(
        mix_body,
        jax.ShapeDtypeStruct((TOK, 128), BF16),
        [],
        0,
        (returned, stream, expert_ids, expert_weights),
        range(4),
    )


def solution(mesh):
    in_specs = (
        P("sp", "tp"),
        P("sp", "tp"),
        P("sp", None),
        P("sp", None),
        P(None, "tp"),
        P(None, "tp"),
        P(None, "tp"),
        P(None, "tp"),
        P("tp", None),
        P("tp", None),
        P("sp", "tp"),
        P(),
        P("sp", None),
        P("sp", None),
        P("sp", None, "tp"),
        P("sp", None, "tp"),
        P("sp", "tp", None),
    )

    return jax.shard_map(
        per_device, mesh=mesh, in_specs=in_specs, out_specs=P("sp", "tp"), check_vma=False
    )
```

```python
import jax
import jax.numpy as jnp
import numpy as np
from jax import lax
from jax.experimental import pallas as pl
from jax.experimental.pallas import tpu as pltpu
from jax.sharding import PartitionSpec as P


F32 = jnp.float32
BF16 = jnp.bfloat16
D = 2048
ROPE = 64
NOPE_MAJOR = 128
NOPE_MINOR = 64
LATENT = 512
TOK = 128
N_TP = 16
N_Z = 16
EXPERTS = 32
CAP = 16
SLOTS = EXPERTS * CAP
ROWS = TOK // N_TP
KEYS = N_Z * TOK
MASKED = -1e30
NORM_EPS = 1e-6
HALF = SLOTS // 2
NEAR = (-2, -1, 0, 1, 2)
FAR = N_Z - len(NEAR)
FAR_ROWS = FAR * ROWS
FIRST_ROPE = -(-FAR_ROWS // 32) * 16
PACKED = 4 * FAR_ROWS + FIRST_ROPE


def along_z(step):
    return [(z * 2 + c, (z + step) % N_Z * 2 + c) for z in range(N_Z) for c in range(2)]


def turns(positions):
    angles = positions[:, None] * (1.0 / 10000.0 ** (np.arange(32) / 32.0))[None, :]
    return np.concatenate([np.cos(angles), np.sin(angles), np.zeros((len(positions), 64))], axis=1)


TABLE = np.concatenate([turns(np.arange(2 * N_Z) * float(TOK)), turns(np.arange(TOK) * 1.0)]).astype(
    np.float32
)

SAME_CORE = [[z * 2 + c for z in range(N_Z)] for c in range(2)]
OTHER_CORE = [(i, i ^ 1) for i in range(2 * N_Z)]


def ring(step):
    moves = []
    for s in range(2 * N_Z):
        for t in range(N_TP):
            y, x = divmod(t, 4)
            to = (y + step) % 4 * 4 + x if s % 2 else y * 4 + (x + step) % 4
            moves.append((s * N_TP + t, s * N_TP + to))
    return moves


HALF = SLOTS // 2
NEAR = (-2, -1, 0, 1, 2)
FAR = N_Z - len(NEAR)
FAR_ROWS = FAR * ROWS
FIRST_ROPE = -(-FAR_ROWS // 32) * 16
PACKED = 4 * FAR_ROWS + FIRST_ROPE


def along_z(step):
    return [(z * 2 + c, (z + step) % N_Z * 2 + c) for z in range(N_Z) for c in range(2)]


def turns(positions):
    angles = positions[:, None] * (1.0 / 10000.0 ** (np.arange(32) / 32.0))[None, :]
    return np.concatenate([np.cos(angles), np.sin(angles), np.zeros((len(positions), 64))], axis=1)


TABLE = np.concatenate([turns(np.arange(2 * N_Z) * float(TOK)), turns(np.arange(TOK) * 1.0)]).astype(
    np.float32
)

SAME_CORE = [[z * 2 + c for z in range(N_Z)] for c in range(2)]
OTHER_CORE = [(i, i ^ 1) for i in range(2 * N_Z)]


ANY = pl.BlockSpec(memory_space=pl.ANY)


def vmem(n):
    return [pl.BlockSpec(memory_space=pltpu.VMEM)] * n


def fetch(pairs, sems):
    copies = [pltpu.make_async_copy(src, dst, sems.at[i]) for i, (src, dst) in enumerate(pairs)]
    for c in copies:
        c.start()
    return copies


def dot(a, b, dims=((1,), (0,))):
    return lax.dot_general(a, b, (dims, ((), ())), preferred_element_type=F32)


def turn_at(table, block, rows):
    first = table[pl.ds(block, 1), :]
    c_0, s_0 = first[:, :32], first[:, 32:64]
    c_1, s_1 = rows[:, :32], rows[:, 32:64]
    return c_0 * c_1 - s_0 * s_1, s_0 * c_1 + c_0 * s_1


def turned(values, cosine, sine):
    low = values[:, :32].astype(F32)
    high = values[:, 32:].astype(F32)
    return jnp.concatenate(
        [low * cosine - high * sine, high * cosine + low * sine], axis=1
    ).astype(BF16)


def rows_body(lat_in, rope_in, table_in, out, lat, rope, table, by_row, sems):
    block, part = lax.axis_index("sp"), lax.axis_index("tp")
    mine = pl.ds(pl.multiple_of(part * ROWS, ROWS), ROWS)
    for c in fetch(((lat_in.at[mine], lat), (rope_in, rope), (table_in, table)), sems):
        c.wait()
    at = pl.ds(pl.multiple_of(2 * N_Z + part * ROWS, ROWS), ROWS)
    cosine, sine = turn_at(table, block, table[at, :])
    by_row[...] = rope[...].astype(F32).T
    key = turned(by_row[pl.ds(pl.multiple_of(part * ROWS, ROWS), ROWS), :], cosine, sine)
    row = jnp.concatenate([lat[...], key, jnp.zeros((ROWS, 64), BF16)], axis=1)
    for z in range(N_Z):
        out[z] = row


def queries_body(
    maj, low_in, table_in, ku_maj, vu_maj, ku_min, vu_min, lat, rope_in,
    out, weights, block,
    low, table, rope, sems,
):
    copies = fetch(
        (
            (low_in, low),
            (table_in, table),
            (rope_in, rope),
            (ku_maj, weights.at[:, pl.ds(0, 128)]),
            (vu_maj, weights.at[:, pl.ds(128, 128)]),
            (lat, block.at[:, pl.ds(0, LATENT)]),
        ),
        sems,
    )
    weights[:, 256:384] = jnp.concatenate([ku_min[...], vu_min[...]], axis=1)
    for c in copies[:3]:
        c.wait()
    c, s = turn_at(table, lax.axis_index("sp"), table[2 * N_Z :, :])
    key = turned(rope[...].astype(F32).T, c, s)
    block[:, LATENT:] = jnp.concatenate([key, jnp.zeros((TOK, 64), BF16)], axis=1)
    out[...] = jnp.concatenate(
        [
            maj[:, :NOPE_MAJOR],
            turned(maj[:, NOPE_MAJOR:], c, s),
            low[:, :NOPE_MINOR],
            turned(low[:, NOPE_MINOR:], c, s),
        ],
        axis=1,
    )
    for c in copies[3:]:
        c.wait()


def choose_body(got, out, flat):
    z = lax.axis_index("sp") // 2
    for o in range(FAR):
        flat[ROWS * o : ROWS * (o + 1), :] = got[(z + NEAR[-1] + 1 + o) % N_Z]
    for k in range(4):
        out[FAR_ROWS * k : FAR_ROWS * (k + 1), :] = flat[:, 128 * k : 128 * (k + 1)]
    rope = flat[:, 512:576]
    rest = jnp.concatenate([rope[FIRST_ROPE:], jnp.zeros((2 * FIRST_ROPE - FAR_ROWS, 64), BF16)], axis=0)
    out[4 * FAR_ROWS :, :] = jnp.concatenate([rope[:FIRST_ROPE], rest], axis=1)


PER = 16
CHUNK = PER * FAR_ROWS
N_CHUNK = N_TP // PER


def attend_body(keys, q_own_in, q_other_in, up_in, *refs):
    near_in = refs[: len(NEAR)]
    own, other, s_maj, s_min, v_all, q_all, up_weights, near, sems = refs[len(NEAR) :]
    copies = fetch(
        (
            (up_in, up_weights),
            (q_own_in, q_all.at[pl.ds(0, TOK)]),
            (q_other_in, q_all.at[pl.ds(TOK, TOK)]),
        )
        + tuple((b, near.at[pl.ds(TOK * i, TOK)]) for i, b in enumerate(near_in)),
        sems,
    )
    me = lax.axis_index("sp")
    core, z = me % 2, me // 2
    row = lax.broadcasted_iota(jnp.int32, (2 * TOK, 1), 0)
    q_pos = jnp.where(row < TOK, me * TOK + row, (me + 1 - 2 * core) * TOK + row - TOK)
    scale_maj = (NOPE_MAJOR + ROPE) ** -0.5
    scale_min = (NOPE_MINOR + ROPE) ** -0.5
    tops = [jnp.full((2 * TOK, 128), MASKED, F32)] * 2
    for c in copies[:3]:
        c.wait()
    weights = up_weights[...]
    q_maj, q_min = q_all[:, :192], q_all[:, 192:320]

    def scored(at, width, lat, rope, k_pos, tops):
        up = dot(lat, weights).astype(BF16)
        k_maj = jnp.concatenate([up[:, :128], rope], axis=1)
        k_min = jnp.concatenate([up[:, 256:320], rope], axis=1)
        v_all[at : at + width, :] = jnp.concatenate([up[:, 128:256], up[:, 320:384]], axis=1)
        seen = k_pos <= q_pos
        found = []
        for q, k, scale, store, top in (
            (q_maj, k_maj, scale_maj, s_maj, tops[0]),
            (q_min, k_min, scale_min, s_min, tops[1]),
        ):
            s = jnp.where(seen, dot(q, k, ((1,), (1,))) * scale, MASKED)
            store[:, at : at + width] = s
            for i in range(width // 128):
                top = jnp.maximum(top, s[:, 128 * i : 128 * (i + 1)])
            found.append(top)
        return found

    col = lax.broadcasted_iota(jnp.int32, (1, CHUNK), 1)
    for n in range(N_CHUNK):
        lat_rows, rope_rows = [], []
        for t in range(n * PER, (n + 1) * PER):
            lat_rows.append(
                jnp.concatenate(
                    [keys[t, FAR_ROWS * k : FAR_ROWS * (k + 1), :] for k in range(4)], axis=1
                )
            )
            half = keys[t, 4 * FAR_ROWS :, :]
            rope_rows.append(jnp.concatenate([half[:, :64], half[: FAR_ROWS - FIRST_ROPE, 64:]], axis=0))
        lat = jnp.concatenate(lat_rows, axis=0)
        rope = jnp.concatenate(rope_rows, axis=0)
        inner = col % FAR_ROWS
        k_z = (z + NEAR[-1] + 1 + inner // ROWS) % N_Z
        k_pos = (2 * k_z + core) * TOK + ROWS * (n * PER + col // FAR_ROWS) + inner % ROWS
        tops = scored(CHUNK * n, CHUNK, lat, rope, k_pos, tops)
    for c in copies[3:]:
        c.wait()
    col = lax.broadcasted_iota(jnp.int32, (1, len(NEAR) * TOK), 1)
    k_pos = (2 * ((z + NEAR[0] + N_Z + col // TOK) % N_Z) + core) * TOK + col % TOK
    tops = scored(N_CHUNK * CHUNK, len(NEAR) * TOK, near[:, :512], near[:, 512:576], k_pos, tops)
    top_maj, top_min = tops
    m_maj = jnp.max(top_maj, axis=1, keepdims=True)
    m_min = jnp.max(top_min, axis=1, keepdims=True)
    sum_maj = jnp.zeros((2 * TOK, 128), F32)
    sum_min = jnp.zeros((2 * TOK, 128), F32)
    o_maj = jnp.zeros((2 * TOK, 128), F32)
    o_min = jnp.zeros((2 * TOK, 64), F32)
    step = 512
    for at in range(0, KEYS, step):
        p = jnp.exp(s_maj[:, at : at + step] - m_maj)
        r = jnp.exp(s_min[:, at : at + step] - m_min)
        for k in range(step // 128):
            sum_maj = sum_maj + p[:, 128 * k : 128 * (k + 1)]
            sum_min = sum_min + r[:, 128 * k : 128 * (k + 1)]
        v = v_all[at : at + step, :]
        o_maj = o_maj + dot(p.astype(BF16), v[:, :128])
        o_min = o_min + dot(r.astype(BF16), v[:, 128:192])
    l_maj = jnp.sum(sum_maj, axis=1, keepdims=True)
    l_min = jnp.sum(sum_min, axis=1, keepdims=True)
    lane = lax.broadcasted_iota(jnp.int32, (2 * TOK, 64), 1)
    stats = jnp.where(
        lane == 0, m_maj, jnp.where(lane == 1, l_maj, jnp.where(lane == 2, m_min, l_min))
    )
    result = jnp.concatenate([o_maj, o_min, stats], axis=1)
    own[...] = result[:TOK]
    other[...] = result[TOK:]


def project_body(a, b, out_maj, out_min, parts):
    a, b = a[...], b[...]

    def joined(m_at, lo, hi):
        m_a, m_b = a[:, m_at : m_at + 1], b[:, m_at : m_at + 1]
        l_a, l_b = a[:, m_at + 1 : m_at + 2], b[:, m_at + 1 : m_at + 2]
        top = jnp.maximum(m_a, m_b)
        f_a, f_b = jnp.exp(m_a - top), jnp.exp(m_b - top)
        total = l_a * f_a + l_b * f_b
        return ((a[:, lo:hi] * f_a + b[:, lo:hi] * f_b) / total).astype(BF16)

    attn_maj = joined(192, 0, 128)
    attn_min = joined(194, 128, 192)
    value = dot(attn_maj, out_maj[...]) + dot(attn_min, out_min[...])
    for t in range(N_TP):
        parts[t] = value[:, 128 * t : 128 * (t + 1)].astype(BF16)


def slot_columns(ids):
    lane = lax.broadcasted_iota(jnp.int32, (TOK, EXPERTS), 1)
    first = (ids[:, 0:1] == lane).astype(F32)
    second = (ids[:, 1:2] == lane).astype(F32)
    below = (
        lax.broadcasted_iota(jnp.int32, (TOK, TOK), 1) < lax.broadcasted_iota(jnp.int32, (TOK, TOK), 0)
    ).astype(BF16)
    earlier = dot(below, (first + second).astype(BF16))
    rank_0 = jnp.sum(first * earlier, axis=1, keepdims=True).astype(jnp.int32)
    rank_1 = jnp.sum(second * earlier, axis=1, keepdims=True).astype(jnp.int32)
    return ids[:, 0:1] * CAP + rank_0, ids[:, 1:2] * CAP + rank_1


def place_body(parts, residual, ids, stream, placed):
    slot_0, slot_1 = slot_columns(ids[...])
    lane = lax.broadcasted_iota(jnp.int32, (TOK, SLOTS), 1)
    select = ((lane == slot_0) | (lane == slot_1)).astype(BF16)
    summed = parts[0].astype(F32)
    for t in range(1, N_TP):
        summed = summed + parts[t].astype(F32)
    rows = (residual[...].astype(F32) + summed).astype(BF16)
    stream[...] = rows
    placed[...] = dot(select, rows, ((0,), (0,))).astype(BF16)


def pack_body(gate, up, down, low, high, sems):
    pairs = []
    for i, out in enumerate((low, high)):
        mine = pl.ds(128 * i, 128)
        pairs.append((gate.at[0, :, mine], out.at[pl.ds(0, D)]))
        pairs.append((up.at[0, :, mine], out.at[pl.ds(D, D)]))
        for t in range(N_TP):
            pairs.append((down.at[0, mine, pl.ds(128 * t, 128)], out.at[pl.ds(2 * D + 128 * t, 128)]))
    for c in fetch(pairs, sems):
        c.wait()


def assemble_body(gate_a, low, high, gate_w, sems):
    pairs = [(gate_a.at[0], gate_w.at[:, pl.ds(0, 256)])]
    for i, packed in enumerate((low, high)):
        pairs.append((packed.at[pl.ds(0, D)], gate_w.at[:, pl.ds(256 + 128 * i, 128)]))
    for c in fetch(pairs, sems):
        c.wait()


def expert_body(got, gain, gate_w, up_a, down_a, low, high, parts, up_w, down_w, x, sems):
    own = pl.ds(0, 256)
    pairs = [(up_a.at[0], up_w.at[:, own])]
    for i, packed in enumerate((low, high)):
        pairs.append((packed.at[pl.ds(D, D)], up_w.at[:, pl.ds(256 + 128 * i, 128)]))
    pairs.append((down_a.at[0], down_w.at[own]))
    for i, packed in enumerate((low, high)):
        for t in range(N_TP):
            mine, cols = pl.ds(256 + 128 * i, 128), pl.ds(128 * t, 128)
            pairs.append((packed.at[pl.ds(2 * D + 128 * t, 128)], down_w.at[mine, cols]))
    copies = fetch(pairs, sems)
    squares = jnp.zeros((HALF, 128), F32)
    for t in range(N_TP):
        v = got[t].astype(F32)
        squares = squares + v * v
    factor = lax.rsqrt(jnp.sum(squares, axis=1, keepdims=True) / D + NORM_EPS)
    for t in range(N_TP):
        x[:, 128 * t : 128 * (t + 1)] = (
            got[t].astype(F32) * factor * gain[:, 128 * t : 128 * (t + 1)]
        ).astype(BF16)
    gate = dot(x[...], gate_w[...])
    for c in copies[:3]:
        c.wait()
    up = dot(x[...], up_w[...])
    hidden = (gate / (1.0 + jnp.exp(-gate)) * up).astype(BF16)
    for c in copies[3:]:
        c.wait()
    for t in range(0, N_TP, 2):
        value = dot(hidden, down_w[:, 128 * t : 128 * (t + 2)])
        parts[t] = value[:, :128].astype(BF16)
        parts[t + 1] = value[:, 128:].astype(BF16)


def gather_sum_body(parts, out):
    core = lax.axis_index("sp") % 2
    for half in range(2):
        total = jnp.zeros((HALF, 128), F32)
        for k in range(N_TP // 2):
            by_x = 2 * k + half
            by_y = (k // 4) * 8 + half * 4 + k % 4
            total = total + parts[jnp.where(core == 0, by_x, by_y)].astype(F32)
        out[half * HALF : (half + 1) * HALF, :] = total.astype(BF16)


def mix_body(returned, stream, ids, weights, out):
    slot_0, slot_1 = slot_columns(ids[...])
    lane = lax.broadcasted_iota(jnp.int32, (TOK, SLOTS), 1)
    rows = returned[...]
    w = weights[...]
    first = dot((lane == slot_0).astype(BF16), rows) * w[:, 0:1]
    second = dot((lane == slot_1).astype(BF16), rows) * w[:, 1:2]
    out[...] = (stream[...].astype(F32) + (first + second)).astype(BF16)


def shape(dims, kind=BF16):
    return pltpu.VMEM(dims, kind)


def room(dims, kind=BF16):
    return pltpu.VMEM(dims, kind)


def kernel(body, outs, rooms, sems, operands, near=()):
    single = not isinstance(outs, tuple)
    places = [pltpu.VMEM if i in near else pltpu.HBM for i in range(len(operands))]
    operands = [pltpu.with_memory_space_constraint(x, m) for x, m in zip(operands, places)]
    return pl.pallas_call(
        body,
        out_shape=outs,
        in_specs=[pl.BlockSpec(memory_space=m) for m in places],
        out_specs=vmem(1)[0] if single else tuple(vmem(len(outs))),
        scratch_shapes=rooms + ([pltpu.SemaphoreType.DMA((sems,))] if sems else []),
        compiler_params=pltpu.CompilerParams(vmem_limit_bytes=24 * 2**20),
    )(*operands)


def to_each(array, axis, groups=None):
    return lax.all_to_all(array, axis, 0, 0, tiled=True, axis_index_groups=groups)


def per_device(
    query_major,
    query_minor,
    latent_rows,
    rope_keys,
    key_up_major,
    value_up_major,
    key_up_minor,
    value_up_minor,
    out_major,
    out_minor,
    residual,
    norm_gain,
    expert_ids,
    expert_weights,
    gate_proj,
    up_proj,
    down_proj,
):
    table = jnp.asarray(TABLE)
    rows = kernel(
        rows_body,
        shape((N_Z, ROWS, 640)),
        [room((ROWS, LATENT)), room((ROPE, TOK)), room((160, 128), F32), room((TOK, ROPE), F32)],
        3,
        (latent_rows, rope_keys.T, table),
    )
    got_rows = to_each(rows, "sp", SAME_CORE)
    low, high = kernel(
        pack_body,
        (shape((3 * D, 128)), shape((3 * D, 128))),
        [],
        4 + 2 * N_TP,
        (gate_proj, up_proj, down_proj),
    )
    packed = kernel(
        choose_body, shape((PACKED, 128)), [room((FAR_ROWS, 640))], 0, (got_rows,), (0,)
    )
    spread = jnp.broadcast_to(packed, (N_TP, PACKED, 128))
    keys = to_each(spread, "tp")
    q_own, up_weights, own_block = kernel(
        queries_body,
        (shape((TOK, 320)), shape((LATENT, 384)), shape((TOK, 640))),
        [room((TOK, 128)), room((160, 128), F32), room((ROPE, TOK))],
        6,
        (
            query_major,
            query_minor,
            table,
            key_up_major,
            value_up_major,
            key_up_minor,
            value_up_minor,
            latent_rows,
            rope_keys.T,
        ),
        (0, 5, 6),
    )
    q_other = lax.ppermute(q_own, "sp", OTHER_CORE)
    blocks = [lax.ppermute(own_block, "sp", along_z(-step)) if step else own_block for step in NEAR]
    from_low = lax.ppermute(low, ("sp", "tp"), ring(1))
    from_high = lax.ppermute(high, ("sp", "tp"), ring(-1))
    own, other = kernel(
        attend_body,
        (shape((TOK, 256), F32), shape((TOK, 256), F32)),
        [
            room((2 * TOK, KEYS), F32),
            room((2 * TOK, KEYS), F32),
            room((KEYS, 192)),
            room((2 * TOK, 320)),
            room((LATENT, 384)),
            room((len(NEAR) * TOK, 640)),
        ],
        3 + len(NEAR),
        (keys, q_own, q_other, up_weights, *blocks),
        (0,),
    )
    from_other = lax.ppermute(other, "sp", OTHER_CORE)
    head_parts = kernel(
        project_body,
        shape((N_TP, TOK, 128)),
        [],
        0,
        (own, from_other, out_major, out_minor),
        range(4),
    )
    head_parts = to_each(head_parts, "tp")
    stream, placed = kernel(
        place_body,
        (shape((TOK, 128)), shape((SLOTS, 128))),
        [],
        0,
        (head_parts, residual, expert_ids),
        range(3),
    )
    arrived = to_each(placed.reshape(EXPERTS, CAP, 128), "sp").reshape(2, 1, HALF, 128)
    peers = jnp.arange(N_TP, dtype=jnp.int32)
    half_of = jnp.where(lax.axis_index("sp") % 2 == 0, peers % 2, (peers // 4) % 2)
    half_rows = jnp.where(half_of[:, None, None] == 0, arrived[0], arrived[1])
    everyone = to_each(half_rows, "tp")
    gate_w = kernel(assemble_body, shape((D, 512)), [], 3, (gate_proj, from_low, from_high))
    down_parts = kernel(
        expert_body,
        shape((N_TP, HALF, 128)),
        [room((D, 512)), room((512, D)), room((HALF, D))],
        4 + 2 * N_TP,
        (everyone, norm_gain.reshape(1, D), gate_w, up_proj, down_proj, from_low, from_high),
        (0, 1, 2),
    )
    down_parts = to_each(down_parts, "tp")
    expert_out = kernel(gather_sum_body, shape((SLOTS, 128)), [], 0, (down_parts,), (0,))
    returned = to_each(expert_out.reshape(EXPERTS, CAP, 128), "sp").reshape(SLOTS, 128)
    return kernel(
        mix_body,
        jax.ShapeDtypeStruct((TOK, 128), BF16),
        [],
        0,
        (returned, stream, expert_ids, expert_weights),
        range(4),
    )


def solution(mesh):
    in_specs = (
        P("sp", "tp"),
        P("sp", "tp"),
        P("sp", None),
        P("sp", None),
        P(None, "tp"),
        P(None, "tp"),
        P(None, "tp"),
        P(None, "tp"),
        P("tp", None),
        P("tp", None),
        P("sp", "tp"),
        P(),
        P("sp", None),
        P("sp", None),
        P("sp", None, "tp"),
        P("sp", None, "tp"),
        P("sp", "tp", None),
    )

    return jax.shard_map(
        per_device, mesh=mesh, in_specs=in_specs, out_specs=P("sp", "tp"), check_vma=False
    )
```

```python
import jax
import jax.numpy as jnp
import numpy as np
from jax import lax
from jax.experimental import pallas as pl
from jax.experimental.pallas import tpu as pltpu
from jax.sharding import PartitionSpec as P


F32 = jnp.float32
BF16 = jnp.bfloat16
D = 2048
ROPE = 64
NOPE_MAJOR = 128
NOPE_MINOR = 64
LATENT = 512
TOK = 128
N_TP = 16
N_Z = 16
EXPERTS = 32
CAP = 16
SLOTS = EXPERTS * CAP
ROWS = TOK // N_TP
KEYS = N_Z * TOK
MASKED = -1e30
NORM_EPS = 1e-6
HALF = SLOTS // 2
NEAR = (-2, -1, 0, 1)
FAR = N_Z - len(NEAR)
FAR_ROWS = FAR * ROWS
PACKED = 4 * FAR_ROWS + FAR_ROWS // 2


def along_z(step):
    moves = [(z, (z + step) % N_Z) for z in range(N_Z)]
    return [(a * 2 + c, b * 2 + c) for a, b in moves if a <= b for c in range(2)]


def turns(positions):
    angles = positions[:, None] * (1.0 / 10000.0 ** (np.arange(32) / 32.0))[None, :]
    return np.concatenate([np.cos(angles), np.sin(angles), np.zeros((len(positions), 64))], axis=1)


TABLE = np.concatenate([turns(np.arange(2 * N_Z) * float(TOK)), turns(np.arange(TOK) * 1.0)]).astype(
    np.float32
)

SAME_CORE = [[z * 2 + c for z in range(N_Z)] for c in range(2)]
OTHER_CORE = [(i, i ^ 1) for i in range(2 * N_Z)]


def ring(step):
    moves = []
    for s in range(2 * N_Z):
        for t in range(N_TP):
            y, x = divmod(t, 4)
            to = (y + step) % 4 * 4 + x if s % 2 else y * 4 + (x + step) % 4
            moves.append((s * N_TP + t, s * N_TP + to))
    return moves


HALF = SLOTS // 2
NEAR = (-2, -1, 0, 1)
FAR = N_Z - len(NEAR)
FAR_ROWS = FAR * ROWS
PACKED = 4 * FAR_ROWS + FAR_ROWS // 2


def along_z(step):
    moves = [(z, (z + step) % N_Z) for z in range(N_Z)]
    return [(a * 2 + c, b * 2 + c) for a, b in moves if a <= b for c in range(2)]


def turns(positions):
    angles = positions[:, None] * (1.0 / 10000.0 ** (np.arange(32) / 32.0))[None, :]
    return np.concatenate([np.cos(angles), np.sin(angles), np.zeros((len(positions), 64))], axis=1)


TABLE = np.concatenate([turns(np.arange(2 * N_Z) * float(TOK)), turns(np.arange(TOK) * 1.0)]).astype(
    np.float32
)

SAME_CORE = [[z * 2 + c for z in range(N_Z)] for c in range(2)]
OTHER_CORE = [(i, i ^ 1) for i in range(2 * N_Z)]


ANY = pl.BlockSpec(memory_space=pl.ANY)


def vmem(n):
    return [pl.BlockSpec(memory_space=pltpu.VMEM)] * n


def fetch(pairs, sems):
    copies = [pltpu.make_async_copy(src, dst, sems.at[i]) for i, (src, dst) in enumerate(pairs)]
    for c in copies:
        c.start()
    return copies


def dot(a, b, dims=((1,), (0,))):
    return lax.dot_general(a, b, (dims, ((), ())), preferred_element_type=F32)


def turn_at(table, block, rows):
    first = table[pl.ds(block, 1), :]
    c_0, s_0 = first[:, :32], first[:, 32:64]
    c_1, s_1 = rows[:, :32], rows[:, 32:64]
    return c_0 * c_1 - s_0 * s_1, s_0 * c_1 + c_0 * s_1


def turned(values, cosine, sine):
    low = values[:, :32].astype(F32)
    high = values[:, 32:].astype(F32)
    return jnp.concatenate(
        [low * cosine - high * sine, high * cosine + low * sine], axis=1
    ).astype(BF16)


def rows_body(lat_in, rope_in, table_in, out, lat, rope, table, by_row, sems):
    block, part = lax.axis_index("sp"), lax.axis_index("tp")
    mine = pl.ds(pl.multiple_of(part * ROWS, ROWS), ROWS)
    for c in fetch(((lat_in.at[mine], lat), (rope_in, rope), (table_in, table)), sems):
        c.wait()
    at = pl.ds(pl.multiple_of(2 * N_Z + part * ROWS, ROWS), ROWS)
    cosine, sine = turn_at(table, block, table[at, :])
    by_row[...] = rope[...].astype(F32).T
    key = turned(by_row[pl.ds(pl.multiple_of(part * ROWS, ROWS), ROWS), :], cosine, sine)
    row = jnp.concatenate([lat[...], key, jnp.zeros((ROWS, 64), BF16)], axis=1)
    for z in range(N_Z):
        out[z] = row


def queries_body(
    maj, low_in, table_in, ku_maj, vu_maj, ku_min, vu_min, lat, rope_in,
    out, weights, block,
    low, table, rope, sems,
):
    copies = fetch(
        (
            (low_in, low),
            (table_in, table),
            (rope_in, rope),
            (ku_maj, weights.at[:, pl.ds(0, 128)]),
            (vu_maj, weights.at[:, pl.ds(128, 128)]),
            (lat, block.at[:, pl.ds(0, LATENT)]),
        ),
        sems,
    )
    weights[:, 256:384] = jnp.concatenate([ku_min[...], vu_min[...]], axis=1)
    for c in copies[:3]:
        c.wait()
    c, s = turn_at(table, lax.axis_index("sp"), table[2 * N_Z :, :])
    key = turned(rope[...].astype(F32).T, c, s)
    block[:, LATENT:] = jnp.concatenate([key, jnp.zeros((TOK, 64), BF16)], axis=1)
    out[...] = jnp.concatenate(
        [
            maj[:, :NOPE_MAJOR],
            turned(maj[:, NOPE_MAJOR:], c, s),
            low[:, :NOPE_MINOR],
            turned(low[:, NOPE_MINOR:], c, s),
        ],
        axis=1,
    )
    for c in copies[3:]:
        c.wait()


def choose_body(got, out, flat):
    z = lax.axis_index("sp") // 2
    for o in range(FAR):
        flat[ROWS * o : ROWS * (o + 1), :] = got[(z + NEAR[-1] + 1 + o) % N_Z]
    for k in range(4):
        out[FAR_ROWS * k : FAR_ROWS * (k + 1), :] = flat[:, 128 * k : 128 * (k + 1)]
    rope = flat[:, 512:576]
    out[4 * FAR_ROWS :, :] = jnp.concatenate([rope[: FAR_ROWS // 2], rope[FAR_ROWS // 2 :]], axis=1)


PER = 4
CHUNK = PER * FAR_ROWS
N_CHUNK = N_TP // PER


def attend_body(keys, q_own_in, q_other_in, up_in, *refs):
    near_in = refs[: len(NEAR)]
    own, other, s_maj, s_min, v_all, q_all, up_weights, near, sems = refs[len(NEAR) :]
    copies = fetch(
        (
            (up_in, up_weights),
            (q_own_in, q_all.at[pl.ds(0, TOK)]),
            (q_other_in, q_all.at[pl.ds(TOK, TOK)]),
        )
        + tuple((b, near.at[pl.ds(TOK * i, TOK)]) for i, b in enumerate(near_in)),
        sems,
    )
    me = lax.axis_index("sp")
    core, z = me % 2, me // 2
    row = lax.broadcasted_iota(jnp.int32, (2 * TOK, 1), 0)
    q_pos = jnp.where(row < TOK, me * TOK + row, (me + 1 - 2 * core) * TOK + row - TOK)
    scale_maj = (NOPE_MAJOR + ROPE) ** -0.5
    scale_min = (NOPE_MINOR + ROPE) ** -0.5
    tops = [jnp.full((2 * TOK, 128), MASKED, F32)] * 2
    for c in copies[:3]:
        c.wait()
    weights = up_weights[...]
    q_maj, q_min = q_all[:, :192], q_all[:, 192:320]

    def scored(at, width, lat, rope, k_pos, tops):
        up = dot(lat, weights).astype(BF16)
        k_maj = jnp.concatenate([up[:, :128], rope], axis=1)
        k_min = jnp.concatenate([up[:, 256:320], rope], axis=1)
        v_all[at : at + width, :] = jnp.concatenate([up[:, 128:256], up[:, 320:384]], axis=1)
        seen = k_pos <= q_pos
        found = []
        for q, k, scale, store, top in (
            (q_maj, k_maj, scale_maj, s_maj, tops[0]),
            (q_min, k_min, scale_min, s_min, tops[1]),
        ):
            s = jnp.where(seen, dot(q, k, ((1,), (1,))) * scale, MASKED)
            store[:, at : at + width] = s
            for i in range(width // 128):
                top = jnp.maximum(top, s[:, 128 * i : 128 * (i + 1)])
            found.append(top)
        return found

    col = lax.broadcasted_iota(jnp.int32, (1, CHUNK), 1)
    for n in range(N_CHUNK):
        lat_rows, rope_rows = [], []
        for t in range(n * PER, (n + 1) * PER):
            lat_rows.append(
                jnp.concatenate(
                    [keys[t, FAR_ROWS * k : FAR_ROWS * (k + 1), :] for k in range(4)], axis=1
                )
            )
            half = keys[t, 4 * FAR_ROWS :, :]
            rope_rows.append(jnp.concatenate([half[:, :64], half[:, 64:]], axis=0))
        lat = jnp.concatenate(lat_rows, axis=0)
        rope = jnp.concatenate(rope_rows, axis=0)
        inner = col % FAR_ROWS
        k_z = (z + NEAR[-1] + 1 + inner // ROWS) % N_Z
        k_pos = (2 * k_z + core) * TOK + ROWS * (n * PER + col // FAR_ROWS) + inner % ROWS
        tops = scored(CHUNK * n, CHUNK, lat, rope, k_pos, tops)
    for c in copies[3:]:
        c.wait()
    col = lax.broadcasted_iota(jnp.int32, (1, len(NEAR) * TOK), 1)
    k_pos = (2 * ((z + NEAR[0] + N_Z + col // TOK) % N_Z) + core) * TOK + col % TOK
    tops = scored(N_CHUNK * CHUNK, len(NEAR) * TOK, near[:, :512], near[:, 512:576], k_pos, tops)
    top_maj, top_min = tops
    m_maj = jnp.max(top_maj, axis=1, keepdims=True)
    m_min = jnp.max(top_min, axis=1, keepdims=True)
    sum_maj = jnp.zeros((2 * TOK, 128), F32)
    sum_min = jnp.zeros((2 * TOK, 128), F32)
    o_maj = jnp.zeros((2 * TOK, 128), F32)
    o_min = jnp.zeros((2 * TOK, 64), F32)
    step = 512
    for at in range(0, KEYS, step):
        p = jnp.exp(s_maj[:, at : at + step] - m_maj)
        r = jnp.exp(s_min[:, at : at + step] - m_min)
        for k in range(step // 128):
            sum_maj = sum_maj + p[:, 128 * k : 128 * (k + 1)]
            sum_min = sum_min + r[:, 128 * k : 128 * (k + 1)]
        v = v_all[at : at + step, :]
        o_maj = o_maj + dot(p.astype(BF16), v[:, :128])
        o_min = o_min + dot(r.astype(BF16), v[:, 128:192])
    l_maj = jnp.sum(sum_maj, axis=1, keepdims=True)
    l_min = jnp.sum(sum_min, axis=1, keepdims=True)
    lane = lax.broadcasted_iota(jnp.int32, (2 * TOK, 64), 1)
    stats = jnp.where(
        lane == 0, m_maj, jnp.where(lane == 1, l_maj, jnp.where(lane == 2, m_min, l_min))
    )
    result = jnp.concatenate([o_maj, o_min, stats], axis=1)
    own[...] = result[:TOK]
    other[...] = result[TOK:]


def project_body(a, b, out_maj, out_min, parts):
    a, b = a[...], b[...]

    def joined(m_at, lo, hi):
        m_a, m_b = a[:, m_at : m_at + 1], b[:, m_at : m_at + 1]
        l_a, l_b = a[:, m_at + 1 : m_at + 2], b[:, m_at + 1 : m_at + 2]
        top = jnp.maximum(m_a, m_b)
        f_a, f_b = jnp.exp(m_a - top), jnp.exp(m_b - top)
        total = l_a * f_a + l_b * f_b
        return ((a[:, lo:hi] * f_a + b[:, lo:hi] * f_b) / total).astype(BF16)

    attn_maj = joined(192, 0, 128)
    attn_min = joined(194, 128, 192)
    value = dot(attn_maj, out_maj[...]) + dot(attn_min, out_min[...])
    for t in range(N_TP):
        parts[t] = value[:, 128 * t : 128 * (t + 1)].astype(BF16)


def slot_columns(ids):
    lane = lax.broadcasted_iota(jnp.int32, (TOK, EXPERTS), 1)
    first = (ids[:, 0:1] == lane).astype(F32)
    second = (ids[:, 1:2] == lane).astype(F32)
    below = (
        lax.broadcasted_iota(jnp.int32, (TOK, TOK), 1) < lax.broadcasted_iota(jnp.int32, (TOK, TOK), 0)
    ).astype(BF16)
    earlier = dot(below, (first + second).astype(BF16))
    rank_0 = jnp.sum(first * earlier, axis=1, keepdims=True).astype(jnp.int32)
    rank_1 = jnp.sum(second * earlier, axis=1, keepdims=True).astype(jnp.int32)
    return ids[:, 0:1] * CAP + rank_0, ids[:, 1:2] * CAP + rank_1


def place_body(parts, residual, ids, stream, placed):
    slot_0, slot_1 = slot_columns(ids[...])
    lane = lax.broadcasted_iota(jnp.int32, (TOK, SLOTS), 1)
    select = ((lane == slot_0) | (lane == slot_1)).astype(BF16)
    summed = parts[0].astype(F32)
    for t in range(1, N_TP):
        summed = summed + parts[t].astype(F32)
    rows = (residual[...].astype(F32) + summed).astype(BF16)
    stream[...] = rows
    placed[...] = dot(select, rows, ((0,), (0,))).astype(BF16)


def pack_body(gate, up, down, low, high, sems):
    pairs = []
    for i, out in enumerate((low, high)):
        mine = pl.ds(128 * i, 128)
        pairs.append((gate.at[0, :, mine], out.at[pl.ds(0, D)]))
        pairs.append((up.at[0, :, mine], out.at[pl.ds(D, D)]))
        for t in range(N_TP):
            pairs.append((down.at[0, mine, pl.ds(128 * t, 128)], out.at[pl.ds(2 * D + 128 * t, 128)]))
    for c in fetch(pairs, sems):
        c.wait()


def assemble_body(gate_a, low, high, gate_w, sems):
    pairs = [(gate_a.at[0], gate_w.at[:, pl.ds(0, 256)])]
    for i, packed in enumerate((low, high)):
        pairs.append((packed.at[pl.ds(0, D)], gate_w.at[:, pl.ds(256 + 128 * i, 128)]))
    for c in fetch(pairs, sems):
        c.wait()


def expert_body(got, gain, gate_w, up_a, down_a, low, high, parts, up_w, down_w, x, sems):
    own = pl.ds(0, 256)
    pairs = [(up_a.at[0], up_w.at[:, own])]
    for i, packed in enumerate((low, high)):
        pairs.append((packed.at[pl.ds(D, D)], up_w.at[:, pl.ds(256 + 128 * i, 128)]))
    pairs.append((down_a.at[0], down_w.at[own]))
    for i, packed in enumerate((low, high)):
        for t in range(N_TP):
            mine, cols = pl.ds(256 + 128 * i, 128), pl.ds(128 * t, 128)
            pairs.append((packed.at[pl.ds(2 * D + 128 * t, 128)], down_w.at[mine, cols]))
    copies = fetch(pairs, sems)
    squares = jnp.zeros((HALF, 128), F32)
    gate = jnp.zeros((HALF, 512), F32)
    wide = 4
    for n in range(0, N_TP, wide):
        for t in range(n, n + wide):
            cols = slice(128 * t, 128 * (t + 1))
            v = got[t].astype(F32)
            squares = squares + v * v
            x[:, cols] = (v * gain[:, cols]).astype(BF16)
        cols = slice(128 * n, 128 * (n + wide))
        gate = gate + dot(x[:, cols], gate_w[cols, :])
    factor = lax.rsqrt(jnp.sum(squares, axis=1, keepdims=True) / D + NORM_EPS)
    for c in copies[:3]:
        c.wait()
    gate = gate * factor
    up = dot(x[...], up_w[...]) * factor
    hidden = (gate / (1.0 + jnp.exp(-gate)) * up).astype(BF16)
    for c in copies[3:]:
        c.wait()
    for t in range(0, N_TP, 2):
        value = dot(hidden, down_w[:, 128 * t : 128 * (t + 2)])
        parts[t] = value[:, :128].astype(BF16)
        parts[t + 1] = value[:, 128:].astype(BF16)


def gather_sum_body(parts, out):
    core = lax.axis_index("sp") % 2
    for half in range(2):
        total = jnp.zeros((HALF, 128), F32)
        for k in range(N_TP // 2):
            by_x = 2 * k + half
            by_y = (k // 4) * 8 + half * 4 + k % 4
            total = total + parts[jnp.where(core == 0, by_x, by_y)].astype(F32)
        out[half * HALF : (half + 1) * HALF, :] = total.astype(BF16)


def mix_body(returned, stream, ids, weights, out):
    slot_0, slot_1 = slot_columns(ids[...])
    lane = lax.broadcasted_iota(jnp.int32, (TOK, SLOTS), 1)
    rows = returned[...]
    w = weights[...]
    first = dot((lane == slot_0).astype(BF16), rows) * w[:, 0:1]
    second = dot((lane == slot_1).astype(BF16), rows) * w[:, 1:2]
    out[...] = (stream[...].astype(F32) + (first + second)).astype(BF16)


def shape(dims, kind=BF16):
    return pltpu.VMEM(dims, kind)


def room(dims, kind=BF16):
    return pltpu.VMEM(dims, kind)


def kernel(body, outs, rooms, sems, operands, near=()):
    single = not isinstance(outs, tuple)
    places = [pltpu.VMEM if i in near else pltpu.HBM for i in range(len(operands))]
    operands = [pltpu.with_memory_space_constraint(x, m) for x, m in zip(operands, places)]
    return pl.pallas_call(
        body,
        out_shape=outs,
        in_specs=[pl.BlockSpec(memory_space=m) for m in places],
        out_specs=vmem(1)[0] if single else tuple(vmem(len(outs))),
        scratch_shapes=rooms + ([pltpu.SemaphoreType.DMA((sems,))] if sems else []),
        compiler_params=pltpu.CompilerParams(vmem_limit_bytes=24 * 2**20),
    )(*operands)


def to_each(array, axis, groups=None):
    return lax.all_to_all(array, axis, 0, 0, tiled=True, axis_index_groups=groups)


def per_device(
    query_major,
    query_minor,
    latent_rows,
    rope_keys,
    key_up_major,
    value_up_major,
    key_up_minor,
    value_up_minor,
    out_major,
    out_minor,
    residual,
    norm_gain,
    expert_ids,
    expert_weights,
    gate_proj,
    up_proj,
    down_proj,
):
    table = jnp.asarray(TABLE)
    rows = kernel(
        rows_body,
        shape((N_Z, ROWS, 640)),
        [room((ROWS, LATENT)), room((ROPE, TOK)), room((160, 128), F32), room((TOK, ROPE), F32)],
        3,
        (latent_rows, rope_keys.T, table),
    )
    got_rows = to_each(rows, "sp", SAME_CORE)
    low, high = kernel(
        pack_body,
        (shape((3 * D, 128)), shape((3 * D, 128))),
        [],
        4 + 2 * N_TP,
        (gate_proj, up_proj, down_proj),
    )
    packed = kernel(
        choose_body, shape((PACKED, 128)), [room((FAR_ROWS, 640))], 0, (got_rows,), (0,)
    )
    spread = jnp.broadcast_to(packed, (N_TP, PACKED, 128))
    keys = to_each(spread, "tp")
    q_own, up_weights, own_block = kernel(
        queries_body,
        (shape((TOK, 320)), shape((LATENT, 384)), shape((TOK, 640))),
        [room((TOK, 128)), room((160, 128), F32), room((ROPE, TOK))],
        6,
        (
            query_major,
            query_minor,
            table,
            key_up_major,
            value_up_major,
            key_up_minor,
            value_up_minor,
            latent_rows,
            rope_keys.T,
        ),
        (0, 5, 6),
    )
    q_other = lax.ppermute(q_own, "sp", OTHER_CORE)
    blocks = [lax.ppermute(own_block, "sp", along_z(-step)) if step else own_block for step in NEAR]
    from_low = lax.ppermute(low, ("sp", "tp"), ring(1))
    from_high = lax.ppermute(high, ("sp", "tp"), ring(-1))
    own, other = kernel(
        attend_body,
        (shape((TOK, 256), F32), shape((TOK, 256), F32)),
        [
            room((2 * TOK, KEYS), F32),
            room((2 * TOK, KEYS), F32),
            room((KEYS, 192)),
            room((2 * TOK, 320)),
            room((LATENT, 384)),
            room((len(NEAR) * TOK, 640)),
        ],
        3 + len(NEAR),
        (keys, q_own, q_other, up_weights, *blocks),
        (0,),
    )
    from_other = lax.ppermute(other, "sp", OTHER_CORE)
    head_parts = kernel(
        project_body,
        shape((N_TP, TOK, 128)),
        [],
        0,
        (own, from_other, out_major, out_minor),
        range(4),
    )
    head_parts = to_each(head_parts, "tp")
    stream, placed = kernel(
        place_body,
        (shape((TOK, 128)), shape((SLOTS, 128))),
        [],
        0,
        (head_parts, residual, expert_ids),
        range(3),
    )
    arrived = to_each(placed.reshape(EXPERTS, CAP, 128), "sp").reshape(2, 1, HALF, 128)
    peers = jnp.arange(N_TP, dtype=jnp.int32)
    half_of = jnp.where(lax.axis_index("sp") % 2 == 0, peers % 2, (peers // 4) % 2)
    half_rows = jnp.where(half_of[:, None, None] == 0, arrived[0], arrived[1])
    everyone = to_each(half_rows, "tp")
    gate_w = kernel(assemble_body, shape((D, 512)), [], 3, (gate_proj, from_low, from_high))
    down_parts = kernel(
        expert_body,
        shape((N_TP, HALF, 128)),
        [room((D, 512)), room((512, D)), room((HALF, D))],
        4 + 2 * N_TP,
        (everyone, norm_gain.reshape(1, D), gate_w, up_proj, down_proj, from_low, from_high),
        (0, 1, 2),
    )
    down_parts = to_each(down_parts, "tp")
    expert_out = kernel(gather_sum_body, shape((SLOTS, 128)), [], 0, (down_parts,), (0,))
    returned = to_each(expert_out.reshape(EXPERTS, CAP, 128), "sp").reshape(SLOTS, 128)
    return kernel(
        mix_body,
        jax.ShapeDtypeStruct((TOK, 128), BF16),
        [],
        0,
        (returned, stream, expert_ids, expert_weights),
        range(4),
    )


def solution(mesh):
    in_specs = (
        P("sp", "tp"),
        P("sp", "tp"),
        P("sp", None),
        P("sp", None),
        P(None, "tp"),
        P(None, "tp"),
        P(None, "tp"),
        P(None, "tp"),
        P("tp", None),
        P("tp", None),
        P("sp", "tp"),
        P(),
        P("sp", None),
        P("sp", None),
        P("sp", None, "tp"),
        P("sp", None, "tp"),
        P("sp", "tp", None),
    )

    return jax.shard_map(
        per_device, mesh=mesh, in_specs=in_specs, out_specs=P("sp", "tp"), check_vma=False
    )
```

```python
import jax
import jax.numpy as jnp
import numpy as np
from jax import lax
from jax.experimental import pallas as pl
from jax.experimental.pallas import tpu as pltpu
from jax.sharding import PartitionSpec as P


F32 = jnp.float32
BF16 = jnp.bfloat16
D = 2048
ROPE = 64
NOPE_MAJOR = 128
NOPE_MINOR = 64
LATENT = 512
TOK = 128
N_TP = 16
N_Z = 16
EXPERTS = 32
CAP = 16
SLOTS = EXPERTS * CAP
ROWS = TOK // N_TP
KEYS = N_Z * TOK
MASKED = -1e30
NORM_EPS = 1e-6
HALF = SLOTS // 2
NEAR = (-2, -1, 0, 1, 2, 3)
FAR = N_Z - len(NEAR)
FAR_ROWS = FAR * ROWS
PACKED = 4 * FAR_ROWS + FAR_ROWS // 2


def along_z(step):
    moves = [(z, (z + step) % N_Z) for z in range(N_Z)]
    return [(a * 2 + c, b * 2 + c) for a, b in moves if a <= b for c in range(2)]


def turns(positions):
    angles = positions[:, None] * (1.0 / 10000.0 ** (np.arange(32) / 32.0))[None, :]
    return np.concatenate([np.cos(angles), np.sin(angles), np.zeros((len(positions), 64))], axis=1)


TABLE = np.concatenate([turns(np.arange(2 * N_Z) * float(TOK)), turns(np.arange(TOK) * 1.0)]).astype(
    np.float32
)

SAME_CORE = [[z * 2 + c for z in range(N_Z)] for c in range(2)]
OTHER_CORE = [(i, i ^ 1) for i in range(2 * N_Z)]


def ring(step):
    moves = []
    for s in range(2 * N_Z):
        for t in range(N_TP):
            y, x = divmod(t, 4)
            to = (y + step) % 4 * 4 + x if s % 2 else y * 4 + (x + step) % 4
            moves.append((s * N_TP + t, s * N_TP + to))
    return moves


HALF = SLOTS // 2
NEAR = (-2, -1, 0, 1, 2, 3)
FAR = N_Z - len(NEAR)
FAR_ROWS = FAR * ROWS
PACKED = 4 * FAR_ROWS + FAR_ROWS // 2


def along_z(step):
    moves = [(z, (z + step) % N_Z) for z in range(N_Z)]
    return [(a * 2 + c, b * 2 + c) for a, b in moves if a <= b for c in range(2)]


def turns(positions):
    angles = positions[:, None] * (1.0 / 10000.0 ** (np.arange(32) / 32.0))[None, :]
    return np.concatenate([np.cos(angles), np.sin(angles), np.zeros((len(positions), 64))], axis=1)


TABLE = np.concatenate([turns(np.arange(2 * N_Z) * float(TOK)), turns(np.arange(TOK) * 1.0)]).astype(
    np.float32
)

SAME_CORE = [[z * 2 + c for z in range(N_Z)] for c in range(2)]
OTHER_CORE = [(i, i ^ 1) for i in range(2 * N_Z)]


ANY = pl.BlockSpec(memory_space=pl.ANY)


def vmem(n):
    return [pl.BlockSpec(memory_space=pltpu.VMEM)] * n


def fetch(pairs, sems):
    copies = [pltpu.make_async_copy(src, dst, sems.at[i]) for i, (src, dst) in enumerate(pairs)]
    for c in copies:
        c.start()
    return copies


def dot(a, b, dims=((1,), (0,))):
    return lax.dot_general(a, b, (dims, ((), ())), preferred_element_type=F32)


def turn_at(table, block, rows):
    first = table[pl.ds(block, 1), :]
    c_0, s_0 = first[:, :32], first[:, 32:64]
    c_1, s_1 = rows[:, :32], rows[:, 32:64]
    return c_0 * c_1 - s_0 * s_1, s_0 * c_1 + c_0 * s_1


def turned(values, cosine, sine):
    low = values[:, :32].astype(F32)
    high = values[:, 32:].astype(F32)
    return jnp.concatenate(
        [low * cosine - high * sine, high * cosine + low * sine], axis=1
    ).astype(BF16)


def rows_body(lat_in, rope_in, table_in, out, lat, rope, table, by_row, sems):
    block, part = lax.axis_index("sp"), lax.axis_index("tp")
    mine = pl.ds(pl.multiple_of(part * ROWS, ROWS), ROWS)
    for c in fetch(((lat_in.at[mine], lat), (rope_in, rope), (table_in, table)), sems):
        c.wait()
    at = pl.ds(pl.multiple_of(2 * N_Z + part * ROWS, ROWS), ROWS)
    cosine, sine = turn_at(table, block, table[at, :])
    by_row[...] = rope[...].astype(F32).T
    key = turned(by_row[pl.ds(pl.multiple_of(part * ROWS, ROWS), ROWS), :], cosine, sine)
    row = jnp.concatenate([lat[...], key, jnp.zeros((ROWS, 64), BF16)], axis=1)
    for z in range(N_Z):
        out[z] = row


def queries_body(
    maj, low_in, table_in, ku_maj, vu_maj, ku_min, vu_min, lat, rope_in,
    out, weights, block,
    low, table, rope, sems,
):
    copies = fetch(
        (
            (low_in, low),
            (table_in, table),
            (rope_in, rope),
            (ku_maj, weights.at[:, pl.ds(0, 128)]),
            (vu_maj, weights.at[:, pl.ds(128, 128)]),
            (lat, block.at[:, pl.ds(0, LATENT)]),
        ),
        sems,
    )
    weights[:, 256:384] = jnp.concatenate([ku_min[...], vu_min[...]], axis=1)
    for c in copies[:3]:
        c.wait()
    c, s = turn_at(table, lax.axis_index("sp"), table[2 * N_Z :, :])
    key = turned(rope[...].astype(F32).T, c, s)
    block[:, LATENT:] = jnp.concatenate([key, jnp.zeros((TOK, 64), BF16)], axis=1)
    out[...] = jnp.concatenate(
        [
            maj[:, :NOPE_MAJOR],
            turned(maj[:, NOPE_MAJOR:], c, s),
            low[:, :NOPE_MINOR],
            turned(low[:, NOPE_MINOR:], c, s),
        ],
        axis=1,
    )
    for c in copies[3:]:
        c.wait()


def choose_body(got, out, flat):
    z = lax.axis_index("sp") // 2
    for o in range(FAR):
        flat[ROWS * o : ROWS * (o + 1), :] = got[(z + NEAR[-1] + 1 + o) % N_Z]
    for k in range(4):
        out[FAR_ROWS * k : FAR_ROWS * (k + 1), :] = flat[:, 128 * k : 128 * (k + 1)]
    rope = flat[:, 512:576]
    out[4 * FAR_ROWS :, :] = jnp.concatenate([rope[: FAR_ROWS // 2], rope[FAR_ROWS // 2 :]], axis=1)


PER = 8
CHUNK = PER * FAR_ROWS
N_CHUNK = N_TP // PER


def attend_body(keys, q_own_in, q_other_in, up_in, *refs):
    near_in = refs[: len(NEAR)]
    own, other, s_maj, s_min, v_all, q_all, up_weights, near, sems = refs[len(NEAR) :]
    copies = fetch(
        (
            (up_in, up_weights),
            (q_own_in, q_all.at[pl.ds(0, TOK)]),
            (q_other_in, q_all.at[pl.ds(TOK, TOK)]),
        )
        + tuple((b, near.at[pl.ds(TOK * i, TOK)]) for i, b in enumerate(near_in)),
        sems,
    )
    me = lax.axis_index("sp")
    core, z = me % 2, me // 2
    row = lax.broadcasted_iota(jnp.int32, (2 * TOK, 1), 0)
    q_pos = jnp.where(row < TOK, me * TOK + row, (me + 1 - 2 * core) * TOK + row - TOK)
    scale_maj = (NOPE_MAJOR + ROPE) ** -0.5
    scale_min = (NOPE_MINOR + ROPE) ** -0.5
    tops = [jnp.full((2 * TOK, 128), MASKED, F32)] * 2
    for c in copies[:3]:
        c.wait()
    weights = up_weights[...]
    q_maj, q_min = q_all[:, :192], q_all[:, 192:320]

    def scored(at, width, lat, rope, k_pos, tops):
        up = dot(lat, weights).astype(BF16)
        k_maj = jnp.concatenate([up[:, :128], rope], axis=1)
        k_min = jnp.concatenate([up[:, 256:320], rope], axis=1)
        v_all[at : at + width, :] = jnp.concatenate([up[:, 128:256], up[:, 320:384]], axis=1)
        seen = k_pos <= q_pos
        found = []
        for q, k, scale, store, top in (
            (q_maj, k_maj, scale_maj, s_maj, tops[0]),
            (q_min, k_min, scale_min, s_min, tops[1]),
        ):
            s = jnp.where(seen, dot(q, k, ((1,), (1,))) * scale, MASKED)
            store[:, at : at + width] = s
            for i in range(width // 128):
                top = jnp.maximum(top, s[:, 128 * i : 128 * (i + 1)])
            found.append(top)
        return found

    col = lax.broadcasted_iota(jnp.int32, (1, CHUNK), 1)
    for n in range(N_CHUNK):
        lat_rows, rope_rows = [], []
        for t in range(n * PER, (n + 1) * PER):
            lat_rows.append(
                jnp.concatenate(
                    [keys[t, FAR_ROWS * k : FAR_ROWS * (k + 1), :] for k in range(4)], axis=1
                )
            )
            half = keys[t, 4 * FAR_ROWS :, :]
            rope_rows.append(jnp.concatenate([half[:, :64], half[:, 64:]], axis=0))
        lat = jnp.concatenate(lat_rows, axis=0)
        rope = jnp.concatenate(rope_rows, axis=0)
        inner = col % FAR_ROWS
        k_z = (z + NEAR[-1] + 1 + inner // ROWS) % N_Z
        k_pos = (2 * k_z + core) * TOK + ROWS * (n * PER + col // FAR_ROWS) + inner % ROWS
        tops = scored(CHUNK * n, CHUNK, lat, rope, k_pos, tops)
    for c in copies[3:]:
        c.wait()
    col = lax.broadcasted_iota(jnp.int32, (1, len(NEAR) * TOK), 1)
    k_pos = (2 * ((z + NEAR[0] + N_Z + col // TOK) % N_Z) + core) * TOK + col % TOK
    tops = scored(N_CHUNK * CHUNK, len(NEAR) * TOK, near[:, :512], near[:, 512:576], k_pos, tops)
    top_maj, top_min = tops
    m_maj = jnp.max(top_maj, axis=1, keepdims=True)
    m_min = jnp.max(top_min, axis=1, keepdims=True)
    sum_maj = jnp.zeros((2 * TOK, 128), F32)
    sum_min = jnp.zeros((2 * TOK, 128), F32)
    o_maj = jnp.zeros((2 * TOK, 128), F32)
    o_min = jnp.zeros((2 * TOK, 64), F32)
    step = 512
    for at in range(0, KEYS, step):
        p = jnp.exp(s_maj[:, at : at + step] - m_maj)
        r = jnp.exp(s_min[:, at : at + step] - m_min)
        for k in range(step // 128):
            sum_maj = sum_maj + p[:, 128 * k : 128 * (k + 1)]
            sum_min = sum_min + r[:, 128 * k : 128 * (k + 1)]
        v = v_all[at : at + step, :]
        o_maj = o_maj + dot(p.astype(BF16), v[:, :128])
        o_min = o_min + dot(r.astype(BF16), v[:, 128:192])
    l_maj = jnp.sum(sum_maj, axis=1, keepdims=True)
    l_min = jnp.sum(sum_min, axis=1, keepdims=True)
    lane = lax.broadcasted_iota(jnp.int32, (2 * TOK, 64), 1)
    stats = jnp.where(
        lane == 0, m_maj, jnp.where(lane == 1, l_maj, jnp.where(lane == 2, m_min, l_min))
    )
    result = jnp.concatenate([o_maj, o_min, stats], axis=1)
    own[...] = result[:TOK]
    other[...] = result[TOK:]


def project_body(a, b, out_maj, out_min, parts):
    a, b = a[...], b[...]

    def joined(m_at, lo, hi):
        m_a, m_b = a[:, m_at : m_at + 1], b[:, m_at : m_at + 1]
        l_a, l_b = a[:, m_at + 1 : m_at + 2], b[:, m_at + 1 : m_at + 2]
        top = jnp.maximum(m_a, m_b)
        f_a, f_b = jnp.exp(m_a - top), jnp.exp(m_b - top)
        total = l_a * f_a + l_b * f_b
        return ((a[:, lo:hi] * f_a + b[:, lo:hi] * f_b) / total).astype(BF16)

    attn_maj = joined(192, 0, 128)
    attn_min = joined(194, 128, 192)
    value = dot(attn_maj, out_maj[...]) + dot(attn_min, out_min[...])
    for t in range(N_TP):
        parts[t] = value[:, 128 * t : 128 * (t + 1)].astype(BF16)


def slot_columns(ids):
    lane = lax.broadcasted_iota(jnp.int32, (TOK, EXPERTS), 1)
    first = (ids[:, 0:1] == lane).astype(F32)
    second = (ids[:, 1:2] == lane).astype(F32)
    below = (
        lax.broadcasted_iota(jnp.int32, (TOK, TOK), 1) < lax.broadcasted_iota(jnp.int32, (TOK, TOK), 0)
    ).astype(BF16)
    earlier = dot(below, (first + second).astype(BF16))
    rank_0 = jnp.sum(first * earlier, axis=1, keepdims=True).astype(jnp.int32)
    rank_1 = jnp.sum(second * earlier, axis=1, keepdims=True).astype(jnp.int32)
    return ids[:, 0:1] * CAP + rank_0, ids[:, 1:2] * CAP + rank_1


def place_body(parts, residual, ids, stream, placed):
    slot_0, slot_1 = slot_columns(ids[...])
    lane = lax.broadcasted_iota(jnp.int32, (TOK, SLOTS), 1)
    select = ((lane == slot_0) | (lane == slot_1)).astype(BF16)
    summed = parts[0].astype(F32)
    for t in range(1, N_TP):
        summed = summed + parts[t].astype(F32)
    rows = (residual[...].astype(F32) + summed).astype(BF16)
    stream[...] = rows
    placed[...] = dot(select, rows, ((0,), (0,))).astype(BF16)


def pack_body(gate, up, down, low, high, sems):
    pairs = []
    for i, out in enumerate((low, high)):
        mine = pl.ds(128 * i, 128)
        pairs.append((gate.at[0, :, mine], out.at[pl.ds(0, D)]))
        pairs.append((up.at[0, :, mine], out.at[pl.ds(D, D)]))
        for t in range(N_TP):
            pairs.append((down.at[0, mine, pl.ds(128 * t, 128)], out.at[pl.ds(2 * D + 128 * t, 128)]))
    for c in fetch(pairs, sems):
        c.wait()


def assemble_body(gate_a, low, high, gate_w, sems):
    pairs = [(gate_a.at[0], gate_w.at[:, pl.ds(0, 256)])]
    for i, packed in enumerate((low, high)):
        pairs.append((packed.at[pl.ds(0, D)], gate_w.at[:, pl.ds(256 + 128 * i, 128)]))
    for c in fetch(pairs, sems):
        c.wait()


def expert_body(got, gain, gate_w, up_a, down_a, low, high, out, up_w, down_w, x, parts, sems, out_sems):
    own = pl.ds(0, 256)
    pairs = [(up_a.at[0], up_w.at[:, own])]
    for i, packed in enumerate((low, high)):
        pairs.append((packed.at[pl.ds(D, D)], up_w.at[:, pl.ds(256 + 128 * i, 128)]))
    pairs.append((down_a.at[0], down_w.at[own]))
    for i, packed in enumerate((low, high)):
        for t in range(N_TP):
            mine, cols = pl.ds(256 + 128 * i, 128), pl.ds(128 * t, 128)
            pairs.append((packed.at[pl.ds(2 * D + 128 * t, 128)], down_w.at[mine, cols]))
    copies = fetch(pairs, sems)
    squares = jnp.zeros((HALF, 128), F32)
    gate = jnp.zeros((HALF, 512), F32)
    wide = 4
    for n in range(0, N_TP, wide):
        for t in range(n, n + wide):
            cols = slice(128 * t, 128 * (t + 1))
            v = got[t].astype(F32)
            squares = squares + v * v
            x[:, cols] = (v * gain[:, cols]).astype(BF16)
        cols = slice(128 * n, 128 * (n + wide))
        gate = gate + dot(x[:, cols], gate_w[cols, :])
    factor = lax.rsqrt(jnp.sum(squares, axis=1, keepdims=True) / D + NORM_EPS)
    for c in copies[:3]:
        c.wait()
    gate = gate * factor
    up = dot(x[...], up_w[...]) * factor
    hidden = (gate / (1.0 + jnp.exp(-gate)) * up).astype(BF16)
    for c in copies[3:]:
        c.wait()
    leaving = []
    for t in range(0, N_TP, 4):
        value = dot(hidden, down_w[:, 128 * t : 128 * (t + 4)])
        for k in range(4):
            parts[t + k] = value[:, 128 * k : 128 * (k + 1)].astype(BF16)
        group = pl.ds(t, 4)
        leaving.append(pltpu.make_async_copy(parts.at[group], out.at[group], out_sems.at[t // 4]))
        leaving[-1].start()
    for c in leaving:
        c.wait()


def gather_sum_body(parts, out):
    core = lax.axis_index("sp") % 2
    for half in range(2):
        total = jnp.zeros((HALF, 128), F32)
        for k in range(N_TP // 2):
            by_x = 2 * k + half
            by_y = (k // 4) * 8 + half * 4 + k % 4
            total = total + parts[jnp.where(core == 0, by_x, by_y)].astype(F32)
        out[half * HALF : (half + 1) * HALF, :] = total.astype(BF16)


def mix_body(returned, stream, ids, weights, out):
    slot_0, slot_1 = slot_columns(ids[...])
    lane = lax.broadcasted_iota(jnp.int32, (TOK, SLOTS), 1)
    rows = returned[...]
    w = weights[...]
    first = dot((lane == slot_0).astype(BF16), rows) * w[:, 0:1]
    second = dot((lane == slot_1).astype(BF16), rows) * w[:, 1:2]
    out[...] = (stream[...].astype(F32) + (first + second)).astype(BF16)


def shape(dims, kind=BF16):
    return pltpu.VMEM(dims, kind)


def room(dims, kind=BF16):
    return pltpu.VMEM(dims, kind)


def kernel(body, outs, rooms, sems, operands, near=(), out_spec=None):
    single = not isinstance(outs, tuple)
    places = [pltpu.VMEM if i in near else pltpu.HBM for i in range(len(operands))]
    operands = [pltpu.with_memory_space_constraint(x, m) for x, m in zip(operands, places)]
    return pl.pallas_call(
        body,
        out_shape=outs,
        in_specs=[pl.BlockSpec(memory_space=m) for m in places],
        out_specs=(out_spec or vmem(1)[0]) if single else tuple(vmem(len(outs))),
        scratch_shapes=rooms + [pltpu.SemaphoreType.DMA((n,)) for n in np.atleast_1d(sems).tolist() if n],
        compiler_params=pltpu.CompilerParams(vmem_limit_bytes=24 * 2**20),
    )(*operands)


def to_each(array, axis, groups=None):
    return lax.all_to_all(array, axis, 0, 0, tiled=True, axis_index_groups=groups)


def per_device(
    query_major,
    query_minor,
    latent_rows,
    rope_keys,
    key_up_major,
    value_up_major,
    key_up_minor,
    value_up_minor,
    out_major,
    out_minor,
    residual,
    norm_gain,
    expert_ids,
    expert_weights,
    gate_proj,
    up_proj,
    down_proj,
):
    table = jnp.asarray(TABLE)
    rows = kernel(
        rows_body,
        shape((N_Z, ROWS, 640)),
        [room((ROWS, LATENT)), room((ROPE, TOK)), room((160, 128), F32), room((TOK, ROPE), F32)],
        3,
        (latent_rows, rope_keys.T, table),
    )
    got_rows = to_each(rows, "sp", SAME_CORE)
    low, high = kernel(
        pack_body,
        (shape((3 * D, 128)), shape((3 * D, 128))),
        [],
        4 + 2 * N_TP,
        (gate_proj, up_proj, down_proj),
    )
    packed = kernel(
        choose_body, shape((PACKED, 128)), [room((FAR_ROWS, 640))], 0, (got_rows,), (0,)
    )
    spread = jnp.broadcast_to(packed, (N_TP, PACKED, 128))
    keys = to_each(spread, "tp")
    q_own, up_weights, own_block = kernel(
        queries_body,
        (shape((TOK, 320)), shape((LATENT, 384)), shape((TOK, 640))),
        [room((TOK, 128)), room((160, 128), F32), room((ROPE, TOK))],
        6,
        (
            query_major,
            query_minor,
            table,
            key_up_major,
            value_up_major,
            key_up_minor,
            value_up_minor,
            latent_rows,
            rope_keys.T,
        ),
        (0, 5, 6),
    )
    q_other = lax.ppermute(q_own, "sp", OTHER_CORE)
    blocks = [lax.ppermute(own_block, "sp", along_z(-step)) if step else own_block for step in NEAR]
    from_low = lax.ppermute(low, ("sp", "tp"), ring(1))
    from_high = lax.ppermute(high, ("sp", "tp"), ring(-1))
    own, other = kernel(
        attend_body,
        (shape((TOK, 256), F32), shape((TOK, 256), F32)),
        [
            room((2 * TOK, KEYS), F32),
            room((2 * TOK, KEYS), F32),
            room((KEYS, 192)),
            room((2 * TOK, 320)),
            room((LATENT, 384)),
            room((len(NEAR) * TOK, 640)),
        ],
        3 + len(NEAR),
        (keys, q_own, q_other, up_weights, *blocks),
        (0,),
    )
    from_other = lax.ppermute(other, "sp", OTHER_CORE)
    head_parts = kernel(
        project_body,
        shape((N_TP, TOK, 128)),
        [],
        0,
        (own, from_other, out_major, out_minor),
        range(4),
    )
    head_parts = to_each(head_parts, "tp")
    stream, placed = kernel(
        place_body,
        (shape((TOK, 128)), shape((SLOTS, 128))),
        [],
        0,
        (head_parts, residual, expert_ids),
        range(3),
    )
    arrived = to_each(placed.reshape(EXPERTS, CAP, 128), "sp").reshape(2, 1, HALF, 128)
    peers = jnp.arange(N_TP, dtype=jnp.int32)
    half_of = jnp.where(lax.axis_index("sp") % 2 == 0, peers % 2, (peers // 4) % 2)
    half_rows = jnp.where(half_of[:, None, None] == 0, arrived[0], arrived[1])
    everyone = to_each(half_rows, "tp")
    gate_w = kernel(assemble_body, shape((D, 512)), [], 3, (gate_proj, from_low, from_high))
    down_parts = kernel(
        expert_body,
        jax.ShapeDtypeStruct((N_TP, HALF, 128), BF16),
        [room((D, 512)), room((512, D)), room((HALF, D)), room((N_TP, HALF, 128))],
        (4 + 2 * N_TP, N_TP // 4),
        (everyone, norm_gain.reshape(1, D), gate_w, up_proj, down_proj, from_low, from_high),
        (0, 1, 2),
        ANY,
    )
    down_parts = to_each(down_parts, "tp")
    expert_out = kernel(gather_sum_body, shape((SLOTS, 128)), [], 0, (down_parts,), (0,))
    returned = to_each(expert_out.reshape(EXPERTS, CAP, 128), "sp").reshape(SLOTS, 128)
    return kernel(
        mix_body,
        jax.ShapeDtypeStruct((TOK, 128), BF16),
        [],
        0,
        (returned, stream, expert_ids, expert_weights),
        range(4),
    )


def solution(mesh):
    in_specs = (
        P("sp", "tp"),
        P("sp", "tp"),
        P("sp", None),
        P("sp", None),
        P(None, "tp"),
        P(None, "tp"),
        P(None, "tp"),
        P(None, "tp"),
        P("tp", None),
        P("tp", None),
        P("sp", "tp"),
        P(),
        P("sp", None),
        P("sp", None),
        P("sp", None, "tp"),
        P("sp", None, "tp"),
        P("sp", "tp", None),
    )

    return jax.shard_map(
        per_device, mesh=mesh, in_specs=in_specs, out_specs=P("sp", "tp"), check_vma=False
    )
```

```python
import jax
import jax.numpy as jnp
import numpy as np
from jax import lax
from jax.experimental import pallas as pl
from jax.experimental.pallas import tpu as pltpu
from jax.sharding import PartitionSpec as P


F32 = jnp.float32
BF16 = jnp.bfloat16
D = 2048
ROPE = 64
NOPE_MAJOR = 128
NOPE_MINOR = 64
LATENT = 512
TOK = 128
N_TP = 16
N_Z = 16
EXPERTS = 32
CAP = 16
SLOTS = EXPERTS * CAP
ROWS = TOK // N_TP
KEYS = N_Z * TOK
MASKED = -1e30
NORM_EPS = 1e-6
HALF = SLOTS // 2
NEAR = (-2, -1, 0, 1)
FAR = N_Z - len(NEAR)
FAR_ROWS = FAR * ROWS
PACKED = 4 * FAR_ROWS + FAR_ROWS // 2


def along_z(step):
    moves = [(z, (z + step) % N_Z) for z in range(N_Z)]
    return [(a * 2 + c, b * 2 + c) for a, b in moves if a <= b for c in range(2)]


def turns(positions):
    angles = positions[:, None] * (1.0 / 10000.0 ** (np.arange(32) / 32.0))[None, :]
    return np.concatenate([np.cos(angles), np.sin(angles), np.zeros((len(positions), 64))], axis=1)


TABLE = np.concatenate([turns(np.arange(2 * N_Z) * float(TOK)), turns(np.arange(TOK) * 1.0)]).astype(
    np.float32
)

SAME_CORE = [[z * 2 + c for z in range(N_Z)] for c in range(2)]
OTHER_CORE = [(i, i ^ 1) for i in range(2 * N_Z)]


def ring(step):
    moves = []
    for s in range(2 * N_Z):
        for t in range(N_TP):
            y, x = divmod(t, 4)
            to = (y + step) % 4 * 4 + x if s % 2 else y * 4 + (x + step) % 4
            moves.append((s * N_TP + t, s * N_TP + to))
    return moves


HALF = SLOTS // 2
NEAR = (-2, -1, 0, 1)
FAR = N_Z - len(NEAR)
FAR_ROWS = FAR * ROWS
PACKED = 4 * FAR_ROWS + FAR_ROWS // 2


def along_z(step):
    moves = [(z, (z + step) % N_Z) for z in range(N_Z)]
    return [(a * 2 + c, b * 2 + c) for a, b in moves if a <= b for c in range(2)]


def turns(positions):
    angles = positions[:, None] * (1.0 / 10000.0 ** (np.arange(32) / 32.0))[None, :]
    return np.concatenate([np.cos(angles), np.sin(angles), np.zeros((len(positions), 64))], axis=1)


TABLE = np.concatenate([turns(np.arange(2 * N_Z) * float(TOK)), turns(np.arange(TOK) * 1.0)]).astype(
    np.float32
)

SAME_CORE = [[z * 2 + c for z in range(N_Z)] for c in range(2)]
OTHER_CORE = [(i, i ^ 1) for i in range(2 * N_Z)]


ANY = pl.BlockSpec(memory_space=pl.ANY)


def vmem(n):
    return [pl.BlockSpec(memory_space=pltpu.VMEM)] * n


def fetch(pairs, sems):
    copies = [pltpu.make_async_copy(src, dst, sems.at[i]) for i, (src, dst) in enumerate(pairs)]
    for c in copies:
        c.start()
    return copies


def dot(a, b, dims=((1,), (0,))):
    return lax.dot_general(a, b, (dims, ((), ())), preferred_element_type=F32)


def turn_at(table, block, rows):
    first = table[pl.ds(block, 1), :]
    c_0, s_0 = first[:, :32], first[:, 32:64]
    c_1, s_1 = rows[:, :32], rows[:, 32:64]
    return c_0 * c_1 - s_0 * s_1, s_0 * c_1 + c_0 * s_1


def turned(values, cosine, sine):
    low = values[:, :32].astype(F32)
    high = values[:, 32:].astype(F32)
    return jnp.concatenate(
        [low * cosine - high * sine, high * cosine + low * sine], axis=1
    ).astype(BF16)


def rows_body(lat_in, rope_in, table_in, out, lat, rope, table, by_row, sems):
    block, part = lax.axis_index("sp"), lax.axis_index("tp")
    mine = pl.ds(pl.multiple_of(part * ROWS, ROWS), ROWS)
    for c in fetch(((lat_in.at[mine], lat), (rope_in, rope), (table_in, table)), sems):
        c.wait()
    at = pl.ds(pl.multiple_of(2 * N_Z + part * ROWS, ROWS), ROWS)
    cosine, sine = turn_at(table, block, table[at, :])
    by_row[...] = rope[...].astype(F32).T
    key = turned(by_row[pl.ds(pl.multiple_of(part * ROWS, ROWS), ROWS), :], cosine, sine)
    row = jnp.concatenate([lat[...], key, jnp.zeros((ROWS, 64), BF16)], axis=1)
    for z in range(N_Z):
        out[z] = row


def queries_body(
    maj, low_in, table_in, ku_maj, vu_maj, ku_min, vu_min, lat, rope_in,
    out, weights, block,
    low, table, rope, sems,
):
    copies = fetch(
        (
            (low_in, low),
            (table_in, table),
            (rope_in, rope),
            (ku_maj, weights.at[:, pl.ds(0, 128)]),
            (vu_maj, weights.at[:, pl.ds(128, 128)]),
            (lat, block.at[:, pl.ds(0, LATENT)]),
        ),
        sems,
    )
    weights[:, 256:384] = jnp.concatenate([ku_min[...], vu_min[...]], axis=1)
    for c in copies[:3]:
        c.wait()
    c, s = turn_at(table, lax.axis_index("sp"), table[2 * N_Z :, :])
    key = turned(rope[...].astype(F32).T, c, s)
    block[:, LATENT:] = jnp.concatenate([key, jnp.zeros((TOK, 64), BF16)], axis=1)
    out[...] = jnp.concatenate(
        [
            maj[:, :NOPE_MAJOR],
            turned(maj[:, NOPE_MAJOR:], c, s),
            low[:, :NOPE_MINOR],
            turned(low[:, NOPE_MINOR:], c, s),
        ],
        axis=1,
    )
    for c in copies[3:]:
        c.wait()


def choose_body(got, out, flat):
    z = lax.axis_index("sp") // 2
    for o in range(FAR):
        flat[ROWS * o : ROWS * (o + 1), :] = got[(z + NEAR[-1] + 1 + o) % N_Z]
    for k in range(4):
        out[FAR_ROWS * k : FAR_ROWS * (k + 1), :] = flat[:, 128 * k : 128 * (k + 1)]
    rope = flat[:, 512:576]
    out[4 * FAR_ROWS :, :] = jnp.concatenate([rope[: FAR_ROWS // 2], rope[FAR_ROWS // 2 :]], axis=1)


PER = 4
CHUNK = PER * FAR_ROWS
N_CHUNK = N_TP // PER


def attend_body(keys, q_own_in, q_other_in, up_in, *refs):
    near_in = refs[: len(NEAR)]
    own, other, s_maj, s_min, v_all, q_all, up_weights, near, sems = refs[len(NEAR) :]
    copies = fetch(
        (
            (up_in, up_weights),
            (q_own_in, q_all.at[pl.ds(0, TOK)]),
            (q_other_in, q_all.at[pl.ds(TOK, TOK)]),
        )
        + tuple((b, near.at[pl.ds(TOK * i, TOK)]) for i, b in enumerate(near_in)),
        sems,
    )
    me = lax.axis_index("sp")
    core, z = me % 2, me // 2
    row = lax.broadcasted_iota(jnp.int32, (2 * TOK, 1), 0)
    q_pos = jnp.where(row < TOK, me * TOK + row, (me + 1 - 2 * core) * TOK + row - TOK)
    scale_maj = (NOPE_MAJOR + ROPE) ** -0.5
    scale_min = (NOPE_MINOR + ROPE) ** -0.5
    tops = [jnp.full((2 * TOK, 128), MASKED, F32)] * 2
    for c in copies[:3]:
        c.wait()
    weights = up_weights[...]
    q_maj, q_min = q_all[:, :192], q_all[:, 192:320]

    def scored(at, width, lat, rope, k_pos, tops):
        up = dot(lat, weights).astype(BF16)
        k_maj = jnp.concatenate([up[:, :128], rope], axis=1)
        k_min = jnp.concatenate([up[:, 256:320], rope], axis=1)
        v_all[at : at + width, :] = jnp.concatenate([up[:, 128:256], up[:, 320:384]], axis=1)
        seen = k_pos <= q_pos
        found = []
        for q, k, scale, store, top in (
            (q_maj, k_maj, scale_maj, s_maj, tops[0]),
            (q_min, k_min, scale_min, s_min, tops[1]),
        ):
            s = jnp.where(seen, dot(q, k, ((1,), (1,))) * scale, MASKED)
            store[:, at : at + width] = s
            for i in range(width // 128):
                top = jnp.maximum(top, s[:, 128 * i : 128 * (i + 1)])
            found.append(top)
        return found

    col = lax.broadcasted_iota(jnp.int32, (1, CHUNK), 1)
    for n in range(N_CHUNK):
        lat_rows, rope_rows = [], []
        for t in range(n * PER, (n + 1) * PER):
            lat_rows.append(
                jnp.concatenate(
                    [keys[t, FAR_ROWS * k : FAR_ROWS * (k + 1), :] for k in range(4)], axis=1
                )
            )
            half = keys[t, 4 * FAR_ROWS :, :]
            rope_rows.append(jnp.concatenate([half[:, :64], half[:, 64:]], axis=0))
        lat = jnp.concatenate(lat_rows, axis=0)
        rope = jnp.concatenate(rope_rows, axis=0)
        inner = col % FAR_ROWS
        k_z = (z + NEAR[-1] + 1 + inner // ROWS) % N_Z
        k_pos = (2 * k_z + core) * TOK + ROWS * (n * PER + col // FAR_ROWS) + inner % ROWS
        tops = scored(CHUNK * n, CHUNK, lat, rope, k_pos, tops)
    for c in copies[3:]:
        c.wait()
    col = lax.broadcasted_iota(jnp.int32, (1, len(NEAR) * TOK), 1)
    k_pos = (2 * ((z + NEAR[0] + N_Z + col // TOK) % N_Z) + core) * TOK + col % TOK
    tops = scored(N_CHUNK * CHUNK, len(NEAR) * TOK, near[:, :512], near[:, 512:576], k_pos, tops)
    top_maj, top_min = tops
    m_maj = jnp.max(top_maj, axis=1, keepdims=True)
    m_min = jnp.max(top_min, axis=1, keepdims=True)
    sum_maj = jnp.zeros((2 * TOK, 128), F32)
    sum_min = jnp.zeros((2 * TOK, 128), F32)
    o_maj = jnp.zeros((2 * TOK, 128), F32)
    o_min = jnp.zeros((2 * TOK, 64), F32)
    step = 512
    for at in range(0, KEYS, step):
        p = jnp.exp(s_maj[:, at : at + step] - m_maj)
        r = jnp.exp(s_min[:, at : at + step] - m_min)
        for k in range(step // 128):
            sum_maj = sum_maj + p[:, 128 * k : 128 * (k + 1)]
            sum_min = sum_min + r[:, 128 * k : 128 * (k + 1)]
        v = v_all[at : at + step, :]
        o_maj = o_maj + dot(p.astype(BF16), v[:, :128])
        o_min = o_min + dot(r.astype(BF16), v[:, 128:192])
    l_maj = jnp.sum(sum_maj, axis=1, keepdims=True)
    l_min = jnp.sum(sum_min, axis=1, keepdims=True)
    lane = lax.broadcasted_iota(jnp.int32, (2 * TOK, 64), 1)
    stats = jnp.where(
        lane == 0, m_maj, jnp.where(lane == 1, l_maj, jnp.where(lane == 2, m_min, l_min))
    )
    result = jnp.concatenate([o_maj, o_min, stats], axis=1)
    own[...] = result[:TOK]
    other[...] = result[TOK:]


def project_body(a, b, out_maj, out_min, parts):
    a, b = a[...], b[...]

    def joined(m_at, lo, hi):
        m_a, m_b = a[:, m_at : m_at + 1], b[:, m_at : m_at + 1]
        l_a, l_b = a[:, m_at + 1 : m_at + 2], b[:, m_at + 1 : m_at + 2]
        top = jnp.maximum(m_a, m_b)
        f_a, f_b = jnp.exp(m_a - top), jnp.exp(m_b - top)
        total = l_a * f_a + l_b * f_b
        return ((a[:, lo:hi] * f_a + b[:, lo:hi] * f_b) / total).astype(BF16)

    attn_maj = joined(192, 0, 128)
    attn_min = joined(194, 128, 192)
    value = dot(attn_maj, out_maj[...]) + dot(attn_min, out_min[...])
    for t in range(N_TP):
        parts[t] = value[:, 128 * t : 128 * (t + 1)].astype(BF16)


def slot_columns(ids):
    lane = lax.broadcasted_iota(jnp.int32, (TOK, EXPERTS), 1)
    first = (ids[:, 0:1] == lane).astype(F32)
    second = (ids[:, 1:2] == lane).astype(F32)
    below = (
        lax.broadcasted_iota(jnp.int32, (TOK, TOK), 1) < lax.broadcasted_iota(jnp.int32, (TOK, TOK), 0)
    ).astype(BF16)
    earlier = dot(below, (first + second).astype(BF16))
    rank_0 = jnp.sum(first * earlier, axis=1, keepdims=True).astype(jnp.int32)
    rank_1 = jnp.sum(second * earlier, axis=1, keepdims=True).astype(jnp.int32)
    return ids[:, 0:1] * CAP + rank_0, ids[:, 1:2] * CAP + rank_1


def place_body(parts, residual, ids, stream, placed):
    slot_0, slot_1 = slot_columns(ids[...])
    lane = lax.broadcasted_iota(jnp.int32, (TOK, SLOTS), 1)
    select = ((lane == slot_0) | (lane == slot_1)).astype(BF16)
    summed = parts[0].astype(F32)
    for t in range(1, N_TP):
        summed = summed + parts[t].astype(F32)
    rows = (residual[...].astype(F32) + summed).astype(BF16)
    stream[...] = rows
    placed[...] = dot(select, rows, ((0,), (0,))).astype(BF16)


def pack_body(gate, up, down, low, high, sems):
    pairs = []
    for i, out in enumerate((low, high)):
        mine = pl.ds(128 * i, 128)
        pairs.append((gate.at[0, :, mine], out.at[pl.ds(0, D)]))
        pairs.append((up.at[0, :, mine], out.at[pl.ds(D, D)]))
        for t in range(N_TP):
            pairs.append((down.at[0, mine, pl.ds(128 * t, 128)], out.at[pl.ds(2 * D + 128 * t, 128)]))
    for c in fetch(pairs, sems):
        c.wait()


def weights_here_body(low, high, out):
    out[...] = jnp.zeros(out.shape, F32)


def halves_body(arrived, here, out):
    core = lax.axis_index("sp") % 2
    for d in range(N_TP):
        half = jnp.where(core == 0, d % 2, d // 4 % 2)
        out[d] = arrived[pl.ds(pl.multiple_of(half * HALF, HALF), HALF), :]


def expert_body(got, gain, gate_a, up_a, down_a, low, high, parts, gate_w, up_w, down_w, x, sems):
    own = pl.ds(0, 256)
    pairs = []
    for at, (mine, w) in enumerate(((gate_a, gate_w), (up_a, up_w))):
        pairs.append((mine.at[0], w.at[:, own]))
        for i, packed in enumerate((low, high)):
            pairs.append((packed.at[pl.ds(at * D, D)], w.at[:, pl.ds(256 + 128 * i, 128)]))
    pairs.append((down_a.at[0], down_w.at[own]))
    for i, packed in enumerate((low, high)):
        for t in range(N_TP):
            mine, cols = pl.ds(256 + 128 * i, 128), pl.ds(128 * t, 128)
            pairs.append((packed.at[pl.ds(2 * D + 128 * t, 128)], down_w.at[mine, cols]))
    copies = fetch(pairs, sems)
    squares = jnp.zeros((HALF, 128), F32)
    for t in range(N_TP):
        cols = slice(128 * t, 128 * (t + 1))
        v = got[t].astype(F32)
        squares = squares + v * v
        x[:, cols] = (v * gain[:, cols]).astype(BF16)
    factor = lax.rsqrt(jnp.sum(squares, axis=1, keepdims=True) / D + NORM_EPS)
    for c in copies[:3]:
        c.wait()
    gate = dot(x[...], gate_w[...]) * factor
    for c in copies[3:6]:
        c.wait()
    up = dot(x[...], up_w[...]) * factor
    hidden = (gate / (1.0 + jnp.exp(-gate)) * up).astype(BF16)
    for c in copies[6:]:
        c.wait()
    for t in range(0, N_TP, 2):
        value = dot(hidden, down_w[:, 128 * t : 128 * (t + 2)])
        parts[t] = value[:, :128].astype(BF16)
        parts[t + 1] = value[:, 128:].astype(BF16)


def gather_sum_body(parts, out):
    core = lax.axis_index("sp") % 2
    for half in range(2):
        total = jnp.zeros((HALF, 128), F32)
        for k in range(N_TP // 2):
            by_x = 2 * k + half
            by_y = (k // 4) * 8 + half * 4 + k % 4
            total = total + parts[jnp.where(core == 0, by_x, by_y)].astype(F32)
        out[half * HALF : (half + 1) * HALF, :] = total.astype(BF16)


def mix_body(returned, stream, ids, weights, out):
    slot_0, slot_1 = slot_columns(ids[...])
    lane = lax.broadcasted_iota(jnp.int32, (TOK, SLOTS), 1)
    rows = returned[...]
    w = weights[...]
    first = dot((lane == slot_0).astype(BF16), rows) * w[:, 0:1]
    second = dot((lane == slot_1).astype(BF16), rows) * w[:, 1:2]
    out[...] = (stream[...].astype(F32) + (first + second)).astype(BF16)


def shape(dims, kind=BF16):
    return pltpu.VMEM(dims, kind)


def room(dims, kind=BF16):
    return pltpu.VMEM(dims, kind)


def kernel(body, outs, rooms, sems, operands, near=()):
    single = not isinstance(outs, tuple)
    places = [pltpu.VMEM if i in near else pltpu.HBM for i in range(len(operands))]
    operands = [pltpu.with_memory_space_constraint(x, m) for x, m in zip(operands, places)]
    return pl.pallas_call(
        body,
        out_shape=outs,
        in_specs=[pl.BlockSpec(memory_space=m) for m in places],
        out_specs=vmem(1)[0] if single else tuple(vmem(len(outs))),
        scratch_shapes=rooms + ([pltpu.SemaphoreType.DMA((sems,))] if sems else []),
        compiler_params=pltpu.CompilerParams(vmem_limit_bytes=24 * 2**20),
    )(*operands)


def to_each(array, axis, groups=None):
    return lax.all_to_all(array, axis, 0, 0, tiled=True, axis_index_groups=groups)


def per_device(
    query_major,
    query_minor,
    latent_rows,
    rope_keys,
    key_up_major,
    value_up_major,
    key_up_minor,
    value_up_minor,
    out_major,
    out_minor,
    residual,
    norm_gain,
    expert_ids,
    expert_weights,
    gate_proj,
    up_proj,
    down_proj,
):
    table = jnp.asarray(TABLE)
    rows = kernel(
        rows_body,
        shape((N_Z, ROWS, 640)),
        [room((ROWS, LATENT)), room((ROPE, TOK)), room((160, 128), F32), room((TOK, ROPE), F32)],
        3,
        (latent_rows, rope_keys.T, table),
    )
    got_rows = to_each(rows, "sp", SAME_CORE)
    low, high = kernel(
        pack_body,
        (shape((3 * D, 128)), shape((3 * D, 128))),
        [],
        4 + 2 * N_TP,
        (gate_proj, up_proj, down_proj),
    )
    packed = kernel(
        choose_body, shape((PACKED, 128)), [room((FAR_ROWS, 640))], 0, (got_rows,), (0,)
    )
    spread = jnp.broadcast_to(packed, (N_TP, PACKED, 128))
    keys = to_each(spread, "tp")
    q_own, up_weights, own_block = kernel(
        queries_body,
        (shape((TOK, 320)), shape((LATENT, 384)), shape((TOK, 640))),
        [room((TOK, 128)), room((160, 128), F32), room((ROPE, TOK))],
        6,
        (
            query_major,
            query_minor,
            table,
            key_up_major,
            value_up_major,
            key_up_minor,
            value_up_minor,
            latent_rows,
            rope_keys.T,
        ),
        (0, 5, 6),
    )
    q_other = lax.ppermute(q_own, "sp", OTHER_CORE)
    blocks = [lax.ppermute(own_block, "sp", along_z(-step)) if step else own_block for step in NEAR]
    from_low = lax.ppermute(low, ("sp", "tp"), ring(1))
    from_high = lax.ppermute(high, ("sp", "tp"), ring(-1))
    own, other = kernel(
        attend_body,
        (shape((TOK, 256), F32), shape((TOK, 256), F32)),
        [
            room((2 * TOK, KEYS), F32),
            room((2 * TOK, KEYS), F32),
            room((KEYS, 192)),
            room((2 * TOK, 320)),
            room((LATENT, 384)),
            room((len(NEAR) * TOK, 640)),
        ],
        3 + len(NEAR),
        (keys, q_own, q_other, up_weights, *blocks),
        (0,),
    )
    from_other = lax.ppermute(other, "sp", OTHER_CORE)
    head_parts = kernel(
        project_body,
        shape((N_TP, TOK, 128)),
        [],
        0,
        (own, from_other, out_major, out_minor),
        range(4),
    )
    head_parts = to_each(head_parts, "tp")
    stream, placed = kernel(
        place_body,
        (shape((TOK, 128)), shape((SLOTS, 128))),
        [],
        0,
        (head_parts, residual, expert_ids),
        range(3),
    )
    arrived = to_each(placed.reshape(EXPERTS, CAP, 128), "sp").reshape(SLOTS, 128)
    here = kernel(weights_here_body, shape((8, 128), F32), [], 0, (from_low, from_high))
    half_rows = kernel(halves_body, shape((N_TP, HALF, 128)), [], 0, (arrived, here), (0,))
    everyone = to_each(half_rows, "tp")
    down_parts = kernel(
        expert_body,
        shape((N_TP, HALF, 128)),
        [room((D, 512)), room((D, 512)), room((512, D)), room((HALF, D))],
        7 + 2 * N_TP,
        (everyone, norm_gain.reshape(1, D), gate_proj, up_proj, down_proj, from_low, from_high),
        (0, 1),
    )
    down_parts = to_each(down_parts, "tp")
    expert_out = kernel(gather_sum_body, shape((SLOTS, 128)), [], 0, (down_parts,), (0,))
    returned = to_each(expert_out.reshape(EXPERTS, CAP, 128), "sp").reshape(SLOTS, 128)
    return kernel(
        mix_body,
        jax.ShapeDtypeStruct((TOK, 128), BF16),
        [],
        0,
        (returned, stream, expert_ids, expert_weights),
        range(4),
    )


def solution(mesh):
    in_specs = (
        P("sp", "tp"),
        P("sp", "tp"),
        P("sp", None),
        P("sp", None),
        P(None, "tp"),
        P(None, "tp"),
        P(None, "tp"),
        P(None, "tp"),
        P("tp", None),
        P("tp", None),
        P("sp", "tp"),
        P(),
        P("sp", None),
        P("sp", None),
        P("sp", None, "tp"),
        P("sp", None, "tp"),
        P("sp", "tp", None),
    )

    return jax.shard_map(
        per_device, mesh=mesh, in_specs=in_specs, out_specs=P("sp", "tp"), check_vma=False
    )
```

```python
import jax
import jax.numpy as jnp
import numpy as np
from jax import lax
from jax.experimental import pallas as pl
from jax.experimental.pallas import tpu as pltpu
from jax.sharding import PartitionSpec as P


F32 = jnp.float32
BF16 = jnp.bfloat16
D = 2048
ROPE = 64
NOPE_MAJOR = 128
NOPE_MINOR = 64
LATENT = 512
TOK = 128
N_TP = 16
N_Z = 16
EXPERTS = 32
CAP = 16
SLOTS = EXPERTS * CAP
ROWS = TOK // N_TP
KEYS = N_Z * TOK
MASKED = -1e30
LOG2_E = float(np.log2(np.e))
NORM_EPS = 1e-6
HALF = SLOTS // 2
NEAR = (-2, -1, 0, 1)
FAR = N_Z - len(NEAR)
FAR_ROWS = FAR * ROWS
PACKED = 4 * FAR_ROWS + FAR_ROWS // 2


def along_z(step):
    moves = [(z, (z + step) % N_Z) for z in range(N_Z)]
    return [(a * 2 + c, b * 2 + c) for a, b in moves if a <= b for c in range(2)]


def turns(positions):
    angles = positions[:, None] * (1.0 / 10000.0 ** (np.arange(32) / 32.0))[None, :]
    return np.concatenate([np.cos(angles), np.sin(angles), np.zeros((len(positions), 64))], axis=1)


TABLE = np.concatenate([turns(np.arange(2 * N_Z) * float(TOK)), turns(np.arange(TOK) * 1.0)]).astype(
    np.float32
)

SAME_CORE = [[z * 2 + c for z in range(N_Z)] for c in range(2)]
OTHER_CORE = [(i, i ^ 1) for i in range(2 * N_Z)]


def ring(step):
    moves = []
    for s in range(2 * N_Z):
        for t in range(N_TP):
            y, x = divmod(t, 4)
            to = (y + step) % 4 * 4 + x if s % 2 else y * 4 + (x + step) % 4
            moves.append((s * N_TP + t, s * N_TP + to))
    return moves


HALF = SLOTS // 2
NEAR = (-2, -1, 0, 1)
FAR = N_Z - len(NEAR)
FAR_ROWS = FAR * ROWS
PACKED = 4 * FAR_ROWS + FAR_ROWS // 2


def along_z(step):
    moves = [(z, (z + step) % N_Z) for z in range(N_Z)]
    return [(a * 2 + c, b * 2 + c) for a, b in moves if a <= b for c in range(2)]


def turns(positions):
    angles = positions[:, None] * (1.0 / 10000.0 ** (np.arange(32) / 32.0))[None, :]
    return np.concatenate([np.cos(angles), np.sin(angles), np.zeros((len(positions), 64))], axis=1)


TABLE = np.concatenate([turns(np.arange(2 * N_Z) * float(TOK)), turns(np.arange(TOK) * 1.0)]).astype(
    np.float32
)

SAME_CORE = [[z * 2 + c for z in range(N_Z)] for c in range(2)]
OTHER_CORE = [(i, i ^ 1) for i in range(2 * N_Z)]


ANY = pl.BlockSpec(memory_space=pl.ANY)


def vmem(n):
    return [pl.BlockSpec(memory_space=pltpu.VMEM)] * n


def fetch(pairs, sems):
    copies = [pltpu.make_async_copy(src, dst, sems.at[i]) for i, (src, dst) in enumerate(pairs)]
    for c in copies:
        c.start()
    return copies


def dot(a, b, dims=((1,), (0,))):
    return lax.dot_general(a, b, (dims, ((), ())), preferred_element_type=F32)


def turn_at(table, block, rows):
    first = table[pl.ds(block, 1), :]
    c_0, s_0 = first[:, :32], first[:, 32:64]
    c_1, s_1 = rows[:, :32], rows[:, 32:64]
    return c_0 * c_1 - s_0 * s_1, s_0 * c_1 + c_0 * s_1


def turned(values, cosine, sine):
    low = values[:, :32].astype(F32)
    high = values[:, 32:].astype(F32)
    return jnp.concatenate(
        [low * cosine - high * sine, high * cosine + low * sine], axis=1
    ).astype(BF16)


def rows_body(lat_in, rope_in, table_in, out, lat, rope, table, by_row, sems):
    block, part = lax.axis_index("sp"), lax.axis_index("tp")
    mine = pl.ds(pl.multiple_of(part * ROWS, ROWS), ROWS)
    for c in fetch(((lat_in.at[mine], lat), (rope_in, rope), (table_in, table)), sems):
        c.wait()
    at = pl.ds(pl.multiple_of(2 * N_Z + part * ROWS, ROWS), ROWS)
    cosine, sine = turn_at(table, block, table[at, :])
    by_row[...] = rope[...].astype(F32).T
    key = turned(by_row[pl.ds(pl.multiple_of(part * ROWS, ROWS), ROWS), :], cosine, sine)
    row = jnp.concatenate([lat[...], key, jnp.zeros((ROWS, 64), BF16)], axis=1)
    for z in range(N_Z):
        out[z] = row


def queries_body(
    maj, low_in, table_in, ku_maj, vu_maj, ku_min, vu_min, lat, rope_in,
    out, weights, block,
    low, table, rope, sems,
):
    copies = fetch(
        (
            (low_in, low),
            (table_in, table),
            (rope_in, rope),
            (ku_maj, weights.at[:, pl.ds(0, 128)]),
            (vu_maj, weights.at[:, pl.ds(128, 128)]),
            (lat, block.at[:, pl.ds(0, LATENT)]),
        ),
        sems,
    )
    weights[:, 256:384] = jnp.concatenate([ku_min[...], vu_min[...]], axis=1)
    for c in copies[:3]:
        c.wait()
    c, s = turn_at(table, lax.axis_index("sp"), table[2 * N_Z :, :])
    key = turned(rope[...].astype(F32).T, c, s)
    block[:, LATENT:] = jnp.concatenate([key, jnp.zeros((TOK, 64), BF16)], axis=1)
    out[...] = jnp.concatenate(
        [
            maj[:, :NOPE_MAJOR],
            turned(maj[:, NOPE_MAJOR:], c, s),
            low[:, :NOPE_MINOR],
            turned(low[:, NOPE_MINOR:], c, s),
        ],
        axis=1,
    )
    for c in copies[3:]:
        c.wait()


def choose_body(got, out, flat):
    z = lax.axis_index("sp") // 2
    for o in range(FAR):
        flat[ROWS * o : ROWS * (o + 1), :] = got[(z + NEAR[-1] + 1 + o) % N_Z]
    for k in range(4):
        out[FAR_ROWS * k : FAR_ROWS * (k + 1), :] = flat[:, 128 * k : 128 * (k + 1)]
    rope = flat[:, 512:576]
    out[4 * FAR_ROWS :, :] = jnp.concatenate([rope[: FAR_ROWS // 2], rope[FAR_ROWS // 2 :]], axis=1)


PER = 4
CHUNK = PER * FAR_ROWS
N_CHUNK = N_TP // PER


def attend_body(keys, q_own_in, q_other_in, up_in, *refs):
    near_in = refs[: len(NEAR)]
    own, other, s_maj, s_min, v_all, q_all, up_weights, near, sems = refs[len(NEAR) :]
    copies = fetch(
        (
            (up_in, up_weights),
            (q_own_in, q_all.at[pl.ds(0, TOK)]),
            (q_other_in, q_all.at[pl.ds(TOK, TOK)]),
        )
        + tuple((b, near.at[pl.ds(TOK * i, TOK)]) for i, b in enumerate(near_in)),
        sems,
    )
    me = lax.axis_index("sp")
    core, z = me % 2, me // 2
    row = lax.broadcasted_iota(jnp.int32, (2 * TOK, 1), 0)
    q_pos = jnp.where(row < TOK, me * TOK + row, (me + 1 - 2 * core) * TOK + row - TOK)
    scale_maj = (NOPE_MAJOR + ROPE) ** -0.5 * LOG2_E
    scale_min = (NOPE_MINOR + ROPE) ** -0.5 * LOG2_E
    tops = [jnp.full((2 * TOK, 128), MASKED, F32)] * 2
    for c in copies[:3]:
        c.wait()
    weights = up_weights[...]
    q_maj, q_min = q_all[:, :192], q_all[:, 192:320]

    def scored(at, width, lat, rope, k_pos, tops):
        up = dot(lat, weights).astype(BF16)
        k_maj = jnp.concatenate([up[:, :128], rope], axis=1)
        k_min = jnp.concatenate([up[:, 256:320], rope], axis=1)
        v_all[at : at + width, :] = jnp.concatenate([up[:, 128:256], up[:, 320:384]], axis=1)
        seen = k_pos <= q_pos
        found = []
        for q, k, scale, store, top in (
            (q_maj, k_maj, scale_maj, s_maj, tops[0]),
            (q_min, k_min, scale_min, s_min, tops[1]),
        ):
            s = jnp.where(seen, dot(q, k, ((1,), (1,))) * scale, MASKED)
            store[:, at : at + width] = s
            for i in range(width // 128):
                top = jnp.maximum(top, s[:, 128 * i : 128 * (i + 1)])
            found.append(top)
        return found

    col = lax.broadcasted_iota(jnp.int32, (1, CHUNK), 1)
    for n in range(N_CHUNK):
        lat_rows, rope_rows = [], []
        for t in range(n * PER, (n + 1) * PER):
            lat_rows.append(
                jnp.concatenate(
                    [keys[t, FAR_ROWS * k : FAR_ROWS * (k + 1), :] for k in range(4)], axis=1
                )
            )
            half = keys[t, 4 * FAR_ROWS :, :]
            rope_rows.append(jnp.concatenate([half[:, :64], half[:, 64:]], axis=0))
        lat = jnp.concatenate(lat_rows, axis=0)
        rope = jnp.concatenate(rope_rows, axis=0)
        inner = col % FAR_ROWS
        k_z = (z + NEAR[-1] + 1 + inner // ROWS) % N_Z
        k_pos = (2 * k_z + core) * TOK + ROWS * (n * PER + col // FAR_ROWS) + inner % ROWS
        tops = scored(CHUNK * n, CHUNK, lat, rope, k_pos, tops)
    for c in copies[3:]:
        c.wait()
    col = lax.broadcasted_iota(jnp.int32, (1, len(NEAR) * TOK), 1)
    k_pos = (2 * ((z + NEAR[0] + N_Z + col // TOK) % N_Z) + core) * TOK + col % TOK
    tops = scored(N_CHUNK * CHUNK, len(NEAR) * TOK, near[:, :512], near[:, 512:576], k_pos, tops)
    top_maj, top_min = tops
    m_maj = jnp.max(top_maj, axis=1, keepdims=True)
    m_min = jnp.max(top_min, axis=1, keepdims=True)
    sum_maj = jnp.zeros((2 * TOK, 128), F32)
    sum_min = jnp.zeros((2 * TOK, 128), F32)
    o_maj = jnp.zeros((2 * TOK, 128), F32)
    o_min = jnp.zeros((2 * TOK, 64), F32)
    step = 512
    for at in range(0, KEYS, step):
        p = jnp.exp2(s_maj[:, at : at + step] - m_maj)
        r = jnp.exp2(s_min[:, at : at + step] - m_min)
        for k in range(step // 128):
            sum_maj = sum_maj + p[:, 128 * k : 128 * (k + 1)]
            sum_min = sum_min + r[:, 128 * k : 128 * (k + 1)]
        v = v_all[at : at + step, :]
        o_maj = o_maj + dot(p.astype(BF16), v[:, :128])
        o_min = o_min + dot(r.astype(BF16), v[:, 128:192])
    l_maj = jnp.sum(sum_maj, axis=1, keepdims=True)
    l_min = jnp.sum(sum_min, axis=1, keepdims=True)
    lane = lax.broadcasted_iota(jnp.int32, (2 * TOK, 64), 1)
    stats = jnp.where(
        lane == 0, m_maj, jnp.where(lane == 1, l_maj, jnp.where(lane == 2, m_min, l_min))
    )
    result = jnp.concatenate([o_maj, o_min, stats], axis=1)
    own[...] = result[:TOK]
    other[...] = result[TOK:]


def project_body(a, b, out_maj, out_min, parts):
    a, b = a[...], b[...]

    def joined(m_at, lo, hi):
        m_a, m_b = a[:, m_at : m_at + 1], b[:, m_at : m_at + 1]
        l_a, l_b = a[:, m_at + 1 : m_at + 2], b[:, m_at + 1 : m_at + 2]
        top = jnp.maximum(m_a, m_b)
        f_a, f_b = jnp.exp2(m_a - top), jnp.exp2(m_b - top)
        total = l_a * f_a + l_b * f_b
        return ((a[:, lo:hi] * f_a + b[:, lo:hi] * f_b) / total).astype(BF16)

    attn_maj = joined(192, 0, 128)
    attn_min = joined(194, 128, 192)
    value = dot(attn_maj, out_maj[...]) + dot(attn_min, out_min[...])
    for t in range(N_TP):
        parts[t] = value[:, 128 * t : 128 * (t + 1)].astype(BF16)


def slot_columns(ids):
    lane = lax.broadcasted_iota(jnp.int32, (TOK, EXPERTS), 1)
    first = (ids[:, 0:1] == lane).astype(F32)
    second = (ids[:, 1:2] == lane).astype(F32)
    below = (
        lax.broadcasted_iota(jnp.int32, (TOK, TOK), 1) < lax.broadcasted_iota(jnp.int32, (TOK, TOK), 0)
    ).astype(BF16)
    earlier = dot(below, (first + second).astype(BF16))
    rank_0 = jnp.sum(first * earlier, axis=1, keepdims=True).astype(jnp.int32)
    rank_1 = jnp.sum(second * earlier, axis=1, keepdims=True).astype(jnp.int32)
    return ids[:, 0:1] * CAP + rank_0, ids[:, 1:2] * CAP + rank_1


def place_body(parts, residual, ids, weights, stream, placed):
    slot_0, slot_1 = slot_columns(ids[...])
    lane = lax.broadcasted_iota(jnp.int32, (TOK, SLOTS), 1)
    select = ((lane == slot_0) | (lane == slot_1)).astype(BF16)
    summed = parts[0].astype(F32)
    for t in range(1, N_TP):
        summed = summed + parts[t].astype(F32)
    rows = (residual[...].astype(F32) + summed).astype(BF16)
    stream[...] = rows
    placed[...] = dot(select, rows, ((0,), (0,))).astype(BF16)


def pack_body(gate, up, down, low, high, sems):
    pairs = []
    for i, out in enumerate((low, high)):
        mine = pl.ds(128 * i, 128)
        pairs.append((gate.at[0, :, mine], out.at[pl.ds(0, D)]))
        pairs.append((up.at[0, :, mine], out.at[pl.ds(D, D)]))
        for t in range(N_TP):
            pairs.append((down.at[0, mine, pl.ds(128 * t, 128)], out.at[pl.ds(2 * D + 128 * t, 128)]))
    for c in fetch(pairs, sems):
        c.wait()


def weights_here_body(low, high, out):
    out[...] = jnp.zeros(out.shape, F32)


def halves_body(arrived, here, out):
    core = lax.axis_index("sp") % 2
    for d in range(N_TP):
        half = jnp.where(core == 0, d % 2, d // 4 % 2)
        out[d] = arrived[pl.ds(pl.multiple_of(half * HALF, HALF), HALF), :]


def expert_body(got, gain, gate_a, up_a, down_a, low, high, parts, gate_w, up_w, down_w, x, sems):
    own = pl.ds(0, 256)
    pairs = []
    for at, (mine, w) in enumerate(((gate_a, gate_w), (up_a, up_w))):
        pairs.append((mine.at[0], w.at[:, own]))
        for i, packed in enumerate((low, high)):
            pairs.append((packed.at[pl.ds(at * D, D)], w.at[:, pl.ds(256 + 128 * i, 128)]))
    pairs.append((down_a.at[0], down_w.at[own]))
    for i, packed in enumerate((low, high)):
        for t in range(N_TP):
            mine, cols = pl.ds(256 + 128 * i, 128), pl.ds(128 * t, 128)
            pairs.append((packed.at[pl.ds(2 * D + 128 * t, 128)], down_w.at[mine, cols]))
    copies = fetch(pairs, sems)
    squares = jnp.zeros((HALF, 128), F32)
    for t in range(N_TP):
        cols = slice(128 * t, 128 * (t + 1))
        v = got[t].astype(F32)
        squares = squares + v * v
        x[:, cols] = (v * gain[:, cols]).astype(BF16)
    factor = lax.rsqrt(jnp.sum(squares, axis=1, keepdims=True) / D + NORM_EPS)
    for c in copies[:3]:
        c.wait()
    gate = dot(x[...], gate_w[...]) * factor
    for c in copies[3:6]:
        c.wait()
    up = dot(x[...], up_w[...]) * factor
    hidden = (gate / (1.0 + jnp.exp(-gate)) * up).astype(BF16)
    for c in copies[6:]:
        c.wait()
    for t in range(0, N_TP, 2):
        value = dot(hidden, down_w[:, 128 * t : 128 * (t + 2)])
        parts[t] = value[:, :128].astype(BF16)
        parts[t + 1] = value[:, 128:].astype(BF16)


def gather_sum_body(parts, out):
    core = lax.axis_index("sp") % 2
    for half in range(2):
        total = jnp.zeros((HALF, 128), F32)
        for k in range(N_TP // 2):
            by_x = 2 * k + half
            by_y = (k // 4) * 8 + half * 4 + k % 4
            total = total + parts[jnp.where(core == 0, by_x, by_y)].astype(F32)
        out[half * HALF : (half + 1) * HALF, :] = total.astype(BF16)


def mix_body(returned, stream, ids, weights, out):
    slot_0, slot_1 = slot_columns(ids[...])
    lane = lax.broadcasted_iota(jnp.int32, (TOK, SLOTS), 1)
    rows = returned[...]
    w = weights[...]
    first = dot((lane == slot_0).astype(BF16), rows) * w[:, 0:1]
    second = dot((lane == slot_1).astype(BF16), rows) * w[:, 1:2]
    out[...] = (stream[...].astype(F32) + (first + second)).astype(BF16)


def shape(dims, kind=BF16):
    return pltpu.VMEM(dims, kind)


def room(dims, kind=BF16):
    return pltpu.VMEM(dims, kind)


def kernel(body, outs, rooms, sems, operands, near=()):
    single = not isinstance(outs, tuple)
    places = [pltpu.VMEM if i in near else pltpu.HBM for i in range(len(operands))]
    operands = [pltpu.with_memory_space_constraint(x, m) for x, m in zip(operands, places)]
    return pl.pallas_call(
        body,
        out_shape=outs,
        in_specs=[pl.BlockSpec(memory_space=m) for m in places],
        out_specs=vmem(1)[0] if single else tuple(vmem(len(outs))),
        scratch_shapes=rooms + ([pltpu.SemaphoreType.DMA((sems,))] if sems else []),
        compiler_params=pltpu.CompilerParams(vmem_limit_bytes=24 * 2**20),
    )(*operands)


def to_each(array, axis, groups=None):
    return lax.all_to_all(array, axis, 0, 0, tiled=True, axis_index_groups=groups)


def per_device(
    query_major,
    query_minor,
    latent_rows,
    rope_keys,
    key_up_major,
    value_up_major,
    key_up_minor,
    value_up_minor,
    out_major,
    out_minor,
    residual,
    norm_gain,
    expert_ids,
    expert_weights,
    gate_proj,
    up_proj,
    down_proj,
):
    table = jnp.asarray(TABLE)
    rows = kernel(
        rows_body,
        shape((N_Z, ROWS, 640)),
        [room((ROWS, LATENT)), room((ROPE, TOK)), room((160, 128), F32), room((TOK, ROPE), F32)],
        3,
        (latent_rows, rope_keys.T, table),
    )
    got_rows = to_each(rows, "sp", SAME_CORE)
    low, high = kernel(
        pack_body,
        (shape((3 * D, 128)), shape((3 * D, 128))),
        [],
        4 + 2 * N_TP,
        (gate_proj, up_proj, down_proj),
    )
    packed = kernel(
        choose_body, shape((PACKED, 128)), [room((FAR_ROWS, 640))], 0, (got_rows,), (0,)
    )
    spread = jnp.broadcast_to(packed, (N_TP, PACKED, 128))
    keys = to_each(spread, "tp")
    q_own, up_weights, own_block = kernel(
        queries_body,
        (shape((TOK, 320)), shape((LATENT, 384)), shape((TOK, 640))),
        [room((TOK, 128)), room((160, 128), F32), room((ROPE, TOK))],
        6,
        (
            query_major,
            query_minor,
            table,
            key_up_major,
            value_up_major,
            key_up_minor,
            value_up_minor,
            latent_rows,
            rope_keys.T,
        ),
        (0, 5, 6),
    )
    q_other = lax.ppermute(q_own, "sp", OTHER_CORE)
    blocks = [lax.ppermute(own_block, "sp", along_z(-step)) if step else own_block for step in NEAR]
    from_low = lax.ppermute(low, ("sp", "tp"), ring(1))
    from_high = lax.ppermute(high, ("sp", "tp"), ring(-1))
    own, other = kernel(
        attend_body,
        (shape((TOK, 256), F32), shape((TOK, 256), F32)),
        [
            room((2 * TOK, KEYS), F32),
            room((2 * TOK, KEYS), F32),
            room((KEYS, 192)),
            room((2 * TOK, 320)),
            room((LATENT, 384)),
            room((len(NEAR) * TOK, 640)),
        ],
        3 + len(NEAR),
        (keys, q_own, q_other, up_weights, *blocks),
        (0,),
    )
    from_other = lax.ppermute(other, "sp", OTHER_CORE)
    head_parts = kernel(
        project_body,
        shape((N_TP, TOK, 128)),
        [],
        0,
        (own, from_other, out_major, out_minor),
        range(4),
    )
    head_parts = to_each(head_parts, "tp")
    stream, placed = kernel(
        place_body,
        (shape((TOK, 128)), shape((SLOTS, 128))),
        [],
        0,
        (head_parts, residual, expert_ids, expert_weights),
        range(4),
    )
    arrived = to_each(placed.reshape(EXPERTS, CAP, 128), "sp").reshape(SLOTS, 128)
    here = kernel(weights_here_body, shape((8, 128), F32), [], 0, (from_low, from_high))
    half_rows = kernel(halves_body, shape((N_TP, HALF, 128)), [], 0, (arrived, here), (0,))
    everyone = to_each(half_rows, "tp")
    down_parts = kernel(
        expert_body,
        shape((N_TP, HALF, 128)),
        [room((D, 512)), room((D, 512)), room((512, D)), room((HALF, D))],
        7 + 2 * N_TP,
        (everyone, norm_gain.reshape(1, D), gate_proj, up_proj, down_proj, from_low, from_high),
        (0, 1),
    )
    down_parts = to_each(down_parts, "tp")
    expert_out = kernel(gather_sum_body, shape((SLOTS, 128)), [], 0, (down_parts,), (0,))
    returned = to_each(expert_out.reshape(EXPERTS, CAP, 128), "sp").reshape(SLOTS, 128)
    return kernel(
        mix_body,
        jax.ShapeDtypeStruct((TOK, 128), BF16),
        [],
        0,
        (returned, stream, expert_ids, expert_weights),
        range(4),
    )


def solution(mesh):
    in_specs = (
        P("sp", "tp"),
        P("sp", "tp"),
        P("sp", None),
        P("sp", None),
        P(None, "tp"),
        P(None, "tp"),
        P(None, "tp"),
        P(None, "tp"),
        P("tp", None),
        P("tp", None),
        P("sp", "tp"),
        P(),
        P("sp", None),
        P("sp", None),
        P("sp", None, "tp"),
        P("sp", None, "tp"),
        P("sp", "tp", None),
    )

    return jax.shard_map(
        per_device, mesh=mesh, in_specs=in_specs, out_specs=P("sp", "tp"), check_vma=False
    )
```

```python
import jax
import jax.numpy as jnp
import numpy as np
from jax import lax
from jax.experimental import pallas as pl
from jax.experimental.pallas import tpu as pltpu
from jax.sharding import PartitionSpec as P


F32 = jnp.float32
BF16 = jnp.bfloat16
D = 2048
ROPE = 64
NOPE_MAJOR = 128
NOPE_MINOR = 64
LATENT = 512
TOK = 128
N_TP = 16
N_Z = 16
EXPERTS = 32
CAP = 16
SLOTS = EXPERTS * CAP
ROWS = TOK // N_TP
KEYS = N_Z * TOK
MASKED = -1e30
LOG2_E = float(np.log2(np.e))
NORM_EPS = 1e-6
HALF = SLOTS // 2
NEAR = (-2, -1, 0, 1)
FAR = N_Z - len(NEAR)
FAR_ROWS = FAR * ROWS
PACKED = 4 * FAR_ROWS + FAR_ROWS // 2


def along_z(step):
    moves = [(z, (z + step) % N_Z) for z in range(N_Z)]
    return [(a * 2 + c, b * 2 + c) for a, b in moves if a <= b for c in range(2)]


def turns(positions):
    angles = positions[:, None] * (1.0 / 10000.0 ** (np.arange(32) / 32.0))[None, :]
    return np.concatenate([np.cos(angles), np.sin(angles), np.zeros((len(positions), 64))], axis=1)


TABLE = np.concatenate([turns(np.arange(2 * N_Z) * float(TOK)), turns(np.arange(TOK) * 1.0)]).astype(
    np.float32
)

SAME_CORE = [[z * 2 + c for z in range(N_Z)] for c in range(2)]
OTHER_CORE = [(i, i ^ 1) for i in range(2 * N_Z)]


def ring(step):
    moves = []
    for s in range(2 * N_Z):
        for t in range(N_TP):
            y, x = divmod(t, 4)
            to = (y + step) % 4 * 4 + x if s % 2 else y * 4 + (x + step) % 4
            moves.append((s * N_TP + t, s * N_TP + to))
    return moves


HALF = SLOTS // 2
NEAR = (-2, -1, 0, 1)
FAR = N_Z - len(NEAR)
FAR_ROWS = FAR * ROWS
PACKED = 4 * FAR_ROWS + FAR_ROWS // 2


def along_z(step):
    moves = [(z, (z + step) % N_Z) for z in range(N_Z)]
    return [(a * 2 + c, b * 2 + c) for a, b in moves if a <= b for c in range(2)]


def turns(positions):
    angles = positions[:, None] * (1.0 / 10000.0 ** (np.arange(32) / 32.0))[None, :]
    return np.concatenate([np.cos(angles), np.sin(angles), np.zeros((len(positions), 64))], axis=1)


TABLE = np.concatenate([turns(np.arange(2 * N_Z) * float(TOK)), turns(np.arange(TOK) * 1.0)]).astype(
    np.float32
)

SAME_CORE = [[z * 2 + c for z in range(N_Z)] for c in range(2)]
OTHER_CORE = [(i, i ^ 1) for i in range(2 * N_Z)]


ANY = pl.BlockSpec(memory_space=pl.ANY)


def vmem(n):
    return [pl.BlockSpec(memory_space=pltpu.VMEM)] * n


def fetch(pairs, sems):
    copies = [pltpu.make_async_copy(src, dst, sems.at[i]) for i, (src, dst) in enumerate(pairs)]
    for c in copies:
        c.start()
    return copies


def dot(a, b, dims=((1,), (0,))):
    return lax.dot_general(a, b, (dims, ((), ())), preferred_element_type=F32)


def turn_at(table, block, rows):
    first = table[pl.ds(block, 1), :]
    c_0, s_0 = first[:, :32], first[:, 32:64]
    c_1, s_1 = rows[:, :32], rows[:, 32:64]
    return c_0 * c_1 - s_0 * s_1, s_0 * c_1 + c_0 * s_1


def turned(values, cosine, sine):
    low = values[:, :32].astype(F32)
    high = values[:, 32:].astype(F32)
    return jnp.concatenate(
        [low * cosine - high * sine, high * cosine + low * sine], axis=1
    ).astype(BF16)


def rows_body(lat_in, rope_in, table_in, out, lat, rope, table, by_row, sems):
    block, part = lax.axis_index("sp"), lax.axis_index("tp")
    mine = pl.ds(pl.multiple_of(part * ROWS, ROWS), ROWS)
    for c in fetch(((lat_in.at[mine], lat), (rope_in, rope), (table_in, table)), sems):
        c.wait()
    at = pl.ds(pl.multiple_of(2 * N_Z + part * ROWS, ROWS), ROWS)
    cosine, sine = turn_at(table, block, table[at, :])
    by_row[...] = rope[...].astype(F32).T
    key = turned(by_row[pl.ds(pl.multiple_of(part * ROWS, ROWS), ROWS), :], cosine, sine)
    row = jnp.concatenate([lat[...], key, jnp.zeros((ROWS, 64), BF16)], axis=1)
    for z in range(N_Z):
        out[z] = row


def queries_body(
    maj, low_in, table_in, ku_maj, vu_maj, ku_min, vu_min, lat, rope_in,
    out, weights, block,
    low, table, rope, sems,
):
    copies = fetch(
        (
            (low_in, low),
            (table_in, table),
            (rope_in, rope),
            (ku_maj, weights.at[:, pl.ds(0, 128)]),
            (vu_maj, weights.at[:, pl.ds(128, 128)]),
            (lat, block.at[:, pl.ds(0, LATENT)]),
        ),
        sems,
    )
    weights[:, 256:384] = jnp.concatenate([ku_min[...], vu_min[...]], axis=1)
    for c in copies[:3]:
        c.wait()
    c, s = turn_at(table, lax.axis_index("sp"), table[2 * N_Z :, :])
    key = turned(rope[...].astype(F32).T, c, s)
    block[:, LATENT:] = jnp.concatenate([key, jnp.zeros((TOK, 64), BF16)], axis=1)
    out[...] = jnp.concatenate(
        [
            maj[:, :NOPE_MAJOR],
            turned(maj[:, NOPE_MAJOR:], c, s),
            low[:, :NOPE_MINOR],
            turned(low[:, NOPE_MINOR:], c, s),
        ],
        axis=1,
    )
    for c in copies[3:]:
        c.wait()


def choose_body(got, out, flat):
    z = lax.axis_index("sp") // 2
    for o in range(FAR):
        flat[ROWS * o : ROWS * (o + 1), :] = got[(z + NEAR[-1] + 1 + o) % N_Z]
    for k in range(4):
        out[FAR_ROWS * k : FAR_ROWS * (k + 1), :] = flat[:, 128 * k : 128 * (k + 1)]
    rope = flat[:, 512:576]
    out[4 * FAR_ROWS :, :] = jnp.concatenate([rope[: FAR_ROWS // 2], rope[FAR_ROWS // 2 :]], axis=1)


PER = 4
CHUNK = PER * FAR_ROWS
N_CHUNK = N_TP // PER


def attend_body(keys, q_own_in, q_other_in, up_in, *refs):
    near_in = refs[: len(NEAR)]
    own, other, s_maj, s_min, v_all, q_all, up_weights, near, sems = refs[len(NEAR) :]
    copies = fetch(
        (
            (up_in, up_weights),
            (q_own_in, q_all.at[pl.ds(0, TOK)]),
            (q_other_in, q_all.at[pl.ds(TOK, TOK)]),
        ),
        sems,
    )
    me = lax.axis_index("sp")
    core, z = me % 2, me // 2
    row = lax.broadcasted_iota(jnp.int32, (2 * TOK, 1), 0)
    q_pos = jnp.where(row < TOK, me * TOK + row, (me + 1 - 2 * core) * TOK + row - TOK)
    scale_maj = (NOPE_MAJOR + ROPE) ** -0.5 * LOG2_E
    scale_min = (NOPE_MINOR + ROPE) ** -0.5 * LOG2_E
    tops = [jnp.full((2 * TOK, 128), MASKED, F32)] * 2
    for c in copies:
        c.wait()
    blocks = fetch(
        [(b, near.at[pl.ds(TOK * i, TOK)]) for i, b in enumerate(near_in)],
        sems.at[pl.ds(3, len(NEAR))],
    )
    weights = up_weights[...]
    q_maj, q_min = q_all[:, :192], q_all[:, 192:320]

    def scored(at, width, lat, rope, k_pos, tops):
        up = dot(lat, weights).astype(BF16)
        k_maj = jnp.concatenate([up[:, :128], rope], axis=1)
        k_min = jnp.concatenate([up[:, 256:320], rope], axis=1)
        v_all[at : at + width, :] = jnp.concatenate([up[:, 128:256], up[:, 320:384]], axis=1)
        seen = k_pos <= q_pos
        found = []
        for q, k, scale, store, top in (
            (q_maj, k_maj, scale_maj, s_maj, tops[0]),
            (q_min, k_min, scale_min, s_min, tops[1]),
        ):
            s = jnp.where(seen, dot(q, k, ((1,), (1,))) * scale, MASKED)
            store[:, at : at + width] = s
            for i in range(width // 128):
                top = jnp.maximum(top, s[:, 128 * i : 128 * (i + 1)])
            found.append(top)
        return found

    col = lax.broadcasted_iota(jnp.int32, (1, CHUNK), 1)
    for n in range(N_CHUNK):
        lat_rows, rope_rows = [], []
        for t in range(n * PER, (n + 1) * PER):
            lat_rows.append(
                jnp.concatenate(
                    [keys[t, FAR_ROWS * k : FAR_ROWS * (k + 1), :] for k in range(4)], axis=1
                )
            )
            half = keys[t, 4 * FAR_ROWS :, :]
            rope_rows.append(jnp.concatenate([half[:, :64], half[:, 64:]], axis=0))
        lat = jnp.concatenate(lat_rows, axis=0)
        rope = jnp.concatenate(rope_rows, axis=0)
        inner = col % FAR_ROWS
        k_z = (z + NEAR[-1] + 1 + inner // ROWS) % N_Z
        k_pos = (2 * k_z + core) * TOK + ROWS * (n * PER + col // FAR_ROWS) + inner % ROWS
        tops = scored(CHUNK * n, CHUNK, lat, rope, k_pos, tops)
    for c in blocks:
        c.wait()
    col = lax.broadcasted_iota(jnp.int32, (1, len(NEAR) * TOK), 1)
    k_pos = (2 * ((z + NEAR[0] + N_Z + col // TOK) % N_Z) + core) * TOK + col % TOK
    tops = scored(N_CHUNK * CHUNK, len(NEAR) * TOK, near[:, :512], near[:, 512:576], k_pos, tops)
    top_maj, top_min = tops
    m_maj = jnp.max(top_maj, axis=1, keepdims=True)
    m_min = jnp.max(top_min, axis=1, keepdims=True)
    sum_maj = jnp.zeros((2 * TOK, 128), F32)
    sum_min = jnp.zeros((2 * TOK, 128), F32)
    o_maj = jnp.zeros((2 * TOK, 128), F32)
    o_min = jnp.zeros((2 * TOK, 64), F32)
    step = 512
    for at in range(0, KEYS, step):
        p = jnp.exp2(s_maj[:, at : at + step] - m_maj)
        r = jnp.exp2(s_min[:, at : at + step] - m_min)
        for k in range(step // 128):
            sum_maj = sum_maj + p[:, 128 * k : 128 * (k + 1)]
            sum_min = sum_min + r[:, 128 * k : 128 * (k + 1)]
        v = v_all[at : at + step, :]
        o_maj = o_maj + dot(p.astype(BF16), v[:, :128])
        o_min = o_min + dot(r.astype(BF16), v[:, 128:192])
    l_maj = jnp.sum(sum_maj, axis=1, keepdims=True)
    l_min = jnp.sum(sum_min, axis=1, keepdims=True)
    lane = lax.broadcasted_iota(jnp.int32, (2 * TOK, 64), 1)
    stats = jnp.where(
        lane == 0, m_maj, jnp.where(lane == 1, l_maj, jnp.where(lane == 2, m_min, l_min))
    )
    result = jnp.concatenate([o_maj, o_min, stats], axis=1)
    own[...] = result[:TOK]
    other[...] = result[TOK:]


def project_body(a, b, out_maj, out_min, parts):
    a, b = a[...], b[...]

    def joined(m_at, lo, hi):
        m_a, m_b = a[:, m_at : m_at + 1], b[:, m_at : m_at + 1]
        l_a, l_b = a[:, m_at + 1 : m_at + 2], b[:, m_at + 1 : m_at + 2]
        top = jnp.maximum(m_a, m_b)
        f_a, f_b = jnp.exp2(m_a - top), jnp.exp2(m_b - top)
        total = l_a * f_a + l_b * f_b
        return ((a[:, lo:hi] * f_a + b[:, lo:hi] * f_b) / total).astype(BF16)

    attn_maj = joined(192, 0, 128)
    attn_min = joined(194, 128, 192)
    value = dot(attn_maj, out_maj[...]) + dot(attn_min, out_min[...])
    for t in range(N_TP):
        parts[t] = value[:, 128 * t : 128 * (t + 1)].astype(BF16)


def slot_columns(ids):
    lane = lax.broadcasted_iota(jnp.int32, (TOK, EXPERTS), 1)
    first = (ids[:, 0:1] == lane).astype(F32)
    second = (ids[:, 1:2] == lane).astype(F32)
    below = (
        lax.broadcasted_iota(jnp.int32, (TOK, TOK), 1) < lax.broadcasted_iota(jnp.int32, (TOK, TOK), 0)
    ).astype(BF16)
    earlier = dot(below, (first + second).astype(BF16))
    rank_0 = jnp.sum(first * earlier, axis=1, keepdims=True).astype(jnp.int32)
    rank_1 = jnp.sum(second * earlier, axis=1, keepdims=True).astype(jnp.int32)
    return ids[:, 0:1] * CAP + rank_0, ids[:, 1:2] * CAP + rank_1


def place_body(parts, residual, ids, weights, stream, placed):
    slot_0, slot_1 = slot_columns(ids[...])
    lane = lax.broadcasted_iota(jnp.int32, (TOK, SLOTS), 1)
    select = ((lane == slot_0) | (lane == slot_1)).astype(BF16)
    summed = parts[0].astype(F32)
    for t in range(1, N_TP):
        summed = summed + parts[t].astype(F32)
    rows = (residual[...].astype(F32) + summed).astype(BF16)
    stream[...] = rows
    placed[...] = dot(select, rows, ((0,), (0,))).astype(BF16)


def pack_body(gate, up, down, low, high, sems):
    pairs = []
    for i, out in enumerate((low, high)):
        mine = pl.ds(128 * i, 128)
        pairs.append((gate.at[0, :, mine], out.at[pl.ds(0, D)]))
        pairs.append((up.at[0, :, mine], out.at[pl.ds(D, D)]))
        for t in range(N_TP):
            pairs.append((down.at[0, mine, pl.ds(128 * t, 128)], out.at[pl.ds(2 * D + 128 * t, 128)]))
    for c in fetch(pairs, sems):
        c.wait()


def weights_here_body(low, high, out):
    out[...] = jnp.zeros(out.shape, F32)


def halves_body(arrived, here, out):
    core = lax.axis_index("sp") % 2
    for d in range(N_TP):
        half = jnp.where(core == 0, d % 2, d // 4 % 2)
        out[d] = arrived[pl.ds(pl.multiple_of(half * HALF, HALF), HALF), :]


def expert_body(got, gain, gate_a, up_a, down_a, low, high, parts, gate_w, up_w, down_w, x, sems):
    own = pl.ds(0, 256)
    pairs = []
    for at, (mine, w) in enumerate(((gate_a, gate_w), (up_a, up_w))):
        pairs.append((mine.at[0], w.at[:, own]))
        for i, packed in enumerate((low, high)):
            pairs.append((packed.at[pl.ds(at * D, D)], w.at[:, pl.ds(256 + 128 * i, 128)]))
    pairs.append((down_a.at[0], down_w.at[own]))
    for t in range(N_TP):
        for i, packed in enumerate((low, high)):
            mine, cols = pl.ds(256 + 128 * i, 128), pl.ds(128 * t, 128)
            pairs.append((packed.at[pl.ds(2 * D + 128 * t, 128)], down_w.at[mine, cols]))
    copies = fetch(pairs, sems)
    squares = jnp.zeros((HALF, 128), F32)
    for t in range(N_TP):
        cols = slice(128 * t, 128 * (t + 1))
        v = got[t].astype(F32)
        squares = squares + v * v
        x[:, cols] = (v * gain[:, cols]).astype(BF16)
    factor = lax.rsqrt(jnp.sum(squares, axis=1, keepdims=True) / D + NORM_EPS)
    for c in copies[:3]:
        c.wait()
    gate = dot(x[...], gate_w[...]) * factor
    for c in copies[3:6]:
        c.wait()
    up = dot(x[...], up_w[...]) * factor
    hidden = (gate / (1.0 + jnp.exp(-gate)) * up).astype(BF16)
    copies[6].wait()
    for t in range(0, N_TP, 2):
        for c in copies[7 + 2 * t : 11 + 2 * t]:
            c.wait()
        value = dot(hidden, down_w[:, 128 * t : 128 * (t + 2)])
        parts[t] = value[:, :128].astype(BF16)
        parts[t + 1] = value[:, 128:].astype(BF16)


def gather_sum_body(parts, out):
    core = lax.axis_index("sp") % 2
    for half in range(2):
        total = jnp.zeros((HALF, 128), F32)
        for k in range(N_TP // 2):
            by_x = 2 * k + half
            by_y = (k // 4) * 8 + half * 4 + k % 4
            total = total + parts[jnp.where(core == 0, by_x, by_y)].astype(F32)
        out[half * HALF : (half + 1) * HALF, :] = total.astype(BF16)


def mix_body(returned, stream, ids, weights, out):
    slot_0, slot_1 = slot_columns(ids[...])
    lane = lax.broadcasted_iota(jnp.int32, (TOK, SLOTS), 1)
    rows = returned[...]
    w = weights[...]
    first = dot((lane == slot_0).astype(BF16), rows) * w[:, 0:1]
    second = dot((lane == slot_1).astype(BF16), rows) * w[:, 1:2]
    out[...] = (stream[...].astype(F32) + (first + second)).astype(BF16)


def shape(dims, kind=BF16):
    return pltpu.VMEM(dims, kind)


def room(dims, kind=BF16):
    return pltpu.VMEM(dims, kind)


def kernel(body, outs, rooms, sems, operands, near=()):
    single = not isinstance(outs, tuple)
    places = [pltpu.VMEM if i in near else pltpu.HBM for i in range(len(operands))]
    operands = [pltpu.with_memory_space_constraint(x, m) for x, m in zip(operands, places)]
    return pl.pallas_call(
        body,
        out_shape=outs,
        in_specs=[pl.BlockSpec(memory_space=m) for m in places],
        out_specs=vmem(1)[0] if single else tuple(vmem(len(outs))),
        scratch_shapes=rooms + ([pltpu.SemaphoreType.DMA((sems,))] if sems else []),
        compiler_params=pltpu.CompilerParams(vmem_limit_bytes=24 * 2**20),
    )(*operands)


def to_each(array, axis, groups=None):
    return lax.all_to_all(array, axis, 0, 0, tiled=True, axis_index_groups=groups)


def per_device(
    query_major,
    query_minor,
    latent_rows,
    rope_keys,
    key_up_major,
    value_up_major,
    key_up_minor,
    value_up_minor,
    out_major,
    out_minor,
    residual,
    norm_gain,
    expert_ids,
    expert_weights,
    gate_proj,
    up_proj,
    down_proj,
):
    table = jnp.asarray(TABLE)
    rows = kernel(
        rows_body,
        shape((N_Z, ROWS, 640)),
        [room((ROWS, LATENT)), room((ROPE, TOK)), room((160, 128), F32), room((TOK, ROPE), F32)],
        3,
        (latent_rows, rope_keys.T, table),
    )
    got_rows = to_each(rows, "sp", SAME_CORE)
    low, high = kernel(
        pack_body,
        (shape((3 * D, 128)), shape((3 * D, 128))),
        [],
        4 + 2 * N_TP,
        (gate_proj, up_proj, down_proj),
    )
    packed = kernel(
        choose_body, shape((PACKED, 128)), [room((FAR_ROWS, 640))], 0, (got_rows,), (0,)
    )
    spread = jnp.broadcast_to(packed, (N_TP, PACKED, 128))
    keys = to_each(spread, "tp")
    q_own, up_weights, own_block = kernel(
        queries_body,
        (shape((TOK, 320)), shape((LATENT, 384)), shape((TOK, 640))),
        [room((TOK, 128)), room((160, 128), F32), room((ROPE, TOK))],
        6,
        (
            query_major,
            query_minor,
            table,
            key_up_major,
            value_up_major,
            key_up_minor,
            value_up_minor,
            latent_rows,
            rope_keys.T,
        ),
        (0, 5, 6),
    )
    q_other = lax.ppermute(q_own, "sp", OTHER_CORE)
    blocks = [lax.ppermute(own_block, "sp", along_z(-step)) if step else own_block for step in NEAR]
    from_low = lax.ppermute(low, ("sp", "tp"), ring(1))
    from_high = lax.ppermute(high, ("sp", "tp"), ring(-1))
    own, other = kernel(
        attend_body,
        (shape((TOK, 256), F32), shape((TOK, 256), F32)),
        [
            room((2 * TOK, KEYS), F32),
            room((2 * TOK, KEYS), F32),
            room((KEYS, 192)),
            room((2 * TOK, 320)),
            room((LATENT, 384)),
            room((len(NEAR) * TOK, 640)),
        ],
        3 + len(NEAR),
        (keys, q_own, q_other, up_weights, *blocks),
        (0,),
    )
    from_other = lax.ppermute(other, "sp", OTHER_CORE)
    head_parts = kernel(
        project_body,
        shape((N_TP, TOK, 128)),
        [],
        0,
        (own, from_other, out_major, out_minor),
        range(4),
    )
    head_parts = to_each(head_parts, "tp")
    stream, placed = kernel(
        place_body,
        (shape((TOK, 128)), shape((SLOTS, 128))),
        [],
        0,
        (head_parts, residual, expert_ids, expert_weights),
        range(4),
    )
    arrived = to_each(placed.reshape(EXPERTS, CAP, 128), "sp").reshape(SLOTS, 128)
    here = kernel(weights_here_body, shape((8, 128), F32), [], 0, (from_low, from_high))
    half_rows = kernel(halves_body, shape((N_TP, HALF, 128)), [], 0, (arrived, here), (0,))
    everyone = to_each(half_rows, "tp")
    down_parts = kernel(
        expert_body,
        shape((N_TP, HALF, 128)),
        [room((D, 512)), room((D, 512)), room((512, D)), room((HALF, D))],
        7 + 2 * N_TP,
        (everyone, norm_gain.reshape(1, D), gate_proj, up_proj, down_proj, from_low, from_high),
        (0, 1),
    )
    down_parts = to_each(down_parts, "tp")
    expert_out = kernel(gather_sum_body, shape((SLOTS, 128)), [], 0, (down_parts,), (0,))
    returned = to_each(expert_out.reshape(EXPERTS, CAP, 128), "sp").reshape(SLOTS, 128)
    return kernel(
        mix_body,
        jax.ShapeDtypeStruct((TOK, 128), BF16),
        [],
        0,
        (returned, stream, expert_ids, expert_weights),
        range(4),
    )


def solution(mesh):
    in_specs = (
        P("sp", "tp"),
        P("sp", "tp"),
        P("sp", None),
        P("sp", None),
        P(None, "tp"),
        P(None, "tp"),
        P(None, "tp"),
        P(None, "tp"),
        P("tp", None),
        P("tp", None),
        P("sp", "tp"),
        P(),
        P("sp", None),
        P("sp", None),
        P("sp", None, "tp"),
        P("sp", None, "tp"),
        P("sp", "tp", None),
    )

    return jax.shard_map(
        per_device, mesh=mesh, in_specs=in_specs, out_specs=P("sp", "tp"), check_vma=False
    )
```
